32 devices in a mesh: sp: 4 (over z), fs: 4 (over y, x), tp: 2 (over core).
Axes of the slice: x: 2, y: 2, z: 4, core: 2. Of those that a mesh axis runs over, the one named last changes fastest.
Arguments:
- recurrent_query: bfloat16 [4, 1024, 1024], P('fs', 'sp', 'tp'), may hold values from -6 to 6
- forget_logits: bfloat16 [4, 1024, 1024], P('fs', 'sp', 'tp'), may hold values from -6 to 6
- recurrent_value: bfloat16 [4, 1024, 1024], P('fs', 'sp', 'tp'), may hold values from -6 to 6
- forget_floor: float32 [2, 1024], P(None, 'tp'), may hold values from 0.8 to 1
- extra_log_decay: float32 [4, 1024, 8], P('fs', 'sp', 'tp'), may hold values from -1 to 0
- recurrent_norm_gain: float32 [1024], P('tp'), may hold values from 0.1 to 1.9
- attention_query: bfloat16 [4, 1024, 768], P('fs', 'sp', 'tp'), may hold values from -300 to 300
- latent: bfloat16 [4, 1024, 256], P('fs', 'sp'), may hold values from -6 to 6
- rotary_key: bfloat16 [4, 1024, 32], P('fs', 'sp'), may hold values from -15 to 15
- latent_norm_gain: float32 [256], replicated, may hold values from 0.1 to 1.9
- latent_up_weight: bfloat16 [256, 1024], replicated, may hold values from -0.375 to 0.375
- recurrent_output_weight: bfloat16 [1024, 2048], P('tp', 'fs'), may hold values from -0.1875 to 0.1875
- attention_output_weight: bfloat16 [512, 2048], P('tp', 'fs'), may hold values from -2 to 2
Outputs:
- mixed: bfloat16 [4, 1024, 2048], P('fs', ('sp', 'tp'))
- log_weight: float32 [4, 1024, 8], P('fs', 'sp', 'tp')
The draws below stay inside these ranges and needn't reach their ends.
All inputs are finite; a program needn't handle non-finite values.
Results may differ from the reference program's by a relative error of at most 0.013.
The reference program's roundings to bfloat16 on the way count: a program that leaves them out, or rounds other values in their place, can miss the bound.
Values may be sent and summed in bfloat16 or wider, within the bound.
A program may use at most 128 MiB of HBM per device.

```python
import math
import jax
import jax.numpy as jnp
from jax import lax

D = 2048
RECURRENT_HEADS = 8
HG_DK = 128
HG_DV = 128
MLA_HEADS = 8
NOPE = 64
ROPE = 32
VDIM = 64
KV_RANK = 256
HG_BLOCK = 64
TOK_DEV = 256
SEQUENCE_LENGTH = 1024
SEQUENCE_GROUPS = 4
GROUP_TOKENS = 1024
HG_KEY = 1024
HG_WIDTH = 1024
MLA_WIDTH = 512
N_TP = 2


def draw_forget_floor(key, part):
    pick_key, fast_key, rate_key = jax.random.split(jax.random.fold_in(key, 1), 3)
    slow_share = 0.5
    slowly = jax.random.uniform(pick_key, (2, RECURRENT_HEADS, 1), jnp.float32) < slow_share
    fast_bound = jax.random.uniform(fast_key, (2, RECURRENT_HEADS, HG_DK), jnp.float32, 0.8, 0.92)
    slow_rates = jnp.exp(jax.random.uniform(rate_key, (2, RECURRENT_HEADS, HG_DK), jnp.float32, math.log(0.02), math.log(0.08))) / SEQUENCE_LENGTH
    bounds = jnp.where(slowly, 1.0 - slow_rates, fast_bound)
    return bounds.reshape(2, HG_KEY).astype(jnp.float32)


def draw_extra_log_decay(key, part):
    level_key, striking_key, falling_key = jax.random.split(jax.random.fold_in(key, 2), 3)
    blocks = GROUP_TOKENS // TOK_DEV
    levels = jnp.exp(jax.random.uniform(level_key, (SEQUENCE_GROUPS, blocks, 1, RECURRENT_HEADS), jnp.float32, math.log(0.15), math.log(0.6))) / SEQUENCE_LENGTH
    stable_value = -jnp.broadcast_to(levels, (SEQUENCE_GROUPS, blocks, TOK_DEV, RECURRENT_HEADS)).reshape(SEQUENCE_GROUPS, GROUP_TOKENS, RECURRENT_HEADS)
    spike_strikes = jax.random.uniform(striking_key, (SEQUENCE_GROUPS, GROUP_TOKENS, RECURRENT_HEADS), jnp.float32) < 2.0 / SEQUENCE_LENGTH
    spike_falls = jnp.log(jax.random.uniform(falling_key, (SEQUENCE_GROUPS, GROUP_TOKENS, RECURRENT_HEADS), jnp.float32, 0.5, 0.8))
    return (stable_value + jnp.where(spike_strikes, spike_falls, 0.0)).astype(jnp.float32)


def drawn_keys(key):
    base_keys = jnp.clip(jax.random.normal(jax.random.fold_in(key, 5), (SEQUENCE_GROUPS, GROUP_TOKENS, ROPE), jnp.float32), -4.5, 4.5)
    return base_keys


def draw_rotary_key(key, part):
    base_keys = drawn_keys(key)
    values = base_keys
    return values.astype(jnp.bfloat16)


def draw_attention_query(key, part):
    normal = jnp.clip(2.0 * jax.random.normal(jax.random.fold_in(key, 6), (SEQUENCE_GROUPS, GROUP_TOKENS, MLA_HEADS, NOPE + ROPE), jnp.float32), -12.0, 12.0)
    return normal.reshape(SEQUENCE_GROUPS, GROUP_TOKENS, MLA_HEADS * (NOPE + ROPE)).astype(jnp.bfloat16)


def block_levels(key, extent, pieces, least, largest):
    loudness = 1.0
    for axis_at, shards_of in pieces:
        steps = jax.random.uniform(jax.random.fold_in(jax.random.fold_in(key, 6), axis_at), (shards_of,), jnp.float32, least / len(pieces), largest / len(pieces))
        loudness = loudness * jnp.repeat(jnp.exp(steps), extent[axis_at] // shards_of).reshape((-1,) + (1,) * (len(extent) - 1 - axis_at))
    return loudness


def gaussian(own_key, dims, deviation, limit, pieces=(), kind=jnp.bfloat16):
    entries = jax.random.normal(own_key, dims, jnp.float32) * deviation
    if len(pieces) > 0:
        entries = block_levels(own_key, dims, pieces, -0.22, 0.18) * entries
    return jnp.clip(entries, min=-limit, max=limit).astype(kind)


def setup_inputs(seed: int = 0) -> dict:
    key_of = jax.random.split(jax.random.key(seed), 14)
    recurrent_query = gaussian(key_of[0], (SEQUENCE_GROUPS, GROUP_TOKENS, HG_KEY), 1.0, 6.0, ((0, 4), (1, 4), (2, 2)))
    forget_logits = gaussian(key_of[1], (SEQUENCE_GROUPS, GROUP_TOKENS, HG_KEY), 1.0, 6.0, ((0, 4), (1, 4), (2, 2)))
    recurrent_value = gaussian(key_of[2], (SEQUENCE_GROUPS, GROUP_TOKENS, HG_WIDTH), 1.0, 6.0, ((0, 4), (1, 4), (2, 2)))
    forget_floor = draw_forget_floor(jax.random.fold_in(key_of[13], 71), 0)
    extra_log_decay = draw_extra_log_decay(jax.random.fold_in(key_of[13], 71), 0)
    recurrent_norm_gain = jnp.clip(1.0 + 0.18 * jax.random.normal(key_of[5], (HG_WIDTH,), jnp.float32), 0.1, 1.9)
    attention_query = draw_attention_query(jax.random.fold_in(key_of[13], 71), 0)
    latent = gaussian(key_of[7], (SEQUENCE_GROUPS, GROUP_TOKENS, KV_RANK), 1.0, 6.0, ((0, 4), (1, 4)))
    rotary_key = draw_rotary_key(jax.random.fold_in(key_of[13], 71), 0)
    latent_norm_gain = jnp.clip(1.0 + 0.18 * jax.random.normal(key_of[9], (KV_RANK,), jnp.float32), 0.1, 1.9)
    latent_up_weight = gaussian(key_of[10], (KV_RANK, MLA_HEADS * (NOPE + VDIM)), KV_RANK ** -0.5, 0.375)
    recurrent_output_weight = gaussian(key_of[11], (HG_WIDTH, D), HG_WIDTH ** -0.5, 0.1875, ((0, 2), (1, 4)))
    attention_output_weight = gaussian(key_of[12], (MLA_WIDTH, D), (max(MLA_WIDTH // 64, 1)) ** -0.5, 2.0, ((0, 2), (1, 4)))
    return dict(recurrent_query=recurrent_query, forget_logits=forget_logits, recurrent_value=recurrent_value, forget_floor=forget_floor, extra_log_decay=extra_log_decay, recurrent_norm_gain=recurrent_norm_gain, attention_query=attention_query, latent=latent, rotary_key=rotary_key, latent_norm_gain=latent_norm_gain, latent_up_weight=latent_up_weight, recurrent_output_weight=recurrent_output_weight, attention_output_weight=attention_output_weight)


norm_eps = 1e-06
rope_base = 10000.0
largest_value = lax.Precision.HIGHEST

def rope_tables(token_count, offset):
    places = offset + jnp.arange(token_count).astype(jnp.float32)
    pair_count = ROPE // 2
    inverse = rope_base ** (-jnp.arange(pair_count).astype(jnp.float32) / pair_count)
    angles = places[:, None] * inverse[None, :]
    return (jnp.cos(angles), jnp.sin(angles))

def rotate(tensor, cos_table, sin_table):
    half_width = tensor.shape[-1] // 2
    first_half = tensor[..., :half_width]
    second_half = tensor[..., half_width:]
    return jnp.concatenate([first_half * cos_table - second_half * sin_table, first_half * sin_table + second_half * cos_table], axis=-1)

def block_pass(queries, key_matrix, values, decay_logarithm, carried):
    length = queries.shape[0]
    blocks = length // HG_BLOCK

    def split_blocks(tensor):
        return tensor.reshape((blocks, HG_BLOCK) + tensor.shape[1:])
    lower_mask = jnp.tril(jnp.ones((HG_BLOCK, HG_BLOCK), dtype=bool))

    def advance(running_state, input_tuple):
        query_blk, key_tile, value_tile, decay_blk = input_tuple
        inner_block_term = jnp.cumsum(decay_blk, axis=0)
        damped_query = query_blk * jnp.exp(inner_block_term)
        key_decayed = key_tile * jnp.exp(-inner_block_term)
        cross_block_term = jnp.einsum('mcx,cxn->mcn', damped_query, running_state, precision=largest_value)
        scores = jnp.einsum('thk,shk->hts', damped_query, key_decayed, precision=largest_value)
        scores = jnp.where(lower_mask[None], scores, 0.0)
        intra_term = jnp.einsum('hts,shv->thv', scores, value_tile, precision=largest_value)
        decay_total = inner_block_term[-1]
        updated_state = jnp.exp(decay_total)[:, :, None] * running_state + jnp.einsum('jrg,jrb->rgb', key_tile * jnp.exp(decay_total[None] - inner_block_term), value_tile, precision=largest_value)
        return (updated_state, cross_block_term + intra_term)
    final_state, outputs = lax.scan(advance, carried, (split_blocks(queries), split_blocks(key_matrix), split_blocks(values), split_blocks(decay_logarithm)))
    return (outputs.reshape((length,) + outputs.shape[2:]), final_state)

def gate_factors(forget_gate, spike_amount, gate_floor):
    decay_logarithm = jnp.logaddexp(jnp.log(gate_floor), jnp.log1p(-gate_floor) + jax.nn.log_sigmoid(forget_gate)) + spike_amount[:, :, None]
    key_matrix = (1.0 - gate_floor) * jax.nn.sigmoid(-forget_gate)
    return (key_matrix, decay_logarithm)

def head_norm(outputs, gain):
    return outputs * lax.rsqrt(lax.optimization_barrier(jnp.mean(outputs * outputs, axis=-1, keepdims=True)) + norm_eps) * gain

def recurrence_path(query_rows, forget_input, value_input, spike_amount, forget_floor, recurrent_norm_gain):
    length = query_rows.shape[0]
    queries = query_rows.astype(jnp.float32).reshape(length, RECURRENT_HEADS, HG_DK)
    forget_gate = forget_input.astype(jnp.float32).reshape(length, RECURRENT_HEADS, HG_DK)
    values = value_input.astype(jnp.float32).reshape(length, RECURRENT_HEADS, HG_DV)
    summed = jnp.zeros((length, RECURRENT_HEADS, HG_DV), jnp.float32)
    for direction in range(2):
        gate_floor = forget_floor[direction].reshape(RECURRENT_HEADS, HG_DK)
        key_matrix, decay_logarithm = gate_factors(forget_gate, spike_amount, gate_floor)
        sorted_rows = [queries, key_matrix, values, decay_logarithm]
        if direction == 1:
            sorted_rows = [jnp.flip(member, axis=0) for member in sorted_rows]
        result, unused = block_pass(sorted_rows[0], sorted_rows[1], sorted_rows[2], sorted_rows[3], jnp.zeros((RECURRENT_HEADS, HG_DK, HG_DV), jnp.float32))
        if direction == 1:
            result = jnp.flip(result, axis=0)
        summed = summed + result
    normed = head_norm(summed, recurrent_norm_gain.reshape(RECURRENT_HEADS, HG_DV))
    return normed.astype(jnp.bfloat16).reshape(length, RECURRENT_HEADS * HG_DV)

def attention_branch(query_rows, latent, rotary_key, latent_norm_gain, latent_up_weight):
    length = query_rows.shape[0]
    latent_wide = latent.astype(jnp.float32)
    normed = (latent_wide * lax.rsqrt(lax.optimization_barrier(jnp.mean(latent_wide * latent_wide, axis=-1, keepdims=True)) + norm_eps) * latent_norm_gain).astype(jnp.bfloat16)
    expanded = jnp.dot(normed, latent_up_weight, preferred_element_type=jnp.float32).astype(jnp.bfloat16)
    expanded = expanded.reshape(length, MLA_HEADS, NOPE + VDIM)
    cos_table, sin_table = rope_tables(length, 0.0)
    rotated_key = rotate(rotary_key.astype(jnp.float32), cos_table, sin_table).astype(jnp.bfloat16)
    head_query = query_rows.reshape(length, MLA_HEADS, NOPE + ROPE)
    query_rope = rotate(head_query[..., NOPE:].astype(jnp.float32), cos_table[:, None], sin_table[:, None])
    query_all = jnp.concatenate([head_query[..., :NOPE], query_rope.astype(jnp.bfloat16)], axis=-1)
    keys_all = jnp.concatenate([expanded[..., :NOPE], jnp.broadcast_to(rotated_key[:, None, :], (length, MLA_HEADS, ROPE))], axis=-1)
    values = expanded[..., NOPE:].astype(jnp.float32)
    keys_wide = keys_all.astype(jnp.float32)
    score_scale = (NOPE + ROPE) ** (-0.5)
    rows_block = min(length, 512)

    def one_block(query_block):
        scores = jnp.einsum('qhd,khd->hqk', query_block.astype(jnp.float32), keys_wide) * score_scale
        row_peak = lax.optimization_barrier(jnp.max(scores, axis=-1))
        weights = jnp.exp(scores - row_peak[..., None])
        totals = lax.optimization_barrier(jnp.sum(weights, axis=-1))
        rounded = lax.optimization_barrier(weights.astype(jnp.bfloat16)).astype(jnp.float32)
        weighted = jnp.einsum('hqk,khv->qhv', rounded, values) / totals.T[:, :, None]
        return (weighted.astype(jnp.bfloat16).reshape(rows_block, MLA_HEADS * VDIM), (row_peak + jnp.log(totals)).T)
    outputs, log_weight = lax.map(one_block, query_all.reshape(length // rows_block, rows_block, MLA_HEADS, NOPE + ROPE))
    return (outputs.reshape(length, MLA_HEADS * VDIM), log_weight.reshape(length, MLA_HEADS))

def reference(recurrent_query, forget_logits, recurrent_value, forget_floor, extra_log_decay, recurrent_norm_gain, attention_query, latent, rotary_key, latent_norm_gain, latent_up_weight, recurrent_output_weight, attention_output_weight):
    seq_count = SEQUENCE_GROUPS * (GROUP_TOKENS // SEQUENCE_LENGTH)

    def sequence_view(tensor):
        return tensor.reshape(seq_count, SEQUENCE_LENGTH, tensor.shape[-1])
    recurrence_result = lax.map(lambda input_tuple: recurrence_path(input_tuple[0], input_tuple[1], input_tuple[2], input_tuple[3], forget_floor, recurrent_norm_gain), (sequence_view(recurrent_query), sequence_view(forget_logits), sequence_view(recurrent_value), sequence_view(extra_log_decay)))
    attended, log_weight = lax.map(lambda input_tuple: attention_branch(input_tuple[0], input_tuple[1], input_tuple[2], latent_norm_gain, latent_up_weight), (sequence_view(attention_query), sequence_view(latent), sequence_view(rotary_key)))
    rows_total = SEQUENCE_GROUPS * GROUP_TOKENS
    recurrence_result = recurrence_result.reshape(rows_total, HG_WIDTH)
    attended = attended.reshape(rows_total, MLA_WIDTH)
    hg_share = HG_WIDTH // N_TP
    att_share = MLA_WIDTH // N_TP
    summed = jnp.zeros((rows_total, D), jnp.float32)
    for tp_half in range(N_TP):
        partial_term = jnp.dot(recurrence_result[:, tp_half * hg_share:(tp_half + 1) * hg_share], recurrent_output_weight[tp_half * hg_share:(tp_half + 1) * hg_share], preferred_element_type=jnp.float32)
        partial_term = partial_term + jnp.dot(attended[:, tp_half * att_share:(tp_half + 1) * att_share], attention_output_weight[tp_half * att_share:(tp_half + 1) * att_share], preferred_element_type=jnp.float32)
        summed = summed + lax.optimization_barrier(partial_term.astype(jnp.bfloat16)).astype(jnp.float32)
    mixed = summed.astype(jnp.bfloat16).reshape(SEQUENCE_GROUPS, GROUP_TOKENS, D)
    return (mixed, log_weight.reshape(SEQUENCE_GROUPS, GROUP_TOKENS, MLA_HEADS))
```

```python
import functools

import jax
import jax.numpy as jnp
import numpy as np
from jax import lax
from jax.experimental import pallas as pl
from jax.experimental.pallas import tpu as pltpu
from jax.sharding import PartitionSpec as P

HG_DK = 128
NOPE = 64
ROPE = 32
VDIM = 64
HEAD = NOPE + ROPE
LANES = 128
BLOCK = 128

norm_eps = 1e-06
rope_base = 10000.0
widest_span = 8

F32 = jnp.float32
BF16 = jnp.bfloat16


def mm(a, b):
    return jnp.dot(a, b, preferred_element_type=F32)


def mm_nt(a, b):
    return lax.dot_general(a, b, (((1,), (1,)), ((), ())), preferred_element_type=F32)


def mm_tn(a, b):
    return lax.dot_general(a, b, (((0,), (0,)), ((), ())), preferred_element_type=F32)


def flip_bits(value, mask):
    bit = 1
    while bit <= mask:
        if mask & bit:
            value = value + bit - 2 * bit * lax.rem(value // bit, 2)
        bit *= 2
    return value


def rope_constants(seq_len, heads):
    half = ROPE // 2
    inverse = (np.float32(rope_base) ** (-np.arange(half, dtype=np.float32) / np.float32(half))).astype(np.float32)
    angles = np.arange(seq_len, dtype=np.float32)[:, None] * inverse[None, :]
    cos_pad = np.zeros((seq_len, LANES), np.float32)
    sin_pad = np.zeros((seq_len, LANES), np.float32)
    cos_pad[:, :NOPE] = 1.0
    cos_pad[:, NOPE:HEAD] = np.tile(np.cos(angles), (1, 2))
    sin_pad[:, NOPE:HEAD] = np.tile(np.sin(angles), (1, 2))
    turns = np.concatenate([np.cos(angles).T, np.sin(angles).T], axis=0)
    place = np.zeros((heads * HEAD, heads * LANES), np.float32)
    swap = np.zeros((heads * HEAD, heads * LANES), np.float32)
    for h in range(heads):
        for i in range(HEAD):
            place[h * HEAD + i, h * LANES + i] = 1.0
        for i in range(half):
            a, b = NOPE + i, NOPE + half + i
            swap[h * HEAD + b, h * LANES + a] = -1.0
            swap[h * HEAD + a, h * LANES + b] = 1.0
    return cos_pad, sin_pad, turns, place, swap


def transfer_plan(n_fs, span, groups, cuts):
    count = groups * cuts
    paired = span % 2 == 0
    if n_fs == 4 and paired:
        direct = count - count // 3
        lists = {1: list(range(direct)), 2: list(range(count - 1, count - 1 - direct, -1))}
        half = count // 2
        cross = [(1, v) for v in range(half)], [(2, v) for v in range(count - 1, half - 1, -1)]
        over = [(1, v) for v in range(count - direct)], [(2, v) for v in range(count - 1, direct - 1, -1)]
        steps = []
        for k in range(half):
            step = [(cross[0][k], "cross"), (cross[1][k], "cross")]
            if k < len(over[0]):
                step += [(over[0][k], "pair"), (over[1][k], "pair")]
            steps.append(step)
        when = {}
        for k in range(direct):
            when[1, lists[1][k]] = when[2, lists[2][k]] = k + 1
        for k in range(half):
            when[3, cross[0][k][1]] = when[3, cross[1][k][1]] = direct + k + 1
        for k in range(count - direct):
            when[1, count - 1 - over[0][k][1]] = 5 + 2 * k
            when[2, count - 1 - over[1][k][1]] = 6 + 2 * k
    else:
        lists = {j: list(range(count)) for j in range(1, n_fs)}
        steps = []
        when = {(j, v): v * n_fs + j for j in lists for v in lists[j]}
    order = [(0, g) for g in range(groups)]
    rest = [(max(when[j, g * cuts + b] for b in range(cuts)), j, g) for j in range(1, n_fs) for g in range(groups)]
    order += [(j, g) for _, j, g in sorted(rest)]
    return lists, steps, order


def kernel(
    sizes,
    q_hbm, f_hbm, v_hbm, floor_hbm, extra_hbm, gain_hbm, aq_hbm, lat_hbm, rk_hbm,
    lgain_hbm, wup_hbm, cos_hbm, sin_hbm, turn_hbm, place_hbm, swap_hbm, w1_hbm, w2_hbm,
    out_hbm, logw_hbm,
    q_ref, f_ref, v_ref, floor_ref, extra_ref, gain_ref, aq_ref, lat_ref, rk_ref,
    lgain_ref, wup_ref, cos_ref, sin_ref, turn_ref, place_ref, swap_ref,
    lbuf, ssend, srecv, wbuf, psend, precv, out_ref, logw_ref,
    kbuf, vbuf, intra, qf_ref, qb_ref, sf_ref, sb_ref, act, whole_state, whole_decay,
    in_sem, own_sem, l_send, l_recv, f_send, f_recv, s_send, s_recv, w_send, w_recv, z_send,
    x_send, x_recv, o_sem,
):
    n_fs, span = sizes
    tokens, width = q_ref.shape
    heads = width // HG_DK
    att_heads = aq_ref.shape[1] // HEAD
    up = att_heads * (NOPE + VDIM)
    blocks = tokens // BLOCK
    latent_width = lat_ref.shape[1]
    columns = w1_hbm.shape[1]
    cut_rows = w2_hbm.shape[0]
    cuts = w1_hbm.shape[0] // cut_rows + 1
    groups = columns // LANES
    rows = tokens // 2
    half_rope = ROPE // 2

    sp, fs, tp = lax.axis_index("sp"), lax.axis_index("fs"), lax.axis_index("tp")
    place = lax.rem(sp, span)
    base = sp - place
    parity = lax.rem(place, 2)
    has_left, has_right = place > 0, place < span - 1
    left = {"sp": base + jnp.maximum(place - 1, 0)}
    right = {"sp": base + jnp.minimum(place + 1, span - 1)}
    pair = {"sp": base + flip_bits(place, 1)}
    partner = {"tp": 1 - tp}
    mesh_id = pl.DeviceIdType.MESH

    def fs_peer(j):
        return {"fs": flip_bits(fs, j)}

    direct, steps, order = transfer_plan(n_fs, span, groups, cuts)

    def at_chunk(v):
        g, b = divmod(v, cuts)
        return g + parity * (groups - 1 - 2 * g), b + parity * (cuts - 1 - 2 * b)

    def chunk(j, v):
        g, b = at_chunk(v)
        return wbuf.at[j, g, pl.ds(pl.multiple_of(b * cut_rows, cut_rows), cut_rows), :]

    def chunk_sem(sems, j, v):
        g, b = at_chunk(v)
        return sems.at[j, g * cuts + b]

    def fetch(k, src, dst):
        return pltpu.make_async_copy(src, dst, in_sem.at[k])

    own = []
    for g in range(groups):
        cols = pl.ds(g * LANES, LANES)
        for k, (src, at) in enumerate(((w1_hbm, 0), (w2_hbm, w1_hbm.shape[0]))):
            own.append(pltpu.make_async_copy(
                src.at[:, cols], wbuf.at[0, g, pl.ds(at, src.shape[0]), :], own_sem.at[2 * g + k]))
    for c in own:
        c.start()
    my_tokens = pl.ds(pl.multiple_of(place * tokens, tokens), tokens)
    tp_up = pl.ds(pl.multiple_of(tp * up, LANES), up)
    early = [
        fetch(0, lat_hbm, lat_ref), fetch(1, rk_hbm, rk_ref), fetch(2, lgain_hbm, lgain_ref),
        fetch(3, turn_hbm.at[:, my_tokens], turn_ref),
    ]
    gates = [
        fetch(4, f_hbm, f_ref), fetch(5, q_hbm, q_ref), fetch(6, v_hbm, v_ref),
        fetch(7, floor_hbm, floor_ref), fetch(8, extra_hbm, extra_ref),
    ]
    late = [
        fetch(9, gain_hbm, gain_ref), fetch(10, aq_hbm, aq_ref), fetch(11, wup_hbm.at[:, tp_up], wup_ref),
        fetch(12, cos_hbm.at[my_tokens, :], cos_ref), fetch(13, sin_hbm.at[my_tokens, :], sin_ref),
        fetch(14, place_hbm, place_ref), fetch(15, swap_hbm, swap_ref),
    ]
    for c in early + gates + late:
        c.start()

    barrier = pltpu.get_barrier_semaphore()
    for j in direct:
        pl.semaphore_signal(barrier, inc=1, device_id=fs_peer(j), device_id_type=mesh_id)
    pl.semaphore_signal(barrier, inc=1, device_id=partner, device_id_type=mesh_id)

    @pl.when(has_left)
    def _():
        pl.semaphore_signal(barrier, inc=1, device_id=left, device_id_type=mesh_id)

    @pl.when(has_right)
    def _():
        pl.semaphore_signal(barrier, inc=1, device_id=right, device_id_type=mesh_id)

    for c in own:
        c.wait()
    pl.semaphore_wait(barrier, len(direct) + 1 + has_left.astype(jnp.int32) + has_right.astype(jnp.int32))

    def remote(src, dst, send, recv, device):
        return pltpu.make_async_remote_copy(
            src_ref=src, dst_ref=dst, send_sem=send, recv_sem=recv,
            device_id=device, device_id_type=mesh_id,
        )

    sent = []

    def send(c):
        c.start()
        sent.append(c)

    for k in range(max((len(direct[j]) for j in direct), default=0)):
        for j in direct:
            if k < len(direct[j]):
                v = direct[j][k]
                send(remote(chunk(0, v), chunk(j, v), chunk_sem(w_send, j, v), chunk_sem(w_recv, j, v), fs_peer(j)))

    arrived = set()

    def await_chunk(j, v):
        if (j, v) not in arrived:
            arrived.add((j, v))
            remote(chunk(j, v), chunk(j, v), chunk_sem(w_send, j, v), chunk_sem(w_recv, j, v), fs_peer(j)).wait_recv()

    def relay_step(k):
        if k >= len(steps):
            return
        for (j, v), kind in steps[k]:
            await_chunk(j, v)
            if kind == "cross":
                send(remote(chunk(j, v), chunk(3, v), chunk_sem(w_send, 3, v), chunk_sem(w_recv, 3, v), fs_peer(3 - j)))
            else:
                send(remote(chunk(j, v), chunk(j, v), chunk_sem(z_send, j, v), chunk_sem(w_recv, j, v), pair))

    for c in early:
        c.wait()
    lat = lat_ref[...].astype(F32)
    normed = lat * lax.rsqrt(jnp.mean(lat * lat, axis=-1, keepdims=True) + norm_eps) * lgain_ref[...]
    normed = normed.astype(BF16)
    rope_a, rope_b = rk_ref[:half_rope, :].astype(F32), rk_ref[half_rope:, :].astype(F32)
    turn_c, turn_s = turn_ref[:half_rope, :], turn_ref[half_rope:, :]
    turned_a = (rope_a * turn_c - rope_b * turn_s).astype(BF16)
    turned_b = (rope_a * turn_s + rope_b * turn_c).astype(BF16)
    for t in range(2):
        part = slice(t * rows, (t + 1) * rows)
        lbuf[place, t, :rows, :] = normed[part]
        lbuf[place, t, rows:, :rows] = turned_a[:, part]
        lbuf[place, t, rows:, rows:] = turned_b[:, part]

    def along(d, at):
        return remote(lbuf.at[at, tp], lbuf.at[at, tp], l_send.at[d, at], l_recv.at[at], right if d == 0 else left)

    def across(at):
        return remote(lbuf.at[at, tp], lbuf.at[at, tp], f_send.at[at], f_recv.at[at], partner)

    @pl.when(has_right)
    def _():
        along(0, place).start()

    @pl.when(has_left)
    def _():
        along(1, place).start()

    def latent_round(r):
        for d in range(2):
            at = place - r if d == 0 else place + r
            there = at >= 0 if d == 0 else at < span
            at = jnp.clip(at, 0, span - 1)

            @pl.when(there)
            def _():
                along(d, at).wait_recv()
                across(at).start()

            if r < span - 1:
                @pl.when(jnp.logical_and(there, has_right if d == 0 else has_left))
                def _():
                    along(d, at).start()

    row = lax.broadcasted_iota(jnp.int32, (BLOCK, BLOCK), 0)
    col = lax.broadcasted_iota(jnp.int32, (BLOCK, BLOCK), 1)
    lower = row >= col
    upper = row <= col
    tri = (jnp.where(lower, 1.0, 0.0).astype(BF16), jnp.where(upper, 1.0, 0.0).astype(BF16))
    for c in gates:
        c.wait()
    spikes = lax.dot_general(
        extra_ref[...],
        jnp.where(
            lax.broadcasted_iota(jnp.int32, (heads, width), 0)
            == lax.broadcasted_iota(jnp.int32, (heads, width), 1) // HG_DK, 1.0, 0.0),
        (((0,), (0,)), ((), ())), precision=lax.Precision.HIGHEST, preferred_element_type=F32)
    block_decay = [[[None] * blocks for _ in range(2)] for _ in range(heads)]
    for h in range(heads):
        lanes = slice(h * HG_DK, (h + 1) * HG_DK)
        for b in range(blocks):
            tok = slice(b * BLOCK, (b + 1) * BLOCK)
            q = q_ref[tok, lanes].astype(F32)
            gate = f_ref[tok, lanes].astype(F32)
            v = v_ref[tok, lanes]
            miss = 1.0 / (1.0 + jnp.exp(gate))
            spike = spikes[tok, lanes]
            scores = None
            for d in range(2):
                keyed = (1.0 - floor_ref[d : d + 1, lanes]) * miss
                decay = jnp.log1p(-keyed) + spike
                hi = decay.astype(BF16)
                lo = (decay - hi.astype(F32)).astype(BF16)
                run = mm(tri[d], hi) + mm(tri[d], lo)
                mid_at = BLOCK // 2 - 1 if d == 0 else BLOCK // 2
                end_at = BLOCK - 1 if d == 0 else 0
                mid = run[mid_at : mid_at + 1]
                end = run[end_at : end_at + 1]
                grow = jnp.exp(run - mid)
                qd = q * grow
                kd = keyed * jnp.exp(mid - run)
                s = mm_nt(qd.astype(BF16), kd.astype(BF16))
                s = jnp.where(lower if d == 0 else upper, s, 0.0)
                scores = s if scores is None else scores + s
                cross = qf_ref if d == 0 else qb_ref
                cross[tok, lanes] = (qd * jnp.exp(mid)).astype(BF16)
                state = mm_tn(v, (kd * jnp.exp(end - mid)).astype(BF16))
                keep = sf_ref if d == 0 else sb_ref
                keep[b, :, lanes] = state
                block_decay[h][d][b] = jnp.exp(end)
            intra[tok, lanes] = mm(scores.astype(BF16), v)
        for d in range(2):
            keep = sf_ref if d == 0 else sb_ref
            going = range(blocks) if d == 0 else range(blocks - 1, -1, -1)
            total, decay_all = None, None
            for b in going:
                one = keep[b, :, lanes]
                dec = block_decay[h][d][b]
                total = one if total is None else total * dec + one
                decay_all = dec if decay_all is None else decay_all * dec
            whole_state[d, h] = total
            whole_decay[d, h] = jnp.broadcast_to(decay_all, (8, HG_DK))

    first = jnp.where(2 * place < span, 0, 1)

    def link(d, h):
        towards = jnp.clip(place + 1 - 2 * d, 0, span - 1)
        return remote(ssend.at[d, h], srecv.at[d, h], s_send.at[d, h], s_recv.at[d, h],
                      {"sp": base + towards})

    def has_previous(d):
        return jnp.where(d == 0, place, span - 1 - place) > 0

    def has_next(d):
        return jnp.where(d == 0, span - 1 - place, place) > 0

    def pass_on(d):
        for h in range(heads):
            @pl.when(has_previous(d))
            def _():
                link(d, h).wait_recv()

            @pl.when(jnp.logical_not(has_previous(d)))
            def _():
                srecv[d, h] = jnp.zeros((HG_DK, HG_DK), BF16)

            @pl.when(has_next(d))
            def _():
                reached = srecv[d, h].astype(F32) * whole_decay[d, h, 0:1] + whole_state[d, h]
                ssend[d, h] = reached.astype(BF16)
                link(d, h).start()

    @pl.when(jnp.logical_not(has_previous(first)))
    def _():
        pass_on(first)

    if span > 1:
        latent_round(1)
    relay_step(0)
    relay_step(1)

    @pl.when(has_previous(first))
    def _():
        pass_on(first)

    for r in range(2, span):
        latent_round(r)
        if r == 2:
            relay_step(2)

    @pl.when(has_next(1 - first))
    def _():
        pass_on(1 - first)

    for k in range(2, len(steps) - 2):
        if k > 2 or span < 3:
            relay_step(k)

    for c in late:
        c.wait()
    wup = wup_ref[...]
    lane = lax.broadcasted_iota(jnp.int32, (rows, LANES), 1)
    put_a = place_ref[NOPE : NOPE + half_rope, :LANES]
    put_b = place_ref[NOPE + half_rope : HEAD, :LANES]
    for j in range(span):
        at = flip_bits(place, j)
        if j > 0:
            across(at).wait_recv()
        for t in range(2):
            keys = slice((2 * j + t) * rows, (2 * j + t + 1) * rows)
            expanded = mm(lbuf[at, t, :rows, :], wup)
            rot = mm_tn(lbuf[at, t, rows:, :rows], put_a) + mm_tn(lbuf[at, t, rows:, rows:], put_b)
            vbuf[keys, :] = expanded.astype(BF16)
            for h in range(att_heads):
                lanes = slice(h * LANES, (h + 1) * LANES)
                kbuf[keys, lanes] = jnp.where(lane < NOPE, expanded[:, lanes], rot).astype(BF16)

    def act_slot(t):
        return t + tp * (1 - 2 * t)

    aq = aq_ref[...]
    cos, sin = cos_ref[...], sin_ref[...]
    scale = HEAD ** (-0.5)
    lane = lax.broadcasted_iota(jnp.int32, (tokens, LANES), 1)
    logw = jnp.zeros((tokens, LANES), F32)
    kept = None
    left_steps = list(range(max(len(steps) - 2, 2), len(steps)))
    for h in range(att_heads):
        lanes = slice(h * LANES, (h + 1) * LANES)
        query = mm(aq, place_ref[:, lanes]) * cos + mm(aq, swap_ref[:, lanes]) * sin
        scores = mm_nt(query.astype(BF16), kbuf[:, lanes]) * scale
        peak = jnp.max(scores, axis=-1, keepdims=True)
        weights = jnp.exp(scores - peak)
        totals = jnp.sum(weights, axis=-1, keepdims=True)
        result = mm(weights.astype(BF16), vbuf[:, lanes]) / totals
        logw = jnp.where(lane == h, peak + jnp.log(totals), logw)
        if h % 2 == 0:
            kept = pltpu.roll(result, VDIM, 1)
        else:
            at = width + (h // 2) * LANES
            joined = jnp.where(lane < VDIM, kept, result).astype(BF16)
            for t in range(2):
                act[act_slot(t), :, at : at + LANES] = joined[t * rows : (t + 1) * rows]
            if left_steps:
                relay_step(left_steps.pop(0))
    for k in left_steps:
        relay_step(k)
    logw_ref[...] = jnp.transpose(logw)[:att_heads]
    logw_copy = pltpu.make_async_copy(logw_ref, logw_hbm, o_sem.at[n_fs * groups])
    logw_copy.start()

    @pl.when(jnp.logical_not(has_next(1 - first)))
    def _():
        pass_on(1 - first)

    for h in range(heads):
        lanes = slice(h * HG_DK, (h + 1) * HG_DK)
        carry_f = srecv[0, h].astype(F32)
        carry_b = srecv[1, h].astype(F32)
        starts_f = []
        for b in range(blocks):
            starts_f.append(carry_f)
            carry_f = carry_f * block_decay[h][0][b] + sf_ref[b, :, lanes]
        starts_b = [None] * blocks
        for b in range(blocks - 1, -1, -1):
            starts_b[b] = carry_b
            carry_b = carry_b * block_decay[h][1][b] + sb_ref[b, :, lanes]
        for b in range(blocks):
            tok = slice(b * BLOCK, (b + 1) * BLOCK)
            t, off = divmod(b * BLOCK, rows)
            o = intra[tok, lanes]
            o = o + mm_nt(qf_ref[tok, lanes], starts_f[b].astype(BF16))
            o = o + mm_nt(qb_ref[tok, lanes], starts_b[b].astype(BF16))
            o = o * lax.rsqrt(jnp.mean(o * o, axis=-1, keepdims=True) + norm_eps) * gain_ref[:, lanes]
            act[act_slot(t), off : off + BLOCK, lanes] = o.astype(BF16)

    x_copies, out_copies = [], []

    def finish(i):
        j, g = order[i]
        x_copies[i].wait_recv()
        out_ref[i] = (out_ref[i].astype(F32) + precv[i].astype(F32)).astype(BF16)
        at = flip_bits(fs, j) * columns + (g + parity * (groups - 1 - 2 * g)) * LANES
        c = pltpu.make_async_copy(out_ref.at[i], out_hbm.at[:, pl.ds(pl.multiple_of(at, LANES), LANES)], o_sem.at[i])
        c.start()
        out_copies.append(c)

    behind = 2
    for i, (j, g) in enumerate(order):
        if j > 0:
            for b in range(cuts):
                await_chunk(j, g * cuts + b)
        weight = wbuf[j, g + parity * (groups - 1 - 2 * g)]
        away = mm(act[1], weight)
        psend[i] = away.astype(BF16)
        c = remote(psend.at[i], precv.at[i], x_send.at[i], x_recv.at[i], partner)
        c.start()
        x_copies.append(c)
        out_ref[i] = mm(act[0], weight).astype(BF16)
        if i >= behind:
            finish(i - behind)
    for i in range(max(len(order) - behind, 0), len(order)):
        finish(i)

    for c in sent + x_copies:
        c.wait_send()

    @pl.when(has_right)
    def _():
        along(0, place).wait_send()

    @pl.when(has_left)
    def _():
        along(1, place).wait_send()

    for r in range(1, span):
        for d in range(2):
            at = place - r if d == 0 else place + r
            there = at >= 0 if d == 0 else at < span
            at = jnp.clip(at, 0, span - 1)

            @pl.when(there)
            def _():
                across(at).wait_send()

            if r < span - 1:
                @pl.when(jnp.logical_and(there, has_right if d == 0 else has_left))
                def _():
                    along(d, at).wait_send()

    for d in range(2):
        for h in range(heads):
            @pl.when(has_next(d))
            def _():
                link(d, h).wait_send()

    for c in out_copies + [logw_copy]:
        c.wait()


def local(
    n_fs,
    n_sp,
    recurrent_query,
    forget_logits,
    recurrent_value,
    forget_floor,
    extra_log_decay,
    recurrent_norm_gain,
    attention_query,
    latent,
    rotary_key,
    latent_norm_gain,
    latent_up_weight,
    recurrent_output_weight,
    attention_output_weight,
):
    span = min(n_sp, widest_span)
    tokens, width = recurrent_query.shape[1:]
    heads = width // HG_DK
    att_heads = attention_query.shape[2] // HEAD
    latent_width = latent.shape[2]
    columns = recurrent_output_weight.shape[1]
    att_width = attention_output_weight.shape[0]
    up = att_heads * (NOPE + VDIM)
    blocks = tokens // BLOCK
    rows = tokens // 2
    groups = columns // LANES
    pieces = groups * n_fs
    chunks = groups * (width // att_width + 1)
    cos_pad, sin_pad, turns, place, swap = rope_constants(span * tokens, att_heads)
    anywhere = pl.BlockSpec(memory_space=pl.ANY)
    dma = pltpu.SemaphoreType.DMA
    vmem = pltpu.VMEM
    mixed, log_weight = pl.pallas_call(
        functools.partial(kernel, (n_fs, span)),
        out_shape=(
            jax.ShapeDtypeStruct((rows, columns * n_fs), BF16),
            jax.ShapeDtypeStruct((att_heads, tokens), F32),
        ),
        in_specs=[anywhere] * 18,
        out_specs=(anywhere, anywhere),
        scratch_shapes=[
            vmem((tokens, width), BF16), vmem((tokens, width), BF16), vmem((tokens, width), BF16),
            vmem((2, width), F32), vmem((heads, tokens), F32), vmem((1, width), F32),
            vmem((tokens, att_heads * HEAD), BF16), vmem((tokens, latent_width), BF16), vmem((ROPE, tokens), BF16),
            vmem((1, latent_width), F32), vmem((latent_width, up), BF16),
            vmem((tokens, LANES), F32), vmem((tokens, LANES), F32), vmem((ROPE, tokens), F32),
            vmem((att_heads * HEAD, att_heads * LANES), BF16), vmem((att_heads * HEAD, att_heads * LANES), BF16),
            vmem((span, 2, rows + ROPE // 2, latent_width), BF16),
            vmem((2, heads, HG_DK, HG_DK), BF16),
            vmem((2, heads, HG_DK, HG_DK), BF16),
            vmem((n_fs, groups, width + att_width, LANES), BF16),
            vmem((pieces, rows, LANES), BF16),
            vmem((pieces, rows, LANES), BF16),
            vmem((pieces, rows, LANES), BF16),
            vmem((att_heads, tokens), F32),
            vmem((span * tokens, att_heads * LANES), BF16),
            vmem((span * tokens, att_heads * LANES), BF16),
            vmem((tokens, width), F32),
            vmem((tokens, width), BF16),
            vmem((tokens, width), BF16),
            vmem((blocks, HG_DK, width), F32),
            vmem((blocks, HG_DK, width), F32),
            vmem((2, rows, width + att_width), BF16),
            vmem((2, heads, HG_DK, HG_DK), F32),
            vmem((2, heads, 8, HG_DK), F32),
            dma((16,)), dma((2 * groups,)), dma((2, span)), dma((span,)), dma((span,)), dma((span,)),
            dma((2, heads)), dma((2, heads)),
            dma((n_fs, chunks)), dma((n_fs, chunks)), dma((n_fs, chunks)),
            dma((pieces,)), dma((pieces,)), dma((pieces + 1,)),
        ],
        compiler_params=pltpu.CompilerParams(
            collective_id=0, has_side_effects=True, vmem_limit_bytes=56 * 2**20
        ),
        name="mixers",
    )(
        recurrent_query[0],
        forget_logits[0],
        recurrent_value[0],
        forget_floor,
        extra_log_decay[0].T,
        recurrent_norm_gain[None],
        attention_query[0],
        latent[0],
        rotary_key[0].T,
        latent_norm_gain[None],
        latent_up_weight,
        jnp.asarray(cos_pad),
        jnp.asarray(sin_pad),
        jnp.asarray(turns),
        jnp.asarray(place, BF16),
        jnp.asarray(swap, BF16),
        recurrent_output_weight,
        attention_output_weight,
    )
    return mixed[None], log_weight.T[None]


def solution(mesh):
    placed = (
        P("fs", "sp", "tp"),
        P("fs", "sp", "tp"),
        P("fs", "sp", "tp"),
        P(None, "tp"),
        P("fs", "sp", "tp"),
        P("tp"),
        P("fs", "sp", "tp"),
        P("fs", "sp", None),
        P("fs", "sp", None),
        P(),
        P(),
        P("tp", "fs"),
        P("tp", "fs"),
    )
    return jax.shard_map(
        functools.partial(local, mesh.shape["fs"], mesh.shape["sp"]),
        mesh=mesh,
        in_specs=placed,
        out_specs=(P("fs", ("sp", "tp"), None), P("fs", "sp", "tp")),
        check_vma=False,
    )
```

```python
import functools

import jax
import jax.numpy as jnp
import numpy as np
from jax import lax
from jax.experimental import pallas as pl
from jax.experimental.pallas import tpu as pltpu
from jax.sharding import PartitionSpec as P

HG_DK = 128
NOPE = 64
ROPE = 32
VDIM = 64
HEAD = NOPE + ROPE
LANES = 128
BLOCK = 128

norm_eps = 1e-06
rope_base = 10000.0
widest_span = 8

F32 = jnp.float32
BF16 = jnp.bfloat16


def mm(a, b):
    return jnp.dot(a, b, preferred_element_type=F32)


def mm_nt(a, b):
    return lax.dot_general(a, b, (((1,), (1,)), ((), ())), preferred_element_type=F32)


def mm_tn(a, b):
    return lax.dot_general(a, b, (((0,), (0,)), ((), ())), preferred_element_type=F32)


def flip_bits(value, mask):
    bit = 1
    while bit <= mask:
        if mask & bit:
            value = value + bit - 2 * bit * lax.rem(value // bit, 2)
        bit *= 2
    return value


def window_start(h, heads):
    return min(h * HEAD // LANES * LANES, max(heads * HEAD - 2 * LANES, 0))


def rope_constants(seq_len, heads):
    half = ROPE // 2
    inverse = (np.float32(rope_base) ** (-np.arange(half, dtype=np.float32) / np.float32(half))).astype(np.float32)
    angles = np.arange(seq_len, dtype=np.float32)[:, None] * inverse[None, :]
    cos_pad = np.zeros((seq_len, LANES), np.float32)
    sin_pad = np.zeros((seq_len, LANES), np.float32)
    cos_pad[:, :NOPE] = 1.0
    cos_pad[:, NOPE:HEAD] = np.tile(np.cos(angles), (1, 2))
    sin_pad[:, NOPE:HEAD] = np.tile(np.sin(angles), (1, 2))
    turns = np.concatenate([np.cos(angles).T, np.sin(angles).T], axis=0)
    window = min(2 * LANES, heads * HEAD)
    spread = np.zeros((heads, window, 2 * LANES), np.float32)
    for h in range(heads):
        off = h * HEAD - window_start(h, heads)
        for i in range(HEAD):
            spread[h, off + i, i] = 1.0
        for i in range(half):
            a, b = NOPE + i, NOPE + half + i
            spread[h, off + b, LANES + a] = -1.0
            spread[h, off + a, LANES + b] = 1.0
    return cos_pad, sin_pad, turns, spread


def transfer_plan(n_fs, span, groups, cuts):
    count = groups * cuts
    paired = span % 2 == 0
    if n_fs == 4 and paired:
        direct = count - count // 3
        lists = {1: list(range(direct)), 2: list(range(count - 1, count - 1 - direct, -1))}
        half = count // 2
        cross = [(1, v) for v in range(half)], [(2, v) for v in range(count - 1, half - 1, -1)]
        over = [(1, v) for v in range(count - direct)], [(2, v) for v in range(count - 1, direct - 1, -1)]
        crosses = [[c[k] for c in cross] for k in range(half)]
        pairs = [c[k] for k in range(count - direct) for c in over]
        when = {}
        for k in range(direct):
            when[1, lists[1][k]] = when[2, lists[2][k]] = k + 1
        for k in range(half):
            when[3, cross[0][k][1]] = when[3, cross[1][k][1]] = direct + k + 1
        for k in range(count - direct):
            when[1, count - 1 - over[0][k][1]] = 5 + 2 * k
            when[2, count - 1 - over[1][k][1]] = 6 + 2 * k
    else:
        lists = {j: list(range(count)) for j in range(1, n_fs)}
        crosses, pairs = [], []
        when = {(j, v): v * n_fs + j for j in lists for v in lists[j]}
    last = {(j, g): max(when[j, g * cuts + b] for b in range(cuts)) for j in range(1, n_fs) for g in range(groups)}
    order = [(0, g) for g in range(groups)] + sorted(last, key=lambda one: (last[one], one))
    bounds = [0, len(order) // 2, 3 * len(order) // 4, len(order)]
    batches = []
    for lo, hi in zip(bounds, bounds[1:]):
        batch = []
        for j, g in sorted(order[lo:hi]):
            if batch and batch[-1][0] == j and batch[-1][1] + batch[-1][2] == g and batch[-1][2] == 1:
                batch[-1] = (j, batch[-1][1], 2)
            else:
                batch.append((j, g, 1))
        batches.append(batch)
    return lists, crosses, pairs, batches


def kernel(
    sizes,
    q_hbm, f_hbm, v_hbm, floor_hbm, extra_hbm, gain_hbm, aq_hbm, lat_hbm, rk_hbm,
    lgain_hbm, wup_hbm, cos_hbm, sin_hbm, turn_hbm, spread_hbm, w1_hbm, w2_hbm,
    out_ref, logw_ref,
    q_ref, f_ref, v_ref, floor_ref, extra_ref, gain_ref, aq_ref, lat_ref, rk_ref,
    lgain_ref, wup_ref, cos_ref, sin_ref, turn_ref, spread_ref,
    lbuf, ssend, srecv, wbuf, psend, precv, keep,
    kbuf, vbuf, intra, qd_ref, kd_ref, qc_ref, st_ref, act, whole_state, whole_decay,
    in_sem, own_sem, l_send, l_recv, f_send, f_recv, s_send, s_recv, w_send, w_recv,
    x_send, x_recv,
):
    n_fs, span = sizes
    tokens, width = q_ref.shape
    heads = width // HG_DK
    att_heads = aq_ref.shape[1] // HEAD
    up = att_heads * (NOPE + VDIM)
    blocks = tokens // BLOCK
    latent_width = lat_ref.shape[1]
    columns = w1_hbm.shape[1]
    cut_rows = w2_hbm.shape[0]
    cuts = w1_hbm.shape[0] // cut_rows + 1
    groups = columns // LANES
    rows = tokens // 2
    half_rope = ROPE // 2

    sp, fs, tp = lax.axis_index("sp"), lax.axis_index("fs"), lax.axis_index("tp")
    place = lax.rem(sp, span)
    base = sp - place
    parity = lax.rem(place, 2)
    has_left, has_right = place > 0, place < span - 1
    left = {"sp": base + jnp.maximum(place - 1, 0)}
    right = {"sp": base + jnp.minimum(place + 1, span - 1)}
    pair = {"sp": base + flip_bits(place, 1)}
    partner = {"tp": 1 - tp}
    mesh_id = pl.DeviceIdType.MESH

    def fs_peer(j):
        return {"fs": flip_bits(fs, j)}

    direct, crosses, pairs, batches = transfer_plan(n_fs, span, groups, cuts)

    def at_chunk(v):
        g, b = divmod(v, cuts)
        return g + parity * (groups - 1 - 2 * g), b + parity * (cuts - 1 - 2 * b)

    def chunk(j, v):
        g, b = at_chunk(v)
        return wbuf.at[j, pl.ds(pl.multiple_of(b * cut_rows, cut_rows), cut_rows),
                       pl.ds(pl.multiple_of(g * LANES, LANES), LANES)]

    relayed = set(pairs).union(*crosses)

    def alone(j, v):
        return any((j, v - v % cuts + b) in relayed for b in range(cuts))

    def arrival(j, v, seen):
        g, b = at_chunk(v)
        return w_recv.at[j - 1, g * cuts + (b if alone(j, seen) else 0)]

    def remote(src, dst, send, recv, device):
        return pltpu.make_async_remote_copy(
            src_ref=src, dst_ref=dst, send_sem=send, recv_sem=recv,
            device_id=device, device_id_type=mesh_id,
        )

    def fetch(k, src, dst):
        return pltpu.make_async_copy(src, dst, in_sem.at[k])

    own = [
        pltpu.make_async_copy(src, wbuf.at[0, pl.ds(at, src.shape[0]), :], own_sem.at[k])
        for k, (src, at) in enumerate(((w1_hbm, 0), (w2_hbm, w1_hbm.shape[0])))
    ]
    for c in own:
        c.start()
    my_tokens = pl.ds(pl.multiple_of(place * tokens, tokens), tokens)
    tp_up = pl.ds(pl.multiple_of(tp * up, LANES), up)
    early = [
        fetch(0, lat_hbm, lat_ref), fetch(1, rk_hbm, rk_ref), fetch(2, lgain_hbm, lgain_ref),
        fetch(3, turn_hbm.at[:, my_tokens], turn_ref),
    ]
    gates = [
        fetch(4, f_hbm, f_ref), fetch(5, q_hbm, q_ref), fetch(6, v_hbm, v_ref),
        fetch(7, floor_hbm, floor_ref), fetch(8, extra_hbm, extra_ref),
    ]
    late = [
        fetch(9, gain_hbm, gain_ref), fetch(10, aq_hbm, aq_ref), fetch(11, wup_hbm.at[:, tp_up], wup_ref),
        fetch(12, cos_hbm.at[my_tokens, :], cos_ref), fetch(13, sin_hbm.at[my_tokens, :], sin_ref),
        fetch(14, spread_hbm, spread_ref),
    ]
    for c in early + gates + late:
        c.start()

    barrier = pltpu.get_barrier_semaphore()
    for j in direct:
        pl.semaphore_signal(barrier, inc=1, device_id=fs_peer(j), device_id_type=mesh_id)
    pl.semaphore_signal(barrier, inc=1, device_id=partner, device_id_type=mesh_id)

    @pl.when(has_left)
    def _():
        pl.semaphore_signal(barrier, inc=1, device_id=left, device_id_type=mesh_id)

    @pl.when(has_right)
    def _():
        pl.semaphore_signal(barrier, inc=1, device_id=right, device_id_type=mesh_id)

    for c in early:
        c.wait()
    lat = lat_ref[...].astype(F32)
    normed = lat * lax.rsqrt(jnp.mean(lat * lat, axis=-1, keepdims=True) + norm_eps) * lgain_ref[...]
    normed = normed.astype(BF16)
    rope_a, rope_b = rk_ref[:half_rope, :].astype(F32), rk_ref[half_rope:, :].astype(F32)
    turn_c, turn_s = turn_ref[:half_rope, :], turn_ref[half_rope:, :]
    turned_a = (rope_a * turn_c - rope_b * turn_s).astype(BF16)
    turned_b = (rope_a * turn_s + rope_b * turn_c).astype(BF16)
    for t in range(2):
        part = slice(t * rows, (t + 1) * rows)
        lbuf[place, t, :rows, :] = normed[part]
        lbuf[place, t, rows:, :rows] = turned_a[:, part]
        lbuf[place, t, rows:, rows:] = turned_b[:, part]

    def source(d, r):
        at = place - r if d == 0 else place + r
        there = at >= 0 if d == 0 else at < span
        onward = jnp.logical_and(there, has_right if d == 0 else has_left)
        return jnp.clip(at, 0, span - 1), there, onward

    def along(d, at):
        return remote(lbuf.at[at, tp], lbuf.at[at, tp], l_send.at[d, at], l_recv.at[at], right if d == 0 else left)

    def across(at):
        return remote(lbuf.at[at, tp], lbuf.at[at, tp], f_send.at[at], f_recv.at[at], partner)

    def latent_round(r):
        for d in range(2):
            at, there, onward = source(d, r)
            if r > 0:
                @pl.when(there)
                def _():
                    along(d, at).wait_recv()
                    across(at).start()

            if r < span - 1:
                @pl.when(onward)
                def _():
                    along(d, at).start()

    for c in own:
        c.wait()
    pl.semaphore_wait(barrier, len(direct) + 1 + has_left.astype(jnp.int32) + has_right.astype(jnp.int32))
    latent_round(0)
    for k in range(max((len(direct[j]) for j in direct), default=0)):
        for j in direct:
            if k < len(direct[j]):
                v = direct[j][k]
                remote(chunk(0, v), chunk(j, v), w_send.at[0], arrival(j, v, v), fs_peer(j)).start()
    arrived = set()

    def await_chunk(j, v):
        if not alone(j, v):
            v -= v % cuts
        if (j, v) in arrived:
            return
        arrived.add((j, v))
        ref = chunk(j, v)
        if not alone(j, v):
            ref = wbuf.at[j, :, pl.ds(pl.multiple_of(at_chunk(v)[0] * LANES, LANES), LANES)]
        remote(ref, ref, w_send.at[0], arrival(j, v, v), partner).wait_recv()

    def relay_cross(*ks):
        for k in ks:
            for j, v in crosses[k] if k < len(crosses) else ():
                await_chunk(j, v)
                remote(chunk(j, v), chunk(3, v), w_send.at[0], arrival(3, v, v), fs_peer(3 - j)).start()

    def relay_pair(lo, hi):
        for j, v in pairs[lo:hi]:
            await_chunk(j, v)
            seen = groups * cuts - 1 - v
            remote(chunk(j, v), chunk(j, v), w_send.at[0], arrival(j, v, seen), pair).start()

    row = lax.broadcasted_iota(jnp.int32, (BLOCK, BLOCK), 0)
    col = lax.broadcasted_iota(jnp.int32, (BLOCK, BLOCK), 1)
    lower = row >= col
    upper = row <= col
    tri = (jnp.where(lower, 1.0, 0.0).astype(BF16), jnp.where(upper, 1.0, 0.0).astype(BF16))
    for c in gates:
        c.wait()
    spikes = lax.dot_general(
        extra_ref[...],
        jnp.where(
            lax.broadcasted_iota(jnp.int32, (heads, width), 0)
            == lax.broadcasted_iota(jnp.int32, (heads, width), 1) // HG_DK, 1.0, 0.0),
        (((0,), (0,)), ((), ())), precision=lax.Precision.HIGHEST, preferred_element_type=F32)
    first = jnp.where(2 * place < span, 0, 1)

    def link(d, h):
        towards = jnp.clip(place + 1 - 2 * d, 0, span - 1)
        return remote(ssend.at[d, h], srecv.at[d, h], s_send.at[d], s_recv.at[d, h],
                      {"sp": base + towards})

    def has_previous(d):
        return jnp.where(d == 0, place, span - 1 - place) > 0

    def has_next(d):
        return jnp.where(d == 0, span - 1 - place, place) > 0

    def pass_head(d, h):
        @pl.when(has_previous(d))
        def _():
            link(d, h).wait_recv()

        @pl.when(jnp.logical_not(has_previous(d)))
        def _():
            srecv[d, h] = jnp.zeros((HG_DK, HG_DK), BF16)

        @pl.when(has_next(d))
        def _():
            reached = srecv[d, h].astype(F32) * whole_decay[d, h, 0:1] + whole_state[d, h]
            ssend[d, h] = reached.astype(BF16)
            link(d, h).start()

    def pass_on(d):
        for h in range(heads):
            pass_head(d, h)

    twice = [jnp.concatenate([t, t], axis=1) for t in tri]
    block_decay = [[[None] * blocks for _ in range(2)] for _ in range(heads)]
    ahead = 2 if heads % 2 == 0 else 1
    for h0 in range(0, heads, ahead):
        wide_lanes = slice(h0 * HG_DK, (h0 + ahead) * HG_DK)
        for b in range(blocks):
            tok = slice(b * BLOCK, (b + 1) * BLOCK)
            q = q_ref[tok, wide_lanes].astype(F32)
            miss = 1.0 / (1.0 + jnp.exp(f_ref[tok, wide_lanes].astype(F32)))
            spike = spikes[tok, wide_lanes]
            ending = []
            for d in range(2):
                keyed = (1.0 - floor_ref[d : d + 1, wide_lanes]) * miss
                decay = jnp.log1p(-keyed) + spike
                hi = decay.astype(BF16)
                lo = (decay - hi.astype(F32)).astype(BF16)
                run = mm(twice[d], jnp.concatenate([hi, lo], axis=0))
                mid_at = BLOCK // 2 - 1 if d == 0 else BLOCK // 2
                end_at = BLOCK - 1 if d == 0 else 0
                mid = run[mid_at : mid_at + 1]
                end = run[end_at : end_at + 1]
                qd = q * jnp.exp(run - mid)
                kd = keyed * jnp.exp(mid - run)
                qd_ref[d, tok, wide_lanes] = qd.astype(BF16)
                kd_ref[d, tok, wide_lanes] = kd.astype(BF16)
                reach = (qd * jnp.exp(mid)).astype(BF16)
                ending.append((kd * jnp.exp(end - mid)).astype(BF16))
                last = jnp.exp(end)
                for i in range(ahead):
                    one = slice(i * HG_DK, (i + 1) * HG_DK)
                    qc_ref[tok, (2 * (h0 + i) + d) * HG_DK : (2 * (h0 + i) + d + 1) * HG_DK] = reach[:, one]
                    block_decay[h0 + i][d][b] = last[:, one]
            for i in range(ahead):
                h = h0 + i
                one = slice(i * HG_DK, (i + 1) * HG_DK)
                both = jnp.concatenate([e[:, one] for e in ending], axis=1)
                st_ref[b, h] = mm_tn(v_ref[tok, h * HG_DK : (h + 1) * HG_DK], both)
        for h in range(h0, h0 + ahead):
            for d in range(2):
                side = slice(d * HG_DK, (d + 1) * HG_DK)
                going = range(blocks) if d == 0 else range(blocks - 1, -1, -1)
                total, decay_all = None, None
                for b in going:
                    one = st_ref[b, h, :, side]
                    dec = block_decay[h][d][b]
                    total = one if total is None else total * dec + one
                    decay_all = dec if decay_all is None else decay_all * dec
                whole_state[d, h] = total
                whole_decay[d, h] = jnp.broadcast_to(decay_all, (8, HG_DK))

    if span > 1:
        latent_round(1)
    relay_pair(0, 2)

    @pl.when(jnp.logical_not(has_previous(first)))
    def _():
        pass_on(first)

    for h in range(heads):
        lanes = slice(h * HG_DK, (h + 1) * HG_DK)
        for b in range(blocks):
            tok = slice(b * BLOCK, (b + 1) * BLOCK)
            scores = None
            for d in range(2):
                s = mm_nt(qd_ref[d, tok, lanes], kd_ref[d, tok, lanes])
                s = jnp.where(lower if d == 0 else upper, s, 0.0)
                scores = s if scores is None else scores + s
            intra[tok, lanes] = mm(scores.astype(BF16), v_ref[tok, lanes])

    for c in late:
        c.wait()
    wup = wup_ref[...]
    half_lane = lax.broadcasted_iota(jnp.int32, (rows, LANES), 1)
    put_a = spread_ref[0, NOPE : NOPE + half_rope, :LANES]
    put_b = spread_ref[0, NOPE + half_rope : HEAD, :LANES]

    def expand(j):
        at = flip_bits(place, j)
        for t in range(2):
            keys = slice((2 * j + t) * rows, (2 * j + t + 1) * rows)
            expanded = mm(lbuf[at, t, :rows, :], wup)
            rot = mm_tn(lbuf[at, t, rows:, :rows], put_a) + mm_tn(lbuf[at, t, rows:, rows:], put_b)
            vbuf[keys, :] = expanded.astype(BF16)
            for h in range(att_heads):
                lanes = slice(h * LANES, (h + 1) * LANES)
                kbuf[keys, lanes] = jnp.where(half_lane < NOPE, expanded[:, lanes], rot).astype(BF16)

    for j in range(1, min(2, span)):
        across(flip_bits(place, j)).wait_recv()
    for j in range(min(2, span)):
        expand(j)
    relay_cross(0, 1)
    if span > 2:
        latent_round(2)
    relay_pair(2, 3)
    relay_cross(2)

    @pl.when(has_previous(first))
    def _():
        pass_on(first)

    relay_cross(3)
    for r in range(3, span):
        latent_round(r)
    for j in range(2, span):
        across(flip_bits(place, j)).wait_recv()
    for j in range(2, span):
        expand(j)
    relay_cross(4)

    def act_slot(t):
        return t + tp * (1 - 2 * t)

    cos, sin = cos_ref[...], sin_ref[...]
    scale = HEAD ** (-0.5)
    lane = lax.broadcasted_iota(jnp.int32, (tokens, LANES), 1)
    logw = jnp.zeros((tokens, LANES), F32)
    kept = None
    for h in range(att_heads):
        lanes = slice(h * LANES, (h + 1) * LANES)
        start = window_start(h, att_heads)
        placed = mm(aq_ref[:, start : start + spread_ref.shape[1]], spread_ref[h])
        query = placed[:, :LANES] * cos + placed[:, LANES:] * sin
        scores = mm_nt(query.astype(BF16), kbuf[:, lanes]) * scale
        peak = jnp.max(scores, axis=-1, keepdims=True)
        weights = jnp.exp(scores - peak)
        totals = jnp.sum(weights, axis=-1, keepdims=True)
        result = mm(weights.astype(BF16), vbuf[:, lanes]) / totals
        logw = jnp.where(lane == h, peak + jnp.log(totals), logw)
        if h % 2 == 0:
            kept = pltpu.roll(result, VDIM, 1)
        else:
            at = width + (h // 2) * LANES
            joined = jnp.where(lane < VDIM, kept, result).astype(BF16)
            for t in range(2):
                act[act_slot(t), :, at : at + LANES] = joined[t * rows : (t + 1) * rows]
            if h == 1:
                @pl.when(has_next(1 - first))
                def _():
                    pass_on(1 - first)

                relay_pair(3, len(pairs))
                relay_cross(5)
    relay_cross(*range(6, len(crosses)))
    logw_ref[...] = jnp.transpose(logw)[:att_heads]

    @pl.when(jnp.logical_not(has_next(1 - first)))
    def _():
        pass_on(1 - first)

    for h in range(heads):
        lanes = slice(h * HG_DK, (h + 1) * HG_DK)
        carry = [srecv[d, h].astype(F32) for d in range(2)]
        starts = [[None] * blocks for _ in range(2)]
        for d in range(2):
            side = slice(d * HG_DK, (d + 1) * HG_DK)
            for b in range(blocks) if d == 0 else range(blocks - 1, -1, -1):
                starts[d][b] = carry[d].astype(BF16)
                carry[d] = carry[d] * block_decay[h][d][b] + st_ref[b, h, :, side]
        for b in range(blocks):
            tok = slice(b * BLOCK, (b + 1) * BLOCK)
            t, off = divmod(b * BLOCK, rows)
            begin = jnp.concatenate([starts[0][b], starts[1][b]], axis=1)
            o = intra[tok, lanes] + mm_nt(qc_ref[tok, 2 * h * HG_DK : 2 * (h + 1) * HG_DK], begin)
            o = o * lax.rsqrt(jnp.mean(o * o, axis=-1, keepdims=True) + norm_eps) * gain_ref[:, lanes]
            act[act_slot(t), off : off + BLOCK, lanes] = o.astype(BF16)

    def real_at(g, n):
        return pl.multiple_of((g + parity * (groups - n - 2 * g)) * LANES, LANES)

    x_copies, spans = [], []
    top = act.shape[2]

    def finish(n):
        lo, hi = spans[n]
        x_copies[n].wait_recv()
        at = lo
        for j, g, many in batches[n]:
            w = many * LANES
            there = pl.multiple_of(flip_bits(fs, j) * columns + real_at(g, many), LANES)
            both = keep[:, at : at + w].astype(F32) + precv[:, at : at + w].astype(F32)
            out_ref[:, pl.ds(there, w)] = both.astype(BF16)
            at += w

    offset = 0
    for n, batch in enumerate(batches):
        for j, g, many in batch:
            if j > 0:
                for v in range(g * cuts, (g + many) * cuts):
                    await_chunk(j, v)
        start = offset
        for j, g, many in batch:
            w = many * LANES
            both = mm(act[...].reshape(2 * rows, top), wbuf[j, :, pl.ds(real_at(g, many), w)]).astype(BF16)
            psend[:, offset : offset + w] = both[rows:]
            keep[:, offset : offset + w] = both[:rows]
            offset += w
        part = slice(start, offset)
        spans.append((start, offset))
        c = remote(psend.at[:, part], precv.at[:, part], x_send.at[n], x_recv.at[n], partner)
        c.start()
        x_copies.append(c)
        if n > 0:
            finish(n - 1)
    finish(len(batches) - 1)

    if direct:
        remote(wbuf.at[1:], wbuf.at[1:], w_send.at[0], w_recv.at[0, 0], partner).wait_send()
    for c in x_copies:
        c.wait_send()

    for r in range(span):
        for d in range(2):
            at, there, onward = source(d, r)
            if r > 0:
                @pl.when(there)
                def _():
                    across(at).wait_send()

            if r < span - 1:
                @pl.when(onward)
                def _():
                    along(d, at).wait_send()

    for d in range(2):
        @pl.when(has_next(d))
        def _():
            remote(ssend.at[d], srecv.at[d], s_send.at[d], s_recv.at[d, 0], partner).wait_send()


def local(
    n_fs,
    n_sp,
    recurrent_query,
    forget_logits,
    recurrent_value,
    forget_floor,
    extra_log_decay,
    recurrent_norm_gain,
    attention_query,
    latent,
    rotary_key,
    latent_norm_gain,
    latent_up_weight,
    recurrent_output_weight,
    attention_output_weight,
):
    span = min(n_sp, widest_span)
    tokens, width = recurrent_query.shape[1:]
    heads = width // HG_DK
    att_heads = attention_query.shape[2] // HEAD
    latent_width = latent.shape[2]
    columns = recurrent_output_weight.shape[1]
    att_width = attention_output_weight.shape[0]
    up = att_heads * (NOPE + VDIM)
    blocks = tokens // BLOCK
    rows = tokens // 2
    groups = columns // LANES
    chunks = groups * (width // att_width + 1)
    cos_pad, sin_pad, turns, spread = rope_constants(span * tokens, att_heads)
    vmem = pltpu.VMEM
    whole = pl.BlockSpec(memory_space=vmem)
    hbm = pl.BlockSpec(memory_space=pltpu.HBM)
    dma = pltpu.SemaphoreType.DMA
    mixed, log_weight = pl.pallas_call(
        functools.partial(kernel, (n_fs, span)),
        out_shape=(
            vmem((rows, columns * n_fs), BF16),
            vmem((att_heads, tokens), F32),
        ),
        in_specs=[hbm] * 17,
        out_specs=(whole, whole),
        scratch_shapes=[
            vmem((tokens, width), BF16), vmem((tokens, width), BF16), vmem((tokens, width), BF16),
            vmem((2, width), F32), vmem((heads, tokens), F32), vmem((1, width), F32),
            vmem((tokens, att_heads * HEAD), BF16), vmem((tokens, latent_width), BF16), vmem((ROPE, tokens), BF16),
            vmem((1, latent_width), F32), vmem((latent_width, up), BF16),
            vmem((tokens, LANES), F32), vmem((tokens, LANES), F32), vmem((ROPE, tokens), F32),
            vmem(spread.shape, BF16),
            vmem((span, 2, rows + ROPE // 2, latent_width), BF16),
            vmem((2, heads, HG_DK, HG_DK), BF16),
            vmem((2, heads, HG_DK, HG_DK), BF16),
            vmem((n_fs, width + att_width, columns), BF16),
            vmem((rows, n_fs * columns), BF16),
            vmem((rows, n_fs * columns), BF16),
            vmem((rows, n_fs * columns), BF16),
            vmem((span * tokens, att_heads * LANES), BF16),
            vmem((span * tokens, att_heads * LANES), BF16),
            vmem((tokens, width), F32),
            vmem((2, tokens, width), BF16),
            vmem((2, tokens, width), BF16),
            vmem((tokens, 2 * width), BF16),
            vmem((blocks, heads, HG_DK, 2 * HG_DK), F32),
            vmem((2, rows, width + att_width), BF16),
            vmem((2, heads, HG_DK, HG_DK), F32),
            vmem((2, heads, 8, HG_DK), F32),
            dma((15,)), dma((2,)), dma((2, span)), dma((span,)), dma((span,)), dma((span,)),
            dma((2,)), dma((2, heads)),
            dma((1,)), dma((max(n_fs - 1, 1), chunks)),
            dma((3,)), dma((3,)),
        ],
        compiler_params=pltpu.CompilerParams(
            collective_id=0, has_side_effects=True, vmem_limit_bytes=56 * 2**20
        ),
        name="mixers",
    )(
        recurrent_query[0],
        forget_logits[0],
        recurrent_value[0],
        forget_floor,
        extra_log_decay[0].T,
        recurrent_norm_gain[None],
        attention_query[0],
        latent[0],
        rotary_key[0].T,
        latent_norm_gain[None],
        latent_up_weight,
        jnp.asarray(cos_pad),
        jnp.asarray(sin_pad),
        jnp.asarray(turns),
        jnp.asarray(spread, BF16),
        recurrent_output_weight,
        attention_output_weight,
    )
    return mixed[None], log_weight.T[None]


def solution(mesh):
    placed = (
        P("fs", "sp", "tp"),
        P("fs", "sp", "tp"),
        P("fs", "sp", "tp"),
        P(None, "tp"),
        P("fs", "sp", "tp"),
        P("tp"),
        P("fs", "sp", "tp"),
        P("fs", "sp", None),
        P("fs", "sp", None),
        P(),
        P(),
        P("tp", "fs"),
        P("tp", "fs"),
    )
    return jax.shard_map(
        functools.partial(local, mesh.shape["fs"], mesh.shape["sp"]),
        mesh=mesh,
        in_specs=placed,
        out_specs=(P("fs", ("sp", "tp"), None), P("fs", "sp", "tp")),
        check_vma=False,
    )
```

```python
import functools

import jax
import jax.numpy as jnp
import numpy as np
from jax import lax
from jax.experimental import pallas as pl
from jax.experimental.pallas import tpu as pltpu
from jax.sharding import PartitionSpec as P

HG_DK = 128
NOPE = 64
ROPE = 32
VDIM = 64
HEAD = NOPE + ROPE
LANES = 128
BLOCK = 128

norm_eps = 1e-06
rope_base = 10000.0
widest_span = 8

F32 = jnp.float32
BF16 = jnp.bfloat16


def mm(a, b):
    return jnp.dot(a, b, preferred_element_type=F32)


def mm_nt(a, b):
    return lax.dot_general(a, b, (((1,), (1,)), ((), ())), preferred_element_type=F32)


def mm_tn(a, b):
    return lax.dot_general(a, b, (((0,), (0,)), ((), ())), preferred_element_type=F32)


def flip_bits(value, mask):
    bit = 1
    while bit <= mask:
        if mask & bit:
            value = value + bit - 2 * bit * lax.rem(value // bit, 2)
        bit *= 2
    return value


def window_start(h, heads):
    return min(h * HEAD // LANES * LANES, max(heads * HEAD - 2 * LANES, 0))


def rope_constants(seq_len, heads):
    half = ROPE // 2
    inverse = (np.float32(rope_base) ** (-np.arange(half, dtype=np.float32) / np.float32(half))).astype(np.float32)
    angles = np.arange(seq_len, dtype=np.float32)[:, None] * inverse[None, :]
    cos_pad = np.zeros((seq_len, LANES), np.float32)
    sin_pad = np.zeros((seq_len, LANES), np.float32)
    cos_pad[:, :NOPE] = 1.0
    cos_pad[:, NOPE:HEAD] = np.tile(np.cos(angles), (1, 2))
    sin_pad[:, NOPE:HEAD] = np.tile(np.sin(angles), (1, 2))
    turns = np.concatenate([np.cos(angles).T, np.sin(angles).T], axis=0)
    window = min(2 * LANES, heads * HEAD)
    spread = np.zeros((heads, window, 2 * LANES), np.float32)
    for h in range(heads):
        off = h * HEAD - window_start(h, heads)
        for i in range(HEAD):
            spread[h, off + i, i] = 1.0
        for i in range(half):
            a, b = NOPE + i, NOPE + half + i
            spread[h, off + b, LANES + a] = -1.0
            spread[h, off + a, LANES + b] = 1.0
    return cos_pad, sin_pad, turns, spread


def transfer_plan(n_fs, span, groups, cuts):
    count = groups * cuts
    paired = span % 2 == 0
    if n_fs == 4 and paired:
        direct = {1: count - count // 4, 2: count - count // 3}
        lists = {1: list(range(direct[1])), 2: list(range(count - 1, count - 1 - direct[2], -1))}
        half = count // 2
        by_y = [(1, v, None) for v in range(half)] + [(1, half, 0)]
        by_x = [(2, v, None) for v in range(count - 1, half, -1)] + [(2, half, 1)]
        crosses = [by_y[k : k + 1] + (by_x[k - 1 : k] if k > 0 else []) for k in range(len(by_y))]
        pairs = [(1, v) for v in range(count - direct[1])] + [(2, v) for v in range(count - 1, direct[2] - 1, -1)]
        when = {(j, v): k + 1 for j in lists for k, v in enumerate(lists[j])}
        for k, step in enumerate(crosses):
            for _, v, _ in step:
                when[3, v] = max(direct.values()) + k
        for k, (j, v) in enumerate(pairs):
            when[j, count - 1 - v] = half + 2 + k
    else:
        lists = {j: list(range(count)) for j in range(1, n_fs)}
        crosses, pairs = [], []
        when = {(j, v): v * n_fs + j for j in lists for v in lists[j]}
    last = {(j, g): max(when[j, g * cuts + b] for b in range(cuts)) for j in range(1, n_fs) for g in range(groups)}
    order = [(0, g) for g in range(groups)] + sorted(last, key=lambda one: (last[one], one))
    bounds = [0, len(order) // 2, 3 * len(order) // 4, len(order)]
    batches = []
    for lo, hi in zip(bounds, bounds[1:]):
        batch = []
        for j, g in sorted(order[lo:hi]):
            if batch and batch[-1][0] == j and batch[-1][1] + batch[-1][2] == g and batch[-1][2] == 1:
                batch[-1] = (j, batch[-1][1], 2)
            else:
                batch.append((j, g, 1))
        batches.append(batch)
    return lists, crosses, pairs, batches


def arrival_slots(n_fs, groups, cuts, crosses, pairs):
    relayed = set(pairs) | {(j, v) for step in crosses for j, v, _ in step}
    slots = {}
    for j in range(1, n_fs):
        for g in range(groups):
            chunks = range(g * cuts, (g + 1) * cuts)
            for v in chunks if any((j, v) in relayed for v in chunks) else chunks[:1]:
                slots[j, v] = len(slots)
    return slots


def kernel(
    sizes,
    q_hbm, f_hbm, v_hbm, floor_hbm, extra_hbm, gain_hbm, aq_hbm, lat_hbm, rk_hbm,
    lgain_hbm, wup_hbm, cos_hbm, sin_hbm, turn_hbm, spread_hbm, w1_hbm, w2_hbm,
    out_ref, logw_ref,
    qfv_ref, floor_ref, extra_ref, gain_ref, aq_ref, lat_ref, rk_ref,
    lgain_ref, wup_ref, cs_ref, turn_ref, spread_ref,
    lbuf, ssend, srecv, wbuf, psend, precv, keep,
    kbuf, vbuf, intra, qd_ref, kd_ref, qc_ref, st_ref, act, whole_state, whole_decay,
    in_sem, own_sem, l_send, l_recv, f_send, f_recv, s_send, s_recv, w_send, w_recv,
    x_send, x_recv,
):
    n_fs, span = sizes
    _, tokens, width = qfv_ref.shape
    heads = width // HG_DK
    att_heads = aq_ref.shape[1] // HEAD
    up = att_heads * (NOPE + VDIM)
    blocks = tokens // BLOCK
    latent_width = lat_ref.shape[1]
    columns = w1_hbm.shape[1]
    cut_rows = w2_hbm.shape[0]
    cuts = w1_hbm.shape[0] // cut_rows + 1
    groups = columns // LANES
    rows = tokens // 2
    half_rope = ROPE // 2

    sp, fs, tp = lax.axis_index("sp"), lax.axis_index("fs"), lax.axis_index("tp")
    place = lax.rem(sp, span)
    base = sp - place
    parity = lax.rem(place, 2)
    has_left, has_right = place > 0, place < span - 1
    left = {"sp": base + jnp.maximum(place - 1, 0)}
    right = {"sp": base + jnp.minimum(place + 1, span - 1)}
    pair = {"sp": base + flip_bits(place, 1)}
    partner = {"tp": 1 - tp}
    mesh_id = pl.DeviceIdType.MESH

    def fs_peer(j):
        return {"fs": flip_bits(fs, j)}

    direct, crosses, pairs, batches = transfer_plan(n_fs, span, groups, cuts)

    def at_chunk(v):
        g, b = divmod(v, cuts)
        return g + parity * (groups - 1 - 2 * g), b + parity * (cuts - 1 - 2 * b)

    def chunk(j, v, part=None):
        g, b = at_chunk(v)
        first, size = b * cut_rows, cut_rows
        if part is not None:
            size = cut_rows // 2
            first = first + part * size
        return wbuf.at[j, pl.ds(pl.multiple_of(first, size), size), pl.ds(pl.multiple_of(g * LANES, LANES), LANES)]

    slots = arrival_slots(n_fs, groups, cuts, crosses, pairs)

    def alone(j, v):
        return (j, v - v % cuts + 1) in slots

    def arrival(j, v, seen):
        if not alone(j, seen):
            seen -= seen % cuts
        return w_recv.at[slots[j, seen]]

    def remote(src, dst, send, recv, device):
        return pltpu.make_async_remote_copy(
            src_ref=src, dst_ref=dst, send_sem=send, recv_sem=recv,
            device_id=device, device_id_type=mesh_id,
        )

    def fetch(k, src, dst):
        return pltpu.make_async_copy(src, dst, in_sem.at[k])

    own = [
        pltpu.make_async_copy(src, wbuf.at[0, pl.ds(at, src.shape[0]), :], own_sem.at[0])
        for k, (src, at) in enumerate(((w1_hbm, 0), (w2_hbm, w1_hbm.shape[0])))
    ]
    for c in own:
        c.start()
    my_tokens = pl.ds(pl.multiple_of(place * tokens, tokens), tokens)
    tp_up = pl.ds(pl.multiple_of(tp * up, LANES), up)
    early = [
        fetch(0, lat_hbm, lat_ref), fetch(1, rk_hbm, rk_ref), fetch(2, lgain_hbm, lgain_ref),
        fetch(3, turn_hbm.at[:, my_tokens], turn_ref),
    ]
    qfv = [fetch(6, src, qfv_ref.at[k]) for k, src in enumerate((q_hbm, f_hbm, v_hbm))]
    turning = [fetch(7, src.at[my_tokens, :], cs_ref.at[k]) for k, src in enumerate((cos_hbm, sin_hbm))]
    gates = [
        fetch(4, floor_hbm, floor_ref), fetch(5, extra_hbm, extra_ref),
    ]
    late = [
        fetch(8, gain_hbm, gain_ref), fetch(9, aq_hbm, aq_ref), fetch(10, wup_hbm.at[:, tp_up], wup_ref),
        fetch(11, spread_hbm, spread_ref),
    ]
    for c in early + qfv + gates + turning + late:
        c.start()

    barrier = pltpu.get_barrier_semaphore()
    for j in direct:
        pl.semaphore_signal(barrier, inc=1, device_id=fs_peer(j), device_id_type=mesh_id)
    pl.semaphore_signal(barrier, inc=1, device_id=partner, device_id_type=mesh_id)

    @pl.when(has_left)
    def _():
        pl.semaphore_signal(barrier, inc=1, device_id=left, device_id_type=mesh_id)

    @pl.when(has_right)
    def _():
        pl.semaphore_signal(barrier, inc=1, device_id=right, device_id_type=mesh_id)

    for c in early:
        c.wait()
    lat = lat_ref[...].astype(F32)
    normed = lat * lax.rsqrt(jnp.mean(lat * lat, axis=-1, keepdims=True) + norm_eps) * lgain_ref[...]
    normed = normed.astype(BF16)
    rope_a, rope_b = rk_ref[:half_rope, :].astype(F32), rk_ref[half_rope:, :].astype(F32)
    turn_c, turn_s = turn_ref[:half_rope, :], turn_ref[half_rope:, :]
    turned_a = (rope_a * turn_c - rope_b * turn_s).astype(BF16)
    turned_b = (rope_a * turn_s + rope_b * turn_c).astype(BF16)
    for t in range(2):
        part = slice(t * rows, (t + 1) * rows)
        lbuf[place, t, :rows, :] = normed[part]
        lbuf[place, t, rows:, :rows] = turned_a[:, part]
        lbuf[place, t, rows:, rows:] = turned_b[:, part]

    def source(d, r):
        at = place - r if d == 0 else place + r
        there = at >= 0 if d == 0 else at < span
        onward = jnp.logical_and(there, has_right if d == 0 else has_left)
        return jnp.clip(at, 0, span - 1), there, onward

    def along(d, at):
        return remote(lbuf.at[at, tp], lbuf.at[at, tp], l_send.at[d, at], l_recv.at[at], right if d == 0 else left)

    def across(at):
        return remote(lbuf.at[at, tp], lbuf.at[at, tp], f_send.at[0], f_recv.at[at], partner)

    def latent_round(r):
        for d in range(2):
            at, there, onward = source(d, r)
            if r > 0:
                @pl.when(there)
                def _():
                    along(d, at).wait_recv()
                    across(at).start()

            if r < span - 1:
                @pl.when(onward)
                def _():
                    along(d, at).start()

    pltpu.make_async_copy(wbuf.at[0], wbuf.at[0], own_sem.at[0]).wait()
    pl.semaphore_wait(barrier, len(direct) + 1 + has_left.astype(jnp.int32) + has_right.astype(jnp.int32))
    latent_round(0)
    for k in range(max((len(direct[j]) for j in direct), default=0)):
        for j in direct:
            if k < len(direct[j]):
                v = direct[j][k]
                remote(chunk(0, v), chunk(j, v), w_send.at[0], arrival(j, v, v), fs_peer(j)).start()
    arrived = set()

    def await_chunk(j, v):
        if not alone(j, v):
            v -= v % cuts
        if (j, v) in arrived:
            return
        arrived.add((j, v))
        ref = chunk(j, v)
        if not alone(j, v):
            ref = wbuf.at[j, :, pl.ds(pl.multiple_of(at_chunk(v)[0] * LANES, LANES), LANES)]
        remote(ref, ref, w_send.at[0], arrival(j, v, v), partner).wait_recv()

    def relay_cross(*ks):
        for k in ks:
            for j, v, part in crosses[k] if k < len(crosses) else ():
                await_chunk(j, v)
                remote(chunk(j, v, part), chunk(3, v, part), w_send.at[0], arrival(3, v, v), fs_peer(3 - j)).start()

    def relay_pair(lo, hi):
        for j, v in pairs[lo:hi]:
            await_chunk(j, v)
            seen = groups * cuts - 1 - v
            remote(chunk(j, v), chunk(j, v), w_send.at[0], arrival(j, v, seen), pair).start()

    held_from = max(len(crosses) - 2, 0)
    held_pair = max(len(pairs) - 1, 0)

    def relay_held():
        relay_cross(*range(held_from, len(crosses)))
        relay_pair(held_pair, len(pairs))

    def await_held():
        for j, v, _ in (one for step in crosses[held_from:] for one in step):
            await_chunk(j, v)
        for j, v in pairs[held_pair:]:
            await_chunk(j, v)

    row = lax.broadcasted_iota(jnp.int32, (BLOCK, BLOCK), 0)
    col = lax.broadcasted_iota(jnp.int32, (BLOCK, BLOCK), 1)
    lower = row >= col
    upper = row <= col
    tri = (jnp.where(lower, 1.0, 0.0).astype(BF16), jnp.where(upper, 1.0, 0.0).astype(BF16))
    fetch(6, qfv_ref, qfv_ref).wait()
    for c in gates:
        c.wait()
    spikes = lax.dot_general(
        extra_ref[...],
        jnp.where(
            lax.broadcasted_iota(jnp.int32, (heads, width), 0)
            == lax.broadcasted_iota(jnp.int32, (heads, width), 1) // HG_DK, 1.0, 0.0),
        (((0,), (0,)), ((), ())), precision=lax.Precision.HIGHEST, preferred_element_type=F32)
    first = jnp.where(2 * place < span, 0, 1)

    def link(d, h):
        towards = jnp.clip(place + 1 - 2 * d, 0, span - 1)
        return remote(ssend.at[d, h], srecv.at[d, h], s_send.at[d], s_recv.at[d, h],
                      {"sp": base + towards})

    def has_previous(d):
        return jnp.where(d == 0, place, span - 1 - place) > 0

    def has_next(d):
        return jnp.where(d == 0, span - 1 - place, place) > 0

    def pass_head(d, h):
        @pl.when(has_previous(d))
        def _():
            link(d, h).wait_recv()

        @pl.when(jnp.logical_not(has_previous(d)))
        def _():
            srecv[d, h] = jnp.zeros((HG_DK, HG_DK), BF16)

        @pl.when(has_next(d))
        def _():
            reached = srecv[d, h].astype(F32) * whole_decay[d, h, 0:1] + whole_state[d, h]
            ssend[d, h] = reached.astype(BF16)
            link(d, h).start()

    def pass_on(d):
        for h in range(heads):
            pass_head(d, h)

    twice = [jnp.concatenate([t, t], axis=1) for t in tri]
    block_decay = [[[None] * blocks for _ in range(2)] for _ in range(heads)]
    ahead = 2 if heads % 2 == 0 else 1
    for h0 in range(0, heads, ahead):
        wide_lanes = slice(h0 * HG_DK, (h0 + ahead) * HG_DK)
        for b in range(blocks):
            tok = slice(b * BLOCK, (b + 1) * BLOCK)
            q = qfv_ref[0, tok, wide_lanes].astype(F32)
            miss = 1.0 / (1.0 + jnp.exp(qfv_ref[1, tok, wide_lanes].astype(F32)))
            spike = spikes[tok, wide_lanes]
            ending = []
            for d in range(2):
                keyed = (1.0 - floor_ref[d : d + 1, wide_lanes]) * miss
                decay = jnp.log1p(-keyed) + spike
                hi = decay.astype(BF16)
                lo = (decay - hi.astype(F32)).astype(BF16)
                run = mm(twice[d], jnp.concatenate([hi, lo], axis=0))
                mid_at = BLOCK // 2 - 1 if d == 0 else BLOCK // 2
                end_at = BLOCK - 1 if d == 0 else 0
                mid = run[mid_at : mid_at + 1]
                end = run[end_at : end_at + 1]
                qd = q * jnp.exp(run - mid)
                kd = keyed * jnp.exp(mid - run)
                qd_ref[d, tok, wide_lanes] = qd.astype(BF16)
                kd_ref[d, tok, wide_lanes] = kd.astype(BF16)
                reach = (qd * jnp.exp(mid)).astype(BF16)
                ending.append((kd * jnp.exp(end - mid)).astype(BF16))
                last = jnp.exp(end)
                for i in range(ahead):
                    one = slice(i * HG_DK, (i + 1) * HG_DK)
                    qc_ref[tok, (2 * (h0 + i) + d) * HG_DK : (2 * (h0 + i) + d + 1) * HG_DK] = reach[:, one]
                    block_decay[h0 + i][d][b] = last[:, one]
            for i in range(ahead):
                h = h0 + i
                one = slice(i * HG_DK, (i + 1) * HG_DK)
                both = jnp.concatenate([e[:, one] for e in ending], axis=1)
                st_ref[b, h] = mm_tn(qfv_ref[2, tok, h * HG_DK : (h + 1) * HG_DK], both)
        for h in range(h0, h0 + ahead):
            for d in range(2):
                side = slice(d * HG_DK, (d + 1) * HG_DK)
                going = range(blocks) if d == 0 else range(blocks - 1, -1, -1)
                total, decay_all = None, None
                for b in going:
                    one = st_ref[b, h, :, side]
                    dec = block_decay[h][d][b]
                    total = one if total is None else total * dec + one
                    decay_all = dec if decay_all is None else decay_all * dec
                whole_state[d, h] = total
                whole_decay[d, h] = jnp.broadcast_to(decay_all, (8, HG_DK))

    @pl.when(jnp.logical_not(has_previous(first)))
    def _():
        pass_on(first)

    relay_pair(0, 1)
    if span > 1:
        latent_round(1)
    relay_pair(1, 2)

    for h in range(heads):
        lanes = slice(h * HG_DK, (h + 1) * HG_DK)
        for b in range(blocks):
            tok = slice(b * BLOCK, (b + 1) * BLOCK)
            scores = None
            for d in range(2):
                s = mm_nt(qd_ref[d, tok, lanes], kd_ref[d, tok, lanes])
                s = jnp.where(lower if d == 0 else upper, s, 0.0)
                scores = s if scores is None else scores + s
            intra[tok, lanes] = mm(scores.astype(BF16), qfv_ref[2, tok, lanes])

    fetch(7, cs_ref, cs_ref).wait()
    for c in late:
        c.wait()
    wup = wup_ref[...]
    half_lane = lax.broadcasted_iota(jnp.int32, (rows, LANES), 1)
    put_a = spread_ref[0, NOPE : NOPE + half_rope, :LANES]
    put_b = spread_ref[0, NOPE + half_rope : HEAD, :LANES]

    def expand(j):
        at = flip_bits(place, j)
        for t in range(2):
            keys = slice((2 * j + t) * rows, (2 * j + t + 1) * rows)
            expanded = mm(lbuf[at, t, :rows, :], wup)
            rot = mm_tn(lbuf[at, t, rows:, :rows], put_a) + mm_tn(lbuf[at, t, rows:, rows:], put_b)
            vbuf[keys, :] = expanded.astype(BF16)
            for h in range(att_heads):
                lanes = slice(h * LANES, (h + 1) * LANES)
                kbuf[keys, lanes] = jnp.where(half_lane < NOPE, expanded[:, lanes], rot).astype(BF16)

    for j in range(1, min(2, span)):
        across(flip_bits(place, j)).wait_recv()
    for j in range(min(2, span)):
        expand(j)
    relay_cross(0, 1)
    if span > 2:
        latent_round(2)
    relay_pair(2, 3)
    relay_cross(2)

    @pl.when(has_previous(first))
    def _():
        pass_on(first)

    relay_cross(3)
    for r in range(3, span):
        latent_round(r)
    for j in range(2, span):
        across(flip_bits(place, j)).wait_recv()
    for j in range(2, span):
        expand(j)
    relay_cross(4)

    def act_slot(t):
        return t + tp * (1 - 2 * t)

    cos, sin = cs_ref[0], cs_ref[1]
    scale = HEAD ** (-0.5)
    lane = lax.broadcasted_iota(jnp.int32, (tokens, LANES), 1)
    logw = jnp.zeros((tokens, LANES), F32)
    kept = None
    for h in range(att_heads):
        lanes = slice(h * LANES, (h + 1) * LANES)
        start = window_start(h, att_heads)
        placed = mm(aq_ref[:, start : start + spread_ref.shape[1]], spread_ref[h])
        query = placed[:, :LANES] * cos + placed[:, LANES:] * sin
        scores = mm_nt(query.astype(BF16), kbuf[:, lanes]) * scale
        peak = jnp.max(scores, axis=-1, keepdims=True)
        weights = jnp.exp(scores - peak)
        totals = jnp.sum(weights, axis=-1, keepdims=True)
        result = mm(weights.astype(BF16), vbuf[:, lanes]) / totals
        logw = jnp.where(lane == h, peak + jnp.log(totals), logw)
        if h % 2 == 0:
            kept = pltpu.roll(result, VDIM, 1)
        else:
            at = width + (h // 2) * LANES
            joined = jnp.where(lane < VDIM, kept, result).astype(BF16)
            for t in range(2):
                act[act_slot(t), :, at : at + LANES] = joined[t * rows : (t + 1) * rows]
            if h == 1:
                @pl.when(has_next(1 - first))
                def _():
                    pass_on(1 - first)

                relay_pair(3, held_pair)
    relay_cross(*range(5, held_from))
    await_held()

    @pl.when(tp == 0)
    def _():
        relay_held()

    logw_ref[...] = jnp.transpose(logw)[:att_heads]

    @pl.when(jnp.logical_not(has_next(1 - first)))
    def _():
        pass_on(1 - first)

    for h in range(heads):
        lanes = slice(h * HG_DK, (h + 1) * HG_DK)
        carry = [srecv[d, h].astype(F32) for d in range(2)]
        starts = [[None] * blocks for _ in range(2)]
        for d in range(2):
            side = slice(d * HG_DK, (d + 1) * HG_DK)
            for b in range(blocks) if d == 0 else range(blocks - 1, -1, -1):
                starts[d][b] = carry[d].astype(BF16)
                carry[d] = carry[d] * block_decay[h][d][b] + st_ref[b, h, :, side]
        for b in range(blocks):
            tok = slice(b * BLOCK, (b + 1) * BLOCK)
            t, off = divmod(b * BLOCK, rows)
            begin = jnp.concatenate([starts[0][b], starts[1][b]], axis=1)
            o = intra[tok, lanes] + mm_nt(qc_ref[tok, 2 * h * HG_DK : 2 * (h + 1) * HG_DK], begin)
            o = o * lax.rsqrt(jnp.mean(o * o, axis=-1, keepdims=True) + norm_eps) * gain_ref[:, lanes]
            act[act_slot(t), off : off + BLOCK, lanes] = o.astype(BF16)

    def real_at(g, n):
        return pl.multiple_of((g + parity * (groups - n - 2 * g)) * LANES, LANES)

    x_copies, spans = [], []
    top = act.shape[2]

    def finish(n):
        lo, hi = spans[n]
        x_copies[n].wait_recv()
        at = lo
        for j, g, many in batches[n]:
            w = many * LANES
            there = pl.multiple_of(flip_bits(fs, j) * columns + real_at(g, many), LANES)
            both = keep[:, at : at + w].astype(F32) + precv[:, at : at + w].astype(F32)
            out_ref[:, pl.ds(there, w)] = both.astype(BF16)
            at += w

    offset = 0
    for n, batch in enumerate(batches):
        for j, g, many in batch:
            if j > 0:
                for v in range(g * cuts, (g + many) * cuts):
                    await_chunk(j, v)
        if n == 1:
            @pl.when(tp != 0)
            def _():
                relay_held()

        start = offset
        for j, g, many in batch:
            w = many * LANES
            both = mm(act[...].reshape(2 * rows, top), wbuf[j, :, pl.ds(real_at(g, many), w)]).astype(BF16)
            psend[:, offset : offset + w] = both[rows:]
            keep[:, offset : offset + w] = both[:rows]
            offset += w
        part = slice(start, offset)
        spans.append((start, offset))
        c = remote(psend.at[:, part], precv.at[:, part], x_send.at[0], x_recv.at[n], partner)
        c.start()
        x_copies.append(c)
        if n > 0:
            finish(n - 1)
    finish(len(batches) - 1)

    if direct:
        remote(wbuf.at[1:], wbuf.at[1:], w_send.at[0], w_recv.at[0], partner).wait_send()
    remote(psend, precv, x_send.at[0], x_recv.at[0], partner).wait_send()

    if span > 1:
        all_across = lbuf.at[: span - 1, 0]
        remote(all_across, all_across, f_send.at[0], f_recv.at[0], partner).wait_send()
    for r in range(span):
        for d in range(2):
            at, there, onward = source(d, r)
            if r < span - 1:
                @pl.when(onward)
                def _():
                    along(d, at).wait_send()

    for d in range(2):
        @pl.when(has_next(d))
        def _():
            remote(ssend.at[d], srecv.at[d], s_send.at[d], s_recv.at[d, 0], partner).wait_send()


def local(
    n_fs,
    n_sp,
    recurrent_query,
    forget_logits,
    recurrent_value,
    forget_floor,
    extra_log_decay,
    recurrent_norm_gain,
    attention_query,
    latent,
    rotary_key,
    latent_norm_gain,
    latent_up_weight,
    recurrent_output_weight,
    attention_output_weight,
):
    span = min(n_sp, widest_span)
    tokens, width = recurrent_query.shape[1:]
    heads = width // HG_DK
    att_heads = attention_query.shape[2] // HEAD
    latent_width = latent.shape[2]
    columns = recurrent_output_weight.shape[1]
    att_width = attention_output_weight.shape[0]
    up = att_heads * (NOPE + VDIM)
    blocks = tokens // BLOCK
    rows = tokens // 2
    groups = columns // LANES
    cuts = width // att_width + 1
    _, crosses, pairs, _ = transfer_plan(n_fs, span, groups, cuts)
    slots = len(arrival_slots(n_fs, groups, cuts, crosses, pairs))
    cos_pad, sin_pad, turns, spread = rope_constants(span * tokens, att_heads)
    vmem = pltpu.VMEM
    whole = pl.BlockSpec(memory_space=vmem)
    hbm = pl.BlockSpec(memory_space=pltpu.HBM)
    dma = pltpu.SemaphoreType.DMA
    mixed, log_weight = pl.pallas_call(
        functools.partial(kernel, (n_fs, span)),
        out_shape=(
            vmem((rows, columns * n_fs), BF16),
            vmem((att_heads, tokens), F32),
        ),
        in_specs=[hbm] * 17,
        out_specs=(whole, whole),
        scratch_shapes=[
            vmem((3, tokens, width), BF16),
            vmem((2, width), F32), vmem((heads, tokens), F32), vmem((1, width), F32),
            vmem((tokens, att_heads * HEAD), BF16), vmem((tokens, latent_width), BF16), vmem((ROPE, tokens), BF16),
            vmem((1, latent_width), F32), vmem((latent_width, up), BF16),
            vmem((2, tokens, LANES), F32), vmem((ROPE, tokens), F32),
            vmem(spread.shape, BF16),
            vmem((span, 2, rows + ROPE // 2, latent_width), BF16),
            vmem((2, heads, HG_DK, HG_DK), BF16),
            vmem((2, heads, HG_DK, HG_DK), BF16),
            vmem((n_fs, width + att_width, columns), BF16),
            vmem((rows, n_fs * columns), BF16),
            vmem((rows, n_fs * columns), BF16),
            vmem((rows, n_fs * columns), BF16),
            vmem((span * tokens, att_heads * LANES), BF16),
            vmem((span * tokens, att_heads * LANES), BF16),
            vmem((tokens, width), F32),
            vmem((2, tokens, width), BF16),
            vmem((2, tokens, width), BF16),
            vmem((tokens, 2 * width), BF16),
            vmem((blocks, heads, HG_DK, 2 * HG_DK), F32),
            vmem((2, rows, width + att_width), BF16),
            vmem((2, heads, HG_DK, HG_DK), F32),
            vmem((2, heads, 8, HG_DK), F32),
            dma((12,)), dma((1,)), dma((2, span)), dma((span,)), dma((1,)), dma((span,)),
            dma((2,)), dma((2, heads)),
            dma((1,)), dma((max(slots, 1),)),
            dma((1,)), dma((3,)),
        ],
        compiler_params=pltpu.CompilerParams(
            collective_id=0, has_side_effects=True, vmem_limit_bytes=56 * 2**20
        ),
        name="mixers",
    )(
        recurrent_query[0],
        forget_logits[0],
        recurrent_value[0],
        forget_floor,
        extra_log_decay[0].T,
        recurrent_norm_gain[None],
        attention_query[0],
        latent[0],
        rotary_key[0].T,
        latent_norm_gain[None],
        latent_up_weight,
        jnp.asarray(cos_pad),
        jnp.asarray(sin_pad),
        jnp.asarray(turns),
        jnp.asarray(spread, BF16),
        recurrent_output_weight,
        attention_output_weight,
    )
    return mixed[None], log_weight.T[None]


def solution(mesh):
    placed = (
        P("fs", "sp", "tp"),
        P("fs", "sp", "tp"),
        P("fs", "sp", "tp"),
        P(None, "tp"),
        P("fs", "sp", "tp"),
        P("tp"),
        P("fs", "sp", "tp"),
        P("fs", "sp", None),
        P("fs", "sp", None),
        P(),
        P(),
        P("tp", "fs"),
        P("tp", "fs"),
    )
    return jax.shard_map(
        functools.partial(local, mesh.shape["fs"], mesh.shape["sp"]),
        mesh=mesh,
        in_specs=placed,
        out_specs=(P("fs", ("sp", "tp"), None), P("fs", "sp", "tp")),
        check_vma=False,
    )
```

```python
import functools

import jax
import jax.numpy as jnp
import numpy as np
from jax import lax
from jax.experimental import pallas as pl
from jax.experimental.pallas import tpu as pltpu
from jax.sharding import PartitionSpec as P

HG_DK = 128
NOPE = 64
ROPE = 32
VDIM = 64
HEAD = NOPE + ROPE
LANES = 128
BLOCK = 128

norm_eps = 1e-06
rope_base = 10000.0
widest_span = 8

F32 = jnp.float32
BF16 = jnp.bfloat16


def mm(a, b):
    return jnp.dot(a, b, preferred_element_type=F32)


def mm_nt(a, b):
    return lax.dot_general(a, b, (((1,), (1,)), ((), ())), preferred_element_type=F32)


def mm_tn(a, b):
    return lax.dot_general(a, b, (((0,), (0,)), ((), ())), preferred_element_type=F32)


def flip_bits(value, mask):
    bit = 1
    while bit <= mask:
        if mask & bit:
            value = value + bit - 2 * bit * lax.rem(value // bit, 2)
        bit *= 2
    return value


def window_start(h, heads):
    return min(h * HEAD // LANES * LANES, max(heads * HEAD - 2 * LANES, 0))


def rope_constants(seq_len, heads):
    half = ROPE // 2
    inverse = (np.float32(rope_base) ** (-np.arange(half, dtype=np.float32) / np.float32(half))).astype(np.float32)
    angles = np.arange(seq_len, dtype=np.float32)[:, None] * inverse[None, :]
    cos_pad = np.zeros((seq_len, LANES), np.float32)
    sin_pad = np.zeros((seq_len, LANES), np.float32)
    cos_pad[:, :NOPE] = 1.0
    cos_pad[:, NOPE:HEAD] = np.tile(np.cos(angles), (1, 2))
    sin_pad[:, NOPE:HEAD] = np.tile(np.sin(angles), (1, 2))
    turns = np.concatenate([np.cos(angles).T, np.sin(angles).T], axis=0)
    window = min(2 * LANES, heads * HEAD)
    spread = np.zeros((heads, window, 2 * LANES), np.float32)
    for h in range(heads):
        off = h * HEAD - window_start(h, heads)
        for i in range(HEAD):
            spread[h, off + i, i] = 1.0
        for i in range(half):
            a, b = NOPE + i, NOPE + half + i
            spread[h, off + b, LANES + a] = -1.0
            spread[h, off + a, LANES + b] = 1.0
    return cos_pad, sin_pad, turns, spread


def transfer_plan(n_fs, span, groups, cuts):
    count = groups * cuts
    paired = span % 2 == 0
    if n_fs == 4 and paired:
        direct = {1: count - count // 4, 2: count - count // 3}
        lists = {1: list(range(direct[1])), 2: list(range(count - 1, count - 1 - direct[2], -1))}
        half = count // 2
        by_y = [(1, v, None) for v in range(half)] + [(1, half, 0)]
        by_x = [(2, v, None) for v in range(count - 1, half, -1)] + [(2, half, 1)]
        crosses = [by_y[k : k + 1] + (by_x[k - 1 : k] if k > 0 else []) for k in range(len(by_y))]
        pairs = [(1, v) for v in range(count - direct[1])] + [(2, v) for v in range(count - 1, direct[2] - 1, -1)]
        when = {(j, v): k + 1 for j in lists for k, v in enumerate(lists[j])}
        for k, step in enumerate(crosses):
            for _, v, _ in step:
                when[3, v] = max(direct.values()) + k
        for k, (j, v) in enumerate(pairs):
            when[j, count - 1 - v] = half + 2 + k
    else:
        lists = {j: list(range(count)) for j in range(1, n_fs)}
        crosses, pairs = [], []
        when = {(j, v): v * n_fs + j for j in lists for v in lists[j]}
    last = {(j, g): max(when[j, g * cuts + b] for b in range(cuts)) for j in range(1, n_fs) for g in range(groups)}
    order = [(0, g) for g in range(groups)] + sorted(last, key=lambda one: (last[one], one))
    bounds = [0, len(order) // 2, 3 * len(order) // 4, len(order)]
    batches = []
    for lo, hi in zip(bounds, bounds[1:]):
        batch = []
        for j, g in sorted(order[lo:hi]):
            if batch and batch[-1][0] == j and batch[-1][1] + batch[-1][2] == g and batch[-1][2] == 1:
                batch[-1] = (j, batch[-1][1], 2)
            else:
                batch.append((j, g, 1))
        batches.append(batch)
    return lists, crosses, pairs, batches


def arrival_slots(n_fs, groups, cuts, crosses, pairs):
    relayed = set(pairs) | {(j, v) for step in crosses for j, v, _ in step}
    slots = {}
    for j in range(1, n_fs):
        for g in range(groups):
            chunks = range(g * cuts, (g + 1) * cuts)
            for v in chunks if any((j, v) in relayed for v in chunks) else chunks[:1]:
                slots[j, v] = len(slots)
    return slots


def kernel(
    sizes,
    q_hbm, f_hbm, v_hbm, floor_hbm, extra_hbm, gain_hbm, aq_hbm, lat_hbm, rk_hbm,
    lgain_hbm, wup_hbm, cos_hbm, sin_hbm, turn_hbm, spread_hbm, w1_hbm, w2_hbm,
    out_ref, logw_ref,
    qfv_ref, floor_ref, extra_ref, gain_ref, aq_ref, lat_ref, rk_ref,
    lgain_ref, wup_ref, cs_ref, turn_ref, spread_ref,
    lbuf, ssend, srecv, wbuf, psend, precv, keep,
    kbuf, vbuf, intra, qd_ref, kd_ref, qc_ref, st_ref, act, whole_state, whole_decay,
    in_sem, own_sem, l_send, l_recv, f_send, f_recv, s_send, s_recv, w_send, w_recv,
    x_send, x_recv,
):
    n_fs, span = sizes
    _, tokens, width = qfv_ref.shape
    heads = width // HG_DK
    att_heads = aq_ref.shape[1] // HEAD
    up = att_heads * (NOPE + VDIM)
    blocks = tokens // BLOCK
    latent_width = lat_ref.shape[1]
    columns = w1_hbm.shape[1]
    cut_rows = w2_hbm.shape[0]
    cuts = w1_hbm.shape[0] // cut_rows + 1
    groups = columns // LANES
    rows = tokens // 2
    half_rope = ROPE // 2

    sp, fs, tp = lax.axis_index("sp"), lax.axis_index("fs"), lax.axis_index("tp")
    place = lax.rem(sp, span)
    base = sp - place
    parity = lax.rem(place, 2)
    has_left, has_right = place > 0, place < span - 1
    left = {"sp": base + jnp.maximum(place - 1, 0)}
    right = {"sp": base + jnp.minimum(place + 1, span - 1)}
    pair = {"sp": base + flip_bits(place, 1)}
    partner = {"tp": 1 - tp}
    mesh_id = pl.DeviceIdType.MESH

    def fs_peer(j):
        return {"fs": flip_bits(fs, j)}

    direct, crosses, pairs, batches = transfer_plan(n_fs, span, groups, cuts)

    def at_chunk(v):
        g, b = divmod(v, cuts)
        return g + parity * (groups - 1 - 2 * g), b + parity * (cuts - 1 - 2 * b)

    def chunk(j, v, part=None):
        g, b = at_chunk(v)
        first, size = b * cut_rows, cut_rows
        if part is not None:
            size = cut_rows // 2
            first = first + part * size
        return wbuf.at[j, pl.ds(pl.multiple_of(first, size), size), pl.ds(pl.multiple_of(g * LANES, LANES), LANES)]

    slots = arrival_slots(n_fs, groups, cuts, crosses, pairs)

    def alone(j, v):
        return (j, v - v % cuts + 1) in slots

    def arrival(j, v, seen):
        if not alone(j, seen):
            seen -= seen % cuts
        return w_recv.at[slots[j, seen]]

    def remote(src, dst, send, recv, device):
        return pltpu.make_async_remote_copy(
            src_ref=src, dst_ref=dst, send_sem=send, recv_sem=recv,
            device_id=device, device_id_type=mesh_id,
        )

    def fetch(k, src, dst):
        return pltpu.make_async_copy(src, dst, in_sem.at[k])

    own = [
        pltpu.make_async_copy(src, wbuf.at[0, pl.ds(at, src.shape[0]), :], own_sem.at[0])
        for k, (src, at) in enumerate(((w1_hbm, 0), (w2_hbm, w1_hbm.shape[0])))
    ]
    for c in own:
        c.start()
    my_tokens = pl.ds(pl.multiple_of(place * tokens, tokens), tokens)
    tp_up = pl.ds(pl.multiple_of(tp * up, LANES), up)
    early = [
        fetch(0, lat_hbm, lat_ref), fetch(1, rk_hbm, rk_ref), fetch(2, lgain_hbm, lgain_ref),
        fetch(3, turn_hbm.at[:, my_tokens], turn_ref),
    ]
    qfv = [fetch(6, src, qfv_ref.at[k]) for k, src in enumerate((q_hbm, f_hbm, v_hbm))]
    turning = [fetch(7, src.at[my_tokens, :], cs_ref.at[k]) for k, src in enumerate((cos_hbm, sin_hbm))]
    gates = [
        fetch(4, floor_hbm, floor_ref), fetch(5, extra_hbm, extra_ref),
    ]
    late = [
        fetch(8, gain_hbm, gain_ref), fetch(9, aq_hbm, aq_ref), fetch(10, wup_hbm.at[:, tp_up], wup_ref),
        fetch(11, spread_hbm, spread_ref),
    ]
    for c in early + qfv + gates + turning + late:
        c.start()

    barrier = pltpu.get_barrier_semaphore()
    for j in direct:
        pl.semaphore_signal(barrier, inc=1, device_id=fs_peer(j), device_id_type=mesh_id)
    pl.semaphore_signal(barrier, inc=1, device_id=partner, device_id_type=mesh_id)

    @pl.when(has_left)
    def _():
        pl.semaphore_signal(barrier, inc=1, device_id=left, device_id_type=mesh_id)

    @pl.when(has_right)
    def _():
        pl.semaphore_signal(barrier, inc=1, device_id=right, device_id_type=mesh_id)

    for c in early:
        c.wait()
    lat = lat_ref[...].astype(F32)
    normed = lat * lax.rsqrt(jnp.mean(lat * lat, axis=-1, keepdims=True) + norm_eps) * lgain_ref[...]
    normed = normed.astype(BF16)
    rope_a, rope_b = rk_ref[:half_rope, :].astype(F32), rk_ref[half_rope:, :].astype(F32)
    turn_c, turn_s = turn_ref[:half_rope, :], turn_ref[half_rope:, :]
    turned_a = (rope_a * turn_c - rope_b * turn_s).astype(BF16)
    turned_b = (rope_a * turn_s + rope_b * turn_c).astype(BF16)
    for t in range(2):
        part = slice(t * rows, (t + 1) * rows)
        lbuf[place, t, :rows, :] = normed[part]
        lbuf[place, t, rows:, :rows] = turned_a[:, part]
        lbuf[place, t, rows:, rows:] = turned_b[:, part]

    def source(d, r):
        at = place - r if d == 0 else place + r
        there = at >= 0 if d == 0 else at < span
        onward = jnp.logical_and(there, has_right if d == 0 else has_left)
        return jnp.clip(at, 0, span - 1), there, onward

    def along(d, at):
        return remote(lbuf.at[at, tp], lbuf.at[at, tp], l_send.at[d, at], l_recv.at[at], right if d == 0 else left)

    def across(at):
        return remote(lbuf.at[at, tp], lbuf.at[at, tp], f_send.at[0], f_recv.at[at], partner)

    def latent_round(r):
        for d in range(2):
            at, there, onward = source(d, r)
            if r > 0:
                @pl.when(there)
                def _():
                    along(d, at).wait_recv()
                    across(at).start()

            if r < span - 1:
                @pl.when(onward)
                def _():
                    along(d, at).start()

    pltpu.make_async_copy(wbuf.at[0], wbuf.at[0], own_sem.at[0]).wait()
    pl.semaphore_wait(barrier, len(direct) + 1 + has_left.astype(jnp.int32) + has_right.astype(jnp.int32))
    latent_round(0)
    for k in range(max((len(direct[j]) for j in direct), default=0)):
        for j in direct:
            if k < len(direct[j]):
                v = direct[j][k]
                remote(chunk(0, v), chunk(j, v), w_send.at[0], arrival(j, v, v), fs_peer(j)).start()
    arrived = set()

    def await_chunk(j, v):
        if not alone(j, v):
            v -= v % cuts
        if (j, v) in arrived:
            return
        arrived.add((j, v))
        ref = chunk(j, v)
        if not alone(j, v):
            ref = wbuf.at[j, :, pl.ds(pl.multiple_of(at_chunk(v)[0] * LANES, LANES), LANES)]
        remote(ref, ref, w_send.at[0], arrival(j, v, v), partner).wait_recv()

    def relay_cross(*ks):
        for k in ks:
            for j, v, part in crosses[k] if k < len(crosses) else ():
                await_chunk(j, v)
                remote(chunk(j, v, part), chunk(3, v, part), w_send.at[0], arrival(3, v, v), fs_peer(3 - j)).start()

    def relay_pair(lo, hi):
        for j, v in pairs[lo:hi]:
            await_chunk(j, v)
            seen = groups * cuts - 1 - v
            remote(chunk(j, v), chunk(j, v), w_send.at[0], arrival(j, v, seen), pair).start()

    held_from = max(len(crosses) - 2, 0)
    held_pair = max(len(pairs) - 1, 0)

    def relay_held():
        relay_cross(*range(held_from, len(crosses)))
        relay_pair(held_pair, len(pairs))

    def await_held():
        for j, v, _ in (one for step in crosses[held_from:] for one in step):
            await_chunk(j, v)
        for j, v in pairs[held_pair:]:
            await_chunk(j, v)

    row = lax.broadcasted_iota(jnp.int32, (BLOCK, BLOCK), 0)
    col = lax.broadcasted_iota(jnp.int32, (BLOCK, BLOCK), 1)
    lower = row >= col
    upper = row <= col
    tri = (jnp.where(lower, 1.0, 0.0).astype(BF16), jnp.where(upper, 1.0, 0.0).astype(BF16))
    fetch(6, qfv_ref, qfv_ref).wait()
    for c in gates:
        c.wait()
    spikes = lax.dot_general(
        extra_ref[...],
        jnp.where(
            lax.broadcasted_iota(jnp.int32, (heads, width), 0)
            == lax.broadcasted_iota(jnp.int32, (heads, width), 1) // HG_DK, 1.0, 0.0),
        (((0,), (0,)), ((), ())), precision=lax.Precision.HIGHEST, preferred_element_type=F32)
    first = jnp.where(2 * place < span, 0, 1)

    def link(d, h):
        towards = jnp.clip(place + 1 - 2 * d, 0, span - 1)
        return remote(ssend.at[d, h], srecv.at[d, h], s_send.at[d], s_recv.at[d, h],
                      {"sp": base + towards})

    def has_previous(d):
        return jnp.where(d == 0, place, span - 1 - place) > 0

    def has_next(d):
        return jnp.where(d == 0, span - 1 - place, place) > 0

    def pass_head(d, h):
        @pl.when(has_previous(d))
        def _():
            link(d, h).wait_recv()

        @pl.when(jnp.logical_not(has_previous(d)))
        def _():
            srecv[d, h] = jnp.zeros((HG_DK, HG_DK), BF16)

        @pl.when(has_next(d))
        def _():
            reached = srecv[d, h].astype(F32) * whole_decay[d, h, 0:1] + whole_state[d, h]
            ssend[d, h] = reached.astype(BF16)
            link(d, h).start()

    def pass_on(d):
        for h in range(heads):
            pass_head(d, h)

    twice = [jnp.concatenate([t, t], axis=1) for t in tri]
    block_decay = [[[None] * blocks for _ in range(2)] for _ in range(heads)]
    ahead = 2 if heads % 2 == 0 else 1
    for h0 in range(0, heads, ahead):
        wide_lanes = slice(h0 * HG_DK, (h0 + ahead) * HG_DK)
        for b in range(blocks):
            tok = slice(b * BLOCK, (b + 1) * BLOCK)
            q = qfv_ref[0, tok, wide_lanes].astype(F32)
            miss = 1.0 / (1.0 + jnp.exp(qfv_ref[1, tok, wide_lanes].astype(F32)))
            spike = spikes[tok, wide_lanes]
            ending = []
            for d in range(2):
                keyed = (1.0 - floor_ref[d : d + 1, wide_lanes]) * miss
                decay = jnp.log1p(-keyed) + spike
                hi = decay.astype(BF16)
                lo = (decay - hi.astype(F32)).astype(BF16)
                run = mm(twice[d], jnp.concatenate([hi, lo], axis=0))
                mid_at = BLOCK // 2 - 1 if d == 0 else BLOCK // 2
                end_at = BLOCK - 1 if d == 0 else 0
                mid = run[mid_at : mid_at + 1]
                end = run[end_at : end_at + 1]
                qd = q * jnp.exp(run - mid)
                kd = keyed * jnp.exp(mid - run)
                qd_ref[d, tok, wide_lanes] = qd.astype(BF16)
                kd_ref[d, tok, wide_lanes] = kd.astype(BF16)
                reach = (qd * jnp.exp(mid)).astype(BF16)
                ending.append((kd * jnp.exp(end - mid)).astype(BF16))
                last = jnp.exp(end)
                for i in range(ahead):
                    one = slice(i * HG_DK, (i + 1) * HG_DK)
                    qc_ref[tok, (2 * (h0 + i) + d) * HG_DK : (2 * (h0 + i) + d + 1) * HG_DK] = reach[:, one]
                    block_decay[h0 + i][d][b] = last[:, one]
            for i in range(ahead):
                h = h0 + i
                one = slice(i * HG_DK, (i + 1) * HG_DK)
                both = jnp.concatenate([e[:, one] for e in ending], axis=1)
                st_ref[b, h] = mm_tn(qfv_ref[2, tok, h * HG_DK : (h + 1) * HG_DK], both)
        for h in range(h0, h0 + ahead):
            for d in range(2):
                side = slice(d * HG_DK, (d + 1) * HG_DK)
                going = range(blocks) if d == 0 else range(blocks - 1, -1, -1)
                total, decay_all = None, None
                for b in going:
                    one = st_ref[b, h, :, side]
                    dec = block_decay[h][d][b]
                    total = one if total is None else total * dec + one
                    decay_all = dec if decay_all is None else decay_all * dec
                whole_state[d, h] = total
                whole_decay[d, h] = jnp.broadcast_to(decay_all, (8, HG_DK))

    @pl.when(jnp.logical_not(has_previous(first)))
    def _():
        pass_on(first)

    relay_pair(0, 1)
    if span > 1:
        latent_round(1)
    relay_pair(1, 2)

    for h in range(heads):
        lanes = slice(h * HG_DK, (h + 1) * HG_DK)
        for b in range(blocks):
            tok = slice(b * BLOCK, (b + 1) * BLOCK)
            scores = None
            for d in range(2):
                s = mm_nt(qd_ref[d, tok, lanes], kd_ref[d, tok, lanes])
                s = jnp.where(lower if d == 0 else upper, s, 0.0)
                scores = s if scores is None else scores + s
            intra[tok, lanes] = mm(scores.astype(BF16), qfv_ref[2, tok, lanes])

    fetch(7, cs_ref, cs_ref).wait()
    for c in late:
        c.wait()
    wup = wup_ref[...]
    half_lane = lax.broadcasted_iota(jnp.int32, (rows, LANES), 1)
    put_a = spread_ref[0, NOPE : NOPE + half_rope, :LANES]
    put_b = spread_ref[0, NOPE + half_rope : HEAD, :LANES]

    def expand(j):
        at = flip_bits(place, j)
        for t in range(2):
            keys = slice((2 * j + t) * rows, (2 * j + t + 1) * rows)
            expanded = mm(lbuf[at, t, :rows, :], wup)
            rot = mm_tn(lbuf[at, t, rows:, :rows], put_a) + mm_tn(lbuf[at, t, rows:, rows:], put_b)
            vbuf[keys, :] = expanded.astype(BF16)
            for h in range(att_heads):
                lanes = slice(h * LANES, (h + 1) * LANES)
                kbuf[keys, lanes] = jnp.where(half_lane < NOPE, expanded[:, lanes], rot).astype(BF16)

    for j in range(1, min(2, span)):
        across(flip_bits(place, j)).wait_recv()
    for j in range(min(2, span)):
        expand(j)
    relay_cross(0, 1)
    if span > 2:
        latent_round(2)
    relay_pair(2, 3)
    relay_cross(2)

    @pl.when(has_previous(first))
    def _():
        pass_on(first)

    relay_cross(3)
    for r in range(3, span):
        latent_round(r)
    for j in range(2, span):
        across(flip_bits(place, j)).wait_recv()
    for j in range(2, span):
        expand(j)
    relay_cross(4)

    def act_slot(t):
        return t + tp * (1 - 2 * t)

    cos, sin = cs_ref[0], cs_ref[1]
    scale = HEAD ** (-0.5)
    lane = lax.broadcasted_iota(jnp.int32, (tokens, LANES), 1)
    logw = jnp.zeros((tokens, LANES), F32)
    kept = None
    for h in range(att_heads):
        lanes = slice(h * LANES, (h + 1) * LANES)
        start = window_start(h, att_heads)
        placed = mm(aq_ref[:, start : start + spread_ref.shape[1]], spread_ref[h])
        query = placed[:, :LANES] * cos + placed[:, LANES:] * sin
        scores = mm_nt(query.astype(BF16), kbuf[:, lanes]) * scale
        peak = jnp.max(scores, axis=-1, keepdims=True)
        weights = jnp.exp(scores - peak)
        totals = jnp.sum(weights, axis=-1, keepdims=True)
        result = mm(weights.astype(BF16), vbuf[:, lanes]) / totals
        logw = jnp.where(lane == h, peak + jnp.log(totals), logw)
        if h % 2 == 0:
            kept = pltpu.roll(result, VDIM, 1)
        else:
            at = width + (h // 2) * LANES
            joined = jnp.where(lane < VDIM, kept, result).astype(BF16)
            for t in range(2):
                act[act_slot(t), :, at : at + LANES] = joined[t * rows : (t + 1) * rows]
            if h == 1:
                @pl.when(has_next(1 - first))
                def _():
                    pass_on(1 - first)

                relay_pair(3, max(held_pair, 3))
    relay_cross(*range(5, max(held_from, 5)))
    await_held()

    @pl.when(tp == 0)
    def _():
        relay_held()

    logw_ref[...] = jnp.transpose(logw)[:att_heads]

    @pl.when(jnp.logical_not(has_next(1 - first)))
    def _():
        pass_on(1 - first)

    for h in range(heads):
        lanes = slice(h * HG_DK, (h + 1) * HG_DK)
        carry = [srecv[d, h].astype(F32) for d in range(2)]
        starts = [[None] * blocks for _ in range(2)]
        for d in range(2):
            side = slice(d * HG_DK, (d + 1) * HG_DK)
            for b in range(blocks) if d == 0 else range(blocks - 1, -1, -1):
                starts[d][b] = carry[d].astype(BF16)
                carry[d] = carry[d] * block_decay[h][d][b] + st_ref[b, h, :, side]
        for b in range(blocks):
            tok = slice(b * BLOCK, (b + 1) * BLOCK)
            t, off = divmod(b * BLOCK, rows)
            begin = jnp.concatenate([starts[0][b], starts[1][b]], axis=1)
            o = intra[tok, lanes] + mm_nt(qc_ref[tok, 2 * h * HG_DK : 2 * (h + 1) * HG_DK], begin)
            o = o * lax.rsqrt(jnp.mean(o * o, axis=-1, keepdims=True) + norm_eps) * gain_ref[:, lanes]
            act[act_slot(t), off : off + BLOCK, lanes] = o.astype(BF16)

    def real_at(g, n):
        return pl.multiple_of((g + parity * (groups - n - 2 * g)) * LANES, LANES)

    x_copies, spans = [], []
    top = act.shape[2]

    def finish(n):
        lo, hi = spans[n]
        x_copies[n].wait_recv()
        at = lo
        for j, g, many in batches[n]:
            w = many * LANES
            there = pl.multiple_of(flip_bits(fs, j) * columns + real_at(g, many), LANES)
            both = keep[:, at : at + w].astype(F32) + precv[:, at : at + w].astype(F32)
            out_ref[:, pl.ds(there, w)] = both.astype(BF16)
            at += w

    offset = 0
    for n, batch in enumerate(batches):
        for j, g, many in batch:
            if j > 0:
                for v in range(g * cuts, (g + many) * cuts):
                    await_chunk(j, v)
        if n == 1:
            @pl.when(tp != 0)
            def _():
                relay_held()

        start = offset
        for j, g, many in batch:
            w = many * LANES
            both = mm(act[...].reshape(2 * rows, top), wbuf[j, :, pl.ds(real_at(g, many), w)]).astype(BF16)
            psend[:, offset : offset + w] = both[rows:]
            keep[:, offset : offset + w] = both[:rows]
            offset += w
        part = slice(start, offset)
        spans.append((start, offset))
        c = remote(psend.at[:, part], precv.at[:, part], x_send.at[0], x_recv.at[n], partner)
        c.start()
        x_copies.append(c)
        if n > 0:
            finish(n - 1)
    finish(len(batches) - 1)

    if direct:
        remote(wbuf.at[1:], wbuf.at[1:], w_send.at[0], w_recv.at[0], partner).wait_send()
    remote(psend, precv, x_send.at[0], x_recv.at[0], partner).wait_send()

    if span > 1:
        all_across = lbuf.at[: span - 1, 0]
        remote(all_across, all_across, f_send.at[0], f_recv.at[0], partner).wait_send()
    for r in range(span):
        for d in range(2):
            at, there, onward = source(d, r)
            if r < span - 1:
                @pl.when(onward)
                def _():
                    along(d, at).wait_send()

    for d in range(2):
        @pl.when(has_next(d))
        def _():
            remote(ssend.at[d], srecv.at[d], s_send.at[d], s_recv.at[d, 0], partner).wait_send()


def flush(mixed_ref, logw_ref, mixed_hbm, logw_hbm, sems):
    copies = (
        pltpu.make_async_copy(mixed_ref, mixed_hbm, sems.at[0]),
        pltpu.make_async_copy(logw_ref, logw_hbm, sems.at[1]),
    )
    for c in copies:
        c.start()
    for c in copies:
        c.wait()


def local(
    n_fs,
    n_sp,
    recurrent_query,
    forget_logits,
    recurrent_value,
    forget_floor,
    extra_log_decay,
    recurrent_norm_gain,
    attention_query,
    latent,
    rotary_key,
    latent_norm_gain,
    latent_up_weight,
    recurrent_output_weight,
    attention_output_weight,
):
    span = min(n_sp, widest_span)
    tokens, width = recurrent_query.shape[1:]
    heads = width // HG_DK
    att_heads = attention_query.shape[2] // HEAD
    latent_width = latent.shape[2]
    columns = recurrent_output_weight.shape[1]
    att_width = attention_output_weight.shape[0]
    up = att_heads * (NOPE + VDIM)
    blocks = tokens // BLOCK
    rows = tokens // 2
    groups = columns // LANES
    cuts = width // att_width + 1
    _, crosses, pairs, _ = transfer_plan(n_fs, span, groups, cuts)
    slots = len(arrival_slots(n_fs, groups, cuts, crosses, pairs))
    cos_pad, sin_pad, turns, spread = rope_constants(span * tokens, att_heads)
    vmem = pltpu.VMEM
    whole = pl.BlockSpec(memory_space=vmem)
    hbm = pl.BlockSpec(memory_space=pltpu.HBM)
    dma = pltpu.SemaphoreType.DMA
    mixed, log_weight = pl.pallas_call(
        functools.partial(kernel, (n_fs, span)),
        out_shape=(
            vmem((rows, columns * n_fs), BF16),
            vmem((att_heads, tokens), F32),
        ),
        in_specs=[hbm] * 17,
        out_specs=(whole, whole),
        scratch_shapes=[
            vmem((3, tokens, width), BF16),
            vmem((2, width), F32), vmem((heads, tokens), F32), vmem((1, width), F32),
            vmem((tokens, att_heads * HEAD), BF16), vmem((tokens, latent_width), BF16), vmem((ROPE, tokens), BF16),
            vmem((1, latent_width), F32), vmem((latent_width, up), BF16),
            vmem((2, tokens, LANES), F32), vmem((ROPE, tokens), F32),
            vmem(spread.shape, BF16),
            vmem((span, 2, rows + ROPE // 2, latent_width), BF16),
            vmem((2, heads, HG_DK, HG_DK), BF16),
            vmem((2, heads, HG_DK, HG_DK), BF16),
            vmem((n_fs, width + att_width, columns), BF16),
            vmem((rows, n_fs * columns), BF16),
            vmem((rows, n_fs * columns), BF16),
            vmem((rows, n_fs * columns), BF16),
            vmem((span * tokens, att_heads * LANES), BF16),
            vmem((span * tokens, att_heads * LANES), BF16),
            vmem((tokens, width), F32),
            vmem((2, tokens, width), BF16),
            vmem((2, tokens, width), BF16),
            vmem((tokens, 2 * width), BF16),
            vmem((blocks, heads, HG_DK, 2 * HG_DK), F32),
            vmem((2, rows, width + att_width), BF16),
            vmem((2, heads, HG_DK, HG_DK), F32),
            vmem((2, heads, 8, HG_DK), F32),
            dma((12,)), dma((1,)), dma((2, span)), dma((span,)), dma((1,)), dma((span,)),
            dma((2,)), dma((2, heads)),
            dma((1,)), dma((max(slots, 1),)),
            dma((1,)), dma((3,)),
        ],
        compiler_params=pltpu.CompilerParams(
            collective_id=0, has_side_effects=True, vmem_limit_bytes=56 * 2**20
        ),
        name="mixers",
    )(
        recurrent_query[0],
        forget_logits[0],
        recurrent_value[0],
        forget_floor,
        extra_log_decay[0].T,
        recurrent_norm_gain[None],
        attention_query[0],
        latent[0],
        rotary_key[0].T,
        latent_norm_gain[None],
        latent_up_weight,
        jnp.asarray(cos_pad),
        jnp.asarray(sin_pad),
        jnp.asarray(turns),
        jnp.asarray(spread, BF16),
        recurrent_output_weight,
        attention_output_weight,
    )
    mixed = pltpu.with_memory_space_constraint(mixed, vmem)
    log_weight = pltpu.with_memory_space_constraint(log_weight, vmem)
    mixed, log_weight = pl.pallas_call(
        flush,
        out_shape=(
            jax.ShapeDtypeStruct((rows, columns * n_fs), BF16),
            jax.ShapeDtypeStruct((att_heads, tokens), F32),
        ),
        in_specs=[whole, whole],
        out_specs=(hbm, hbm),
        scratch_shapes=[dma((2,))],
        name="flush",
    )(mixed, log_weight)
    return mixed[None], log_weight.T[None]


def solution(mesh):
    placed = (
        P("fs", "sp", "tp"),
        P("fs", "sp", "tp"),
        P("fs", "sp", "tp"),
        P(None, "tp"),
        P("fs", "sp", "tp"),
        P("tp"),
        P("fs", "sp", "tp"),
        P("fs", "sp", None),
        P("fs", "sp", None),
        P(),
        P(),
        P("tp", "fs"),
        P("tp", "fs"),
    )
    return jax.shard_map(
        functools.partial(local, mesh.shape["fs"], mesh.shape["sp"]),
        mesh=mesh,
        in_specs=placed,
        out_specs=(P("fs", ("sp", "tp"), None), P("fs", "sp", "tp")),
        check_vma=False,
    )
```

```python
import functools

import jax
import jax.numpy as jnp
import numpy as np
from jax import lax
from jax.experimental import pallas as pl
from jax.experimental.pallas import tpu as pltpu
from jax.sharding import PartitionSpec as P

HG_DK = 128
NOPE = 64
ROPE = 32
VDIM = 64
HEAD = NOPE + ROPE
LANES = 128
BLOCK = 128

norm_eps = 1e-06
rope_base = 10000.0
widest_span = 8

F32 = jnp.float32
BF16 = jnp.bfloat16


def mm(a, b):
    return jnp.dot(a, b, preferred_element_type=F32)


def mm_nt(a, b):
    return lax.dot_general(a, b, (((1,), (1,)), ((), ())), preferred_element_type=F32)


def mm_tn(a, b):
    return lax.dot_general(a, b, (((0,), (0,)), ((), ())), preferred_element_type=F32)


def flip_bits(value, mask):
    bit = 1
    while bit <= mask:
        if mask & bit:
            value = value + bit - 2 * bit * lax.rem(value // bit, 2)
        bit *= 2
    return value


def window_start(h, heads):
    return min(h * HEAD // LANES * LANES, max(heads * HEAD - 2 * LANES, 0))


def rope_constants(seq_len, heads):
    half = ROPE // 2
    inverse = (np.float32(rope_base) ** (-np.arange(half, dtype=np.float32) / np.float32(half))).astype(np.float32)
    angles = np.arange(seq_len, dtype=np.float32)[:, None] * inverse[None, :]
    cos_pad = np.zeros((seq_len, LANES), np.float32)
    sin_pad = np.zeros((seq_len, LANES), np.float32)
    cos_pad[:, :NOPE] = 1.0
    cos_pad[:, NOPE:HEAD] = np.tile(np.cos(angles), (1, 2))
    sin_pad[:, NOPE:HEAD] = np.tile(np.sin(angles), (1, 2))
    turns = np.concatenate([np.cos(angles).T, np.sin(angles).T], axis=0)
    window = min(2 * LANES, heads * HEAD)
    spread = np.zeros((heads, window, 2 * LANES), np.float32)
    for h in range(heads):
        off = h * HEAD - window_start(h, heads)
        for i in range(HEAD):
            spread[h, off + i, i] = 1.0
        for i in range(half):
            a, b = NOPE + i, NOPE + half + i
            spread[h, off + b, LANES + a] = -1.0
            spread[h, off + a, LANES + b] = 1.0
    return cos_pad, sin_pad, turns, spread


def transfer_plan(n_fs, span, groups, cuts):
    count = groups * cuts
    paired = span % 2 == 0
    if n_fs == 4 and paired:
        third, half = count // 3, count // 2
        keep = count - third
        lists = {1: [(0, (0, 2)), (0, (2, 4))] + [(v, None) for v in range(1, keep)] + [(keep, (0, 2))],
                 2: [(v, None) for v in range(count - 1, third - 1, -1)]}
        by_y = [(1, v, None) for v in range(half)] + [(1, half, (0, 1))]
        by_x = [(2, v, None) for v in range(count - 1, half, -1)] + [(2, half, (1, 4))]
        crosses = [by_y[k : k + 1] + (by_x[k - 1 : k] if k > 0 else []) for k in range(len(by_y))]
        pairs = [(1, 0, (0, 2)), (1, 0, (2, 4)), (2, count - 1, None)]
        pairs += [(1, v, None) for v in range(1, third - 1)] + [(1, third - 1, (2, 4))]
        pairs += [(2, v, None) for v in range(count - 2, keep - 1, -1)]
        when = {(j, v): k + 1 for j in lists for k, (v, _) in enumerate(lists[j])}
        for k, step in enumerate(crosses):
            for _, v, _ in step:
                when[3, v] = keep + k
        for k, (j, v, _) in enumerate(pairs):
            when[j, count - 1 - v] = half + 2 + k
    else:
        lists = {j: [(v, None) for v in range(count)] for j in range(1, n_fs)}
        crosses, pairs = [], []
        when = {(j, v): v * n_fs + j for j in lists for v, _ in lists[j]}
    last = {(j, g): max(when[j, g * cuts + b] for b in range(cuts)) for j in range(1, n_fs) for g in range(groups)}
    order = [(0, g) for g in range(groups)] + sorted(last, key=lambda one: (last[one], one))
    bounds = [0, len(order) // 2, 3 * len(order) // 4, len(order)]
    batches = []
    for lo, hi in zip(bounds, bounds[1:]):
        batch = []
        for j, g in sorted(order[lo:hi]):
            if batch and batch[-1][0] == j and batch[-1][1] + batch[-1][2] == g and batch[-1][2] == 1:
                batch[-1] = (j, batch[-1][1], 2)
            else:
                batch.append((j, g, 1))
        batches.append(batch)
    return lists, crosses, pairs, batches


def arrival_slots(n_fs, groups, cuts, crosses, pairs):
    relayed = {(j, v) for step in crosses + [pairs] for j, v, _ in step}
    slots = {}
    for j in range(1, n_fs):
        for g in range(groups):
            chunks = range(g * cuts, (g + 1) * cuts)
            for v in chunks if any((j, v) in relayed for v in chunks) else chunks[:1]:
                slots[j, v] = len(slots) + (len(slots) > 0)
    return slots


def kernel(
    sizes,
    q_hbm, f_hbm, v_hbm, floor_hbm, extra_hbm, gain_hbm, aq_hbm, lat_hbm, rk_hbm,
    lgain_hbm, wup_hbm, cos_hbm, sin_hbm, turn_hbm, spread_hbm, w1_hbm, w2_hbm,
    out_ref, logw_ref,
    qfv_ref, floor_ref, extra_ref, gain_ref, aq_ref, lat_ref, rk_ref,
    lgain_ref, wup_ref, cs_ref, turn_ref, spread_ref,
    lbuf, ssend, srecv, wbuf, psend, precv, keep,
    kbuf, vbuf, intra, qd_ref, kd_ref, qc_ref, st_ref, act, whole_state, whole_decay,
    in_sem, own_sem, l_send, l_recv, f_send, f_recv, s_send, s_recv, w_send, w_recv,
    x_send, x_recv,
):
    n_fs, span = sizes
    _, tokens, width = qfv_ref.shape
    heads = width // HG_DK
    att_heads = aq_ref.shape[1] // HEAD
    up = att_heads * (NOPE + VDIM)
    blocks = tokens // BLOCK
    latent_width = lat_ref.shape[1]
    columns = w1_hbm.shape[1]
    cut_rows = w2_hbm.shape[0]
    cuts = w1_hbm.shape[0] // cut_rows + 1
    groups = columns // LANES
    rows = tokens // 2
    half_rope = ROPE // 2

    sp, fs, tp = lax.axis_index("sp"), lax.axis_index("fs"), lax.axis_index("tp")
    place = lax.rem(sp, span)
    base = sp - place
    parity = lax.rem(place, 2)
    has_left, has_right = place > 0, place < span - 1
    left = {"sp": base + jnp.maximum(place - 1, 0)}
    right = {"sp": base + jnp.minimum(place + 1, span - 1)}
    pair = {"sp": base + flip_bits(place, 1)}
    partner = {"tp": 1 - tp}
    mesh_id = pl.DeviceIdType.MESH

    def fs_peer(j):
        return {"fs": flip_bits(fs, j)}

    direct, crosses, pairs, batches = transfer_plan(n_fs, span, groups, cuts)

    def at_chunk(v):
        g, b = divmod(v, cuts)
        return g + parity * (groups - 1 - 2 * g), b + parity * (cuts - 1 - 2 * b)

    def chunk(j, v, part=None):
        g, b = at_chunk(v)
        lo, hi = part or (0, 4)
        quarter = cut_rows // 4
        first = pl.multiple_of(b * cut_rows + lo * quarter, quarter)
        return wbuf.at[j, pl.ds(first, (hi - lo) * quarter), pl.ds(pl.multiple_of(g * LANES, LANES), LANES)]

    slots = arrival_slots(n_fs, groups, cuts, crosses, pairs)

    def alone(j, v):
        return (j, v - v % cuts + 1) in slots

    def arrival(j, v, seen, part=None):
        if not alone(j, seen):
            seen -= seen % cuts
        return w_recv.at[slots[j, seen] + ((j, seen) == (1, 0) and part == (2, 4))]

    def remote(src, dst, send, recv, device):
        return pltpu.make_async_remote_copy(
            src_ref=src, dst_ref=dst, send_sem=send, recv_sem=recv,
            device_id=device, device_id_type=mesh_id,
        )

    def fetch(k, src, dst):
        return pltpu.make_async_copy(src, dst, in_sem.at[k])

    own = [
        pltpu.make_async_copy(src, wbuf.at[0, pl.ds(at, src.shape[0]), :], own_sem.at[0])
        for k, (src, at) in enumerate(((w1_hbm, 0), (w2_hbm, w1_hbm.shape[0])))
    ]
    for c in own:
        c.start()
    my_tokens = pl.ds(pl.multiple_of(place * tokens, tokens), tokens)
    tp_up = pl.ds(pl.multiple_of(tp * up, LANES), up)
    early = [
        fetch(0, lat_hbm, lat_ref), fetch(1, rk_hbm, rk_ref), fetch(2, lgain_hbm, lgain_ref),
        fetch(3, turn_hbm.at[:, my_tokens], turn_ref),
    ]
    qfv = [fetch(6, src, qfv_ref.at[k]) for k, src in enumerate((q_hbm, f_hbm, v_hbm))]
    turning = [fetch(7, src.at[my_tokens, :], cs_ref.at[k]) for k, src in enumerate((cos_hbm, sin_hbm))]
    gates = [
        fetch(4, floor_hbm, floor_ref), fetch(5, extra_hbm, extra_ref),
    ]
    late = [
        fetch(8, gain_hbm, gain_ref), fetch(9, aq_hbm, aq_ref), fetch(10, wup_hbm.at[:, tp_up], wup_ref),
        fetch(11, spread_hbm, spread_ref),
    ]
    for c in early + qfv + gates + turning + late:
        c.start()

    barrier = pltpu.get_barrier_semaphore()
    for j in direct:
        pl.semaphore_signal(barrier, inc=1, device_id=fs_peer(j), device_id_type=mesh_id)
    pl.semaphore_signal(barrier, inc=1, device_id=partner, device_id_type=mesh_id)

    @pl.when(has_left)
    def _():
        pl.semaphore_signal(barrier, inc=1, device_id=left, device_id_type=mesh_id)

    @pl.when(has_right)
    def _():
        pl.semaphore_signal(barrier, inc=1, device_id=right, device_id_type=mesh_id)

    for c in early:
        c.wait()
    lat = lat_ref[...].astype(F32)
    normed = lat * lax.rsqrt(jnp.mean(lat * lat, axis=-1, keepdims=True) + norm_eps) * lgain_ref[...]
    normed = normed.astype(BF16)
    rope_a, rope_b = rk_ref[:half_rope, :].astype(F32), rk_ref[half_rope:, :].astype(F32)
    turn_c, turn_s = turn_ref[:half_rope, :], turn_ref[half_rope:, :]
    turned_a = (rope_a * turn_c - rope_b * turn_s).astype(BF16)
    turned_b = (rope_a * turn_s + rope_b * turn_c).astype(BF16)
    for t in range(2):
        part = slice(t * rows, (t + 1) * rows)
        lbuf[place, t, :rows, :] = normed[part]
        lbuf[place, t, rows:, :rows] = turned_a[:, part]
        lbuf[place, t, rows:, rows:] = turned_b[:, part]

    def source(d, r):
        at = place - r if d == 0 else place + r
        there = at >= 0 if d == 0 else at < span
        onward = jnp.logical_and(there, has_right if d == 0 else has_left)
        return jnp.clip(at, 0, span - 1), there, onward

    def along(d, at):
        return remote(lbuf.at[at, tp], lbuf.at[at, tp], l_send.at[d, at], l_recv.at[at], right if d == 0 else left)

    def across(at):
        return remote(lbuf.at[at, tp], lbuf.at[at, tp], f_send.at[0], f_recv.at[at], partner)

    def latent_round(r):
        for d in range(2):
            at, there, onward = source(d, r)
            if r > 0:
                @pl.when(there)
                def _():
                    along(d, at).wait_recv()
                    across(at).start()

            if r < span - 1:
                @pl.when(onward)
                def _():
                    along(d, at).start()

    pltpu.make_async_copy(wbuf.at[0], wbuf.at[0], own_sem.at[0]).wait()
    pl.semaphore_wait(barrier, len(direct) + 1 + has_left.astype(jnp.int32) + has_right.astype(jnp.int32))
    latent_round(0)
    for k in range(max((len(direct[j]) for j in direct), default=0)):
        for j in direct:
            if k < len(direct[j]):
                v, part = direct[j][k]
                remote(chunk(0, v, part), chunk(j, v, part), w_send.at[0], arrival(j, v, v, part), fs_peer(j)).start()
    arrived = set()

    def await_chunk(j, v, part=None):
        if not alone(j, v):
            v -= v % cuts
        halves = (part,)
        if crosses and (j, v) == (1, 0) and part is None:
            halves = ((0, 2), (2, 4))
        elif (j, v) != (1, 0):
            halves = (None,)
        for one in halves:
            if (j, v, one) in arrived:
                continue
            arrived.add((j, v, one))
            ref = chunk(j, v, one)
            if not alone(j, v):
                ref = wbuf.at[j, :, pl.ds(pl.multiple_of(at_chunk(v)[0] * LANES, LANES), LANES)]
            remote(ref, ref, w_send.at[0], arrival(j, v, v, one), partner).wait_recv()

    def relay_cross(*ks):
        for k in ks:
            for j, v, part in crosses[k] if k < len(crosses) else ():
                await_chunk(j, v)
                remote(chunk(j, v, part), chunk(3, v, part), w_send.at[0], arrival(3, v, v), fs_peer(3 - j)).start()

    def relay_pair(lo, hi):
        for j, v, part in pairs[lo:hi]:
            await_chunk(j, v, part)
            seen = groups * cuts - 1 - v
            remote(chunk(j, v, part), chunk(j, v, part), w_send.at[0], arrival(j, v, seen), pair).start()

    held_from = max(len(crosses) - 2, 0)
    held_pair = max(len(pairs) - 1, 0)

    def relay_held():
        relay_cross(*range(held_from, len(crosses)))
        relay_pair(held_pair, len(pairs))

    def await_held():
        for j, v, _ in sum(crosses[held_from:], pairs[held_pair:]):
            await_chunk(j, v)

    row = lax.broadcasted_iota(jnp.int32, (BLOCK, BLOCK), 0)
    col = lax.broadcasted_iota(jnp.int32, (BLOCK, BLOCK), 1)
    lower = row >= col
    upper = row <= col
    tri = (jnp.where(lower, 1.0, 0.0).astype(BF16), jnp.where(upper, 1.0, 0.0).astype(BF16))
    fetch(6, qfv_ref, qfv_ref).wait()
    for c in gates:
        c.wait()
    spikes = lax.dot_general(
        extra_ref[...],
        jnp.where(
            lax.broadcasted_iota(jnp.int32, (heads, width), 0)
            == lax.broadcasted_iota(jnp.int32, (heads, width), 1) // HG_DK, 1.0, 0.0),
        (((0,), (0,)), ((), ())), precision=lax.Precision.HIGHEST, preferred_element_type=F32)
    first = jnp.where(2 * place < span, 0, 1)

    def link(d, h):
        towards = jnp.clip(place + 1 - 2 * d, 0, span - 1)
        return remote(ssend.at[d, h], srecv.at[d, h], s_send.at[d], s_recv.at[d, h],
                      {"sp": base + towards})

    def has_previous(d):
        return jnp.where(d == 0, place, span - 1 - place) > 0

    def has_next(d):
        return jnp.where(d == 0, span - 1 - place, place) > 0

    def pass_head(d, h):
        @pl.when(has_previous(d))
        def _():
            link(d, h).wait_recv()

        @pl.when(jnp.logical_not(has_previous(d)))
        def _():
            srecv[d, h] = jnp.zeros((HG_DK, HG_DK), BF16)

        @pl.when(has_next(d))
        def _():
            reached = srecv[d, h].astype(F32) * whole_decay[d, h, 0:1] + whole_state[d, h]
            ssend[d, h] = reached.astype(BF16)
            link(d, h).start()

    def pass_on(d):
        for h in range(heads):
            pass_head(d, h)

    twice = [jnp.concatenate([t, t], axis=1) for t in tri]
    block_decay = [[[None] * blocks for _ in range(2)] for _ in range(heads)]
    ahead = 2 if heads % 2 == 0 else 1
    for h0 in range(0, heads, ahead):
        wide_lanes = slice(h0 * HG_DK, (h0 + ahead) * HG_DK)
        for b in range(blocks):
            tok = slice(b * BLOCK, (b + 1) * BLOCK)
            q = qfv_ref[0, tok, wide_lanes].astype(F32)
            miss = 1.0 / (1.0 + jnp.exp(qfv_ref[1, tok, wide_lanes].astype(F32)))
            spike = spikes[tok, wide_lanes]
            ending = []
            for d in range(2):
                keyed = (1.0 - floor_ref[d : d + 1, wide_lanes]) * miss
                decay = jnp.log1p(-keyed) + spike
                hi = decay.astype(BF16)
                lo = (decay - hi.astype(F32)).astype(BF16)
                run = mm(twice[d], jnp.concatenate([hi, lo], axis=0))
                mid_at = BLOCK // 2 - 1 if d == 0 else BLOCK // 2
                end_at = BLOCK - 1 if d == 0 else 0
                mid = run[mid_at : mid_at + 1]
                end = run[end_at : end_at + 1]
                qd = q * jnp.exp(run - mid)
                kd = keyed * jnp.exp(mid - run)
                qd_ref[d, tok, wide_lanes] = qd.astype(BF16)
                kd_ref[d, tok, wide_lanes] = kd.astype(BF16)
                reach = (qd * jnp.exp(mid)).astype(BF16)
                ending.append((kd * jnp.exp(end - mid)).astype(BF16))
                last = jnp.exp(end)
                for i in range(ahead):
                    one = slice(i * HG_DK, (i + 1) * HG_DK)
                    qc_ref[tok, (2 * (h0 + i) + d) * HG_DK : (2 * (h0 + i) + d + 1) * HG_DK] = reach[:, one]
                    block_decay[h0 + i][d][b] = last[:, one]
            for i in range(ahead):
                h = h0 + i
                one = slice(i * HG_DK, (i + 1) * HG_DK)
                both = jnp.concatenate([e[:, one] for e in ending], axis=1)
                st_ref[b, h] = mm_tn(qfv_ref[2, tok, h * HG_DK : (h + 1) * HG_DK], both)
        for h in range(h0, h0 + ahead):
            for d in range(2):
                side = slice(d * HG_DK, (d + 1) * HG_DK)
                going = range(blocks) if d == 0 else range(blocks - 1, -1, -1)
                total, decay_all = None, None
                for b in going:
                    one = st_ref[b, h, :, side]
                    dec = block_decay[h][d][b]
                    total = one if total is None else total * dec + one
                    decay_all = dec if decay_all is None else decay_all * dec
                whole_state[d, h] = total
                whole_decay[d, h] = jnp.broadcast_to(decay_all, (8, HG_DK))

    @pl.when(jnp.logical_not(has_previous(first)))
    def _():
        pass_on(first)

    relay_pair(0, 3)
    if span > 1:
        latent_round(1)
    relay_pair(3, 4)

    for h in range(heads):
        lanes = slice(h * HG_DK, (h + 1) * HG_DK)
        for b in range(blocks):
            tok = slice(b * BLOCK, (b + 1) * BLOCK)
            scores = None
            for d in range(2):
                s = mm_nt(qd_ref[d, tok, lanes], kd_ref[d, tok, lanes])
                s = jnp.where(lower if d == 0 else upper, s, 0.0)
                scores = s if scores is None else scores + s
            intra[tok, lanes] = mm(scores.astype(BF16), qfv_ref[2, tok, lanes])

    fetch(7, cs_ref, cs_ref).wait()
    for c in late:
        c.wait()
    wup = wup_ref[...]
    half_lane = lax.broadcasted_iota(jnp.int32, (rows, LANES), 1)
    put_a = spread_ref[0, NOPE : NOPE + half_rope, :LANES]
    put_b = spread_ref[0, NOPE + half_rope : HEAD, :LANES]

    def expand(j):
        at = flip_bits(place, j)
        for t in range(2):
            keys = slice((2 * j + t) * rows, (2 * j + t + 1) * rows)
            expanded = mm(lbuf[at, t, :rows, :], wup)
            rot = mm_tn(lbuf[at, t, rows:, :rows], put_a) + mm_tn(lbuf[at, t, rows:, rows:], put_b)
            vbuf[keys, :] = expanded.astype(BF16)
            for h in range(att_heads):
                lanes = slice(h * LANES, (h + 1) * LANES)
                kbuf[keys, lanes] = jnp.where(half_lane < NOPE, expanded[:, lanes], rot).astype(BF16)

    for j in range(1, min(2, span)):
        across(flip_bits(place, j)).wait_recv()
    for j in range(min(2, span)):
        expand(j)
    relay_cross(0, 1)
    if span > 2:
        latent_round(2)
    relay_pair(4, 5)
    relay_cross(2)

    @pl.when(has_previous(first))
    def _():
        pass_on(first)

    relay_cross(3)
    for r in range(3, span):
        latent_round(r)
    for j in range(2, span):
        across(flip_bits(place, j)).wait_recv()
    for j in range(2, span):
        expand(j)
    relay_cross(4)

    def act_slot(t):
        return t + tp * (1 - 2 * t)

    cos, sin = cs_ref[0], cs_ref[1]
    scale = HEAD ** (-0.5)
    lane = lax.broadcasted_iota(jnp.int32, (tokens, LANES), 1)
    logw = jnp.zeros((tokens, LANES), F32)
    kept = None
    for h in range(att_heads):
        lanes = slice(h * LANES, (h + 1) * LANES)
        start = window_start(h, att_heads)
        placed = mm(aq_ref[:, start : start + spread_ref.shape[1]], spread_ref[h])
        query = placed[:, :LANES] * cos + placed[:, LANES:] * sin
        scores = mm_nt(query.astype(BF16), kbuf[:, lanes]) * scale
        peak = jnp.max(scores, axis=-1, keepdims=True)
        weights = jnp.exp(scores - peak)
        totals = jnp.sum(weights, axis=-1, keepdims=True)
        result = mm(weights.astype(BF16), vbuf[:, lanes]) / totals
        logw = jnp.where(lane == h, peak + jnp.log(totals), logw)
        if h % 2 == 0:
            kept = pltpu.roll(result, VDIM, 1)
        else:
            at = width + (h // 2) * LANES
            joined = jnp.where(lane < VDIM, kept, result).astype(BF16)
            for t in range(2):
                act[act_slot(t), :, at : at + LANES] = joined[t * rows : (t + 1) * rows]
            if h == 1:
                @pl.when(has_next(1 - first))
                def _():
                    pass_on(1 - first)

                relay_pair(5, max(held_pair, 5))
    relay_cross(*range(5, max(held_from, 5)))
    await_held()

    @pl.when(tp == 0)
    def _():
        relay_held()

    logw_ref[...] = jnp.transpose(logw)[:att_heads]

    @pl.when(jnp.logical_not(has_next(1 - first)))
    def _():
        pass_on(1 - first)

    for h in range(heads):
        lanes = slice(h * HG_DK, (h + 1) * HG_DK)
        carry = [srecv[d, h].astype(F32) for d in range(2)]
        starts = [[None] * blocks for _ in range(2)]
        for d in range(2):
            side = slice(d * HG_DK, (d + 1) * HG_DK)
            for b in range(blocks) if d == 0 else range(blocks - 1, -1, -1):
                starts[d][b] = carry[d].astype(BF16)
                carry[d] = carry[d] * block_decay[h][d][b] + st_ref[b, h, :, side]
        for b in range(blocks):
            tok = slice(b * BLOCK, (b + 1) * BLOCK)
            t, off = divmod(b * BLOCK, rows)
            begin = jnp.concatenate([starts[0][b], starts[1][b]], axis=1)
            o = intra[tok, lanes] + mm_nt(qc_ref[tok, 2 * h * HG_DK : 2 * (h + 1) * HG_DK], begin)
            o = o * lax.rsqrt(jnp.mean(o * o, axis=-1, keepdims=True) + norm_eps) * gain_ref[:, lanes]
            act[act_slot(t), off : off + BLOCK, lanes] = o.astype(BF16)

    def real_at(g, n):
        return pl.multiple_of((g + parity * (groups - n - 2 * g)) * LANES, LANES)

    x_copies, spans = [], []
    top = act.shape[2]

    def finish(n):
        lo, hi = spans[n]
        x_copies[n].wait_recv()
        at = lo
        for j, g, many in batches[n]:
            w = many * LANES
            there = pl.multiple_of(flip_bits(fs, j) * columns + real_at(g, many), LANES)
            both = keep[:, at : at + w].astype(F32) + precv[:, at : at + w].astype(F32)
            out_ref[:, pl.ds(there, w)] = both.astype(BF16)
            at += w

    offset = 0
    for n, batch in enumerate(batches):
        for j, g, many in batch:
            if j > 0:
                for v in range(g * cuts, (g + many) * cuts):
                    await_chunk(j, v)
        if n == 1:
            @pl.when(tp != 0)
            def _():
                relay_held()

        start = offset
        for j, g, many in batch:
            w = many * LANES
            both = mm(act[...].reshape(2 * rows, top), wbuf[j, :, pl.ds(real_at(g, many), w)]).astype(BF16)
            psend[:, offset : offset + w] = both[rows:]
            keep[:, offset : offset + w] = both[:rows]
            offset += w
        part = slice(start, offset)
        spans.append((start, offset))
        c = remote(psend.at[:, part], precv.at[:, part], x_send.at[0], x_recv.at[n], partner)
        c.start()
        x_copies.append(c)
        if n > 0:
            finish(n - 1)
    finish(len(batches) - 1)

    if direct:
        remote(wbuf.at[1:], wbuf.at[1:], w_send.at[0], w_recv.at[0], partner).wait_send()
    remote(psend, precv, x_send.at[0], x_recv.at[0], partner).wait_send()

    if span > 1:
        all_across = lbuf.at[: span - 1, 0]
        remote(all_across, all_across, f_send.at[0], f_recv.at[0], partner).wait_send()
    for r in range(span):
        for d in range(2):
            at, there, onward = source(d, r)
            if r < span - 1:
                @pl.when(onward)
                def _():
                    along(d, at).wait_send()

    for d in range(2):
        @pl.when(has_next(d))
        def _():
            remote(ssend.at[d], srecv.at[d], s_send.at[d], s_recv.at[d, 0], partner).wait_send()


def flush(mixed_ref, logw_ref, mixed_hbm, logw_hbm, sems):
    copies = (
        pltpu.make_async_copy(mixed_ref, mixed_hbm, sems.at[0]),
        pltpu.make_async_copy(logw_ref, logw_hbm, sems.at[1]),
    )
    for c in copies:
        c.start()
    for c in copies:
        c.wait()


def local(
    n_fs,
    n_sp,
    recurrent_query,
    forget_logits,
    recurrent_value,
    forget_floor,
    extra_log_decay,
    recurrent_norm_gain,
    attention_query,
    latent,
    rotary_key,
    latent_norm_gain,
    latent_up_weight,
    recurrent_output_weight,
    attention_output_weight,
):
    span = min(n_sp, widest_span)
    tokens, width = recurrent_query.shape[1:]
    heads = width // HG_DK
    att_heads = attention_query.shape[2] // HEAD
    latent_width = latent.shape[2]
    columns = recurrent_output_weight.shape[1]
    att_width = attention_output_weight.shape[0]
    up = att_heads * (NOPE + VDIM)
    blocks = tokens // BLOCK
    rows = tokens // 2
    groups = columns // LANES
    cuts = width // att_width + 1
    _, crosses, pairs, _ = transfer_plan(n_fs, span, groups, cuts)
    slots = len(arrival_slots(n_fs, groups, cuts, crosses, pairs)) + 1
    cos_pad, sin_pad, turns, spread = rope_constants(span * tokens, att_heads)
    vmem = pltpu.VMEM
    whole = pl.BlockSpec(memory_space=vmem)
    hbm = pl.BlockSpec(memory_space=pltpu.HBM)
    dma = pltpu.SemaphoreType.DMA
    mixed, log_weight = pl.pallas_call(
        functools.partial(kernel, (n_fs, span)),
        out_shape=(
            vmem((rows, columns * n_fs), BF16),
            vmem((att_heads, tokens), F32),
        ),
        in_specs=[hbm] * 17,
        out_specs=(whole, whole),
        scratch_shapes=[
            vmem((3, tokens, width), BF16),
            vmem((2, width), F32), vmem((heads, tokens), F32), vmem((1, width), F32),
            vmem((tokens, att_heads * HEAD), BF16), vmem((tokens, latent_width), BF16), vmem((ROPE, tokens), BF16),
            vmem((1, latent_width), F32), vmem((latent_width, up), BF16),
            vmem((2, tokens, LANES), F32), vmem((ROPE, tokens), F32),
            vmem(spread.shape, BF16),
            vmem((span, 2, rows + ROPE // 2, latent_width), BF16),
            vmem((2, heads, HG_DK, HG_DK), BF16),
            vmem((2, heads, HG_DK, HG_DK), BF16),
            vmem((n_fs, width + att_width, columns), BF16),
            vmem((rows, n_fs * columns), BF16),
            vmem((rows, n_fs * columns), BF16),
            vmem((rows, n_fs * columns), BF16),
            vmem((span * tokens, att_heads * LANES), BF16),
            vmem((span * tokens, att_heads * LANES), BF16),
            vmem((tokens, width), F32),
            vmem((2, tokens, width), BF16),
            vmem((2, tokens, width), BF16),
            vmem((tokens, 2 * width), BF16),
            vmem((blocks, heads, HG_DK, 2 * HG_DK), F32),
            vmem((2, rows, width + att_width), BF16),
            vmem((2, heads, HG_DK, HG_DK), F32),
            vmem((2, heads, 8, HG_DK), F32),
            dma((12,)), dma((1,)), dma((2, span)), dma((span,)), dma((1,)), dma((span,)),
            dma((2,)), dma((2, heads)),
            dma((1,)), dma((max(slots, 1),)),
            dma((1,)), dma((3,)),
        ],
        compiler_params=pltpu.CompilerParams(
            collective_id=0, has_side_effects=True, vmem_limit_bytes=56 * 2**20
        ),
        name="mixers",
    )(
        recurrent_query[0],
        forget_logits[0],
        recurrent_value[0],
        forget_floor,
        extra_log_decay[0].T,
        recurrent_norm_gain[None],
        attention_query[0],
        latent[0],
        rotary_key[0].T,
        latent_norm_gain[None],
        latent_up_weight,
        jnp.asarray(cos_pad),
        jnp.asarray(sin_pad),
        jnp.asarray(turns),
        jnp.asarray(spread, BF16),
        recurrent_output_weight,
        attention_output_weight,
    )
    mixed = pltpu.with_memory_space_constraint(mixed, vmem)
    log_weight = pltpu.with_memory_space_constraint(log_weight, vmem)
    mixed, log_weight = pl.pallas_call(
        flush,
        out_shape=(
            jax.ShapeDtypeStruct((rows, columns * n_fs), BF16),
            jax.ShapeDtypeStruct((att_heads, tokens), F32),
        ),
        in_specs=[whole, whole],
        out_specs=(hbm, hbm),
        scratch_shapes=[dma((2,))],
        name="flush",
    )(mixed, log_weight)
    return mixed[None], log_weight.T[None]


def solution(mesh):
    placed = (
        P("fs", "sp", "tp"),
        P("fs", "sp", "tp"),
        P("fs", "sp", "tp"),
        P(None, "tp"),
        P("fs", "sp", "tp"),
        P("tp"),
        P("fs", "sp", "tp"),
        P("fs", "sp", None),
        P("fs", "sp", None),
        P(),
        P(),
        P("tp", "fs"),
        P("tp", "fs"),
    )
    return jax.shard_map(
        functools.partial(local, mesh.shape["fs"], mesh.shape["sp"]),
        mesh=mesh,
        in_specs=placed,
        out_specs=(P("fs", ("sp", "tp"), None), P("fs", "sp", "tp")),
        check_vma=False,
    )
```

```python
import functools
import math

import jax
import jax.numpy as jnp
import numpy as np
from jax import lax
from jax.experimental import pallas as pl
from jax.experimental.pallas import tpu as pltpu
from jax.sharding import PartitionSpec as P

HG_DK = 128
NOPE = 64
ROPE = 32
VDIM = 64
HEAD = NOPE + ROPE
LANES = 128
BLOCK = 128

norm_eps = 1e-06
rope_base = 10000.0
widest_span = 8

F32 = jnp.float32
BF16 = jnp.bfloat16


def mm(a, b):
    return jnp.dot(a, b, preferred_element_type=F32)


def mm_nt(a, b):
    return lax.dot_general(a, b, (((1,), (1,)), ((), ())), preferred_element_type=F32)


def mm_tn(a, b):
    return lax.dot_general(a, b, (((0,), (0,)), ((), ())), preferred_element_type=F32)


def flip_bits(value, mask):
    bit = 1
    while bit <= mask:
        if mask & bit:
            value = value + bit - 2 * bit * lax.rem(value // bit, 2)
        bit *= 2
    return value


def window_start(h, heads):
    return min(h * HEAD // LANES * LANES, max(heads * HEAD - 2 * LANES, 0))


def rope_constants(seq_len, heads):
    half = ROPE // 2
    inverse = (np.float32(rope_base) ** (-np.arange(half, dtype=np.float32) / np.float32(half))).astype(np.float32)
    angles = np.arange(seq_len, dtype=np.float32)[:, None] * inverse[None, :]
    cos_pad = np.zeros((seq_len, LANES), np.float32)
    sin_pad = np.zeros((seq_len, LANES), np.float32)
    cos_pad[:, :NOPE] = 1.0
    cos_pad[:, NOPE:HEAD] = np.tile(np.cos(angles), (1, 2))
    sin_pad[:, NOPE:HEAD] = np.tile(np.sin(angles), (1, 2))
    turns = np.concatenate([np.cos(angles).T, np.sin(angles).T], axis=0)
    window = min(2 * LANES, heads * HEAD)
    spread = np.zeros((heads, window, 2 * LANES), np.float32)
    for h in range(heads):
        off = h * HEAD - window_start(h, heads)
        for i in range(HEAD):
            spread[h, off + i, i] = 1.0
        for i in range(half):
            a, b = NOPE + i, NOPE + half + i
            spread[h, off + b, LANES + a] = -1.0
            spread[h, off + a, LANES + b] = 1.0
    return cos_pad, sin_pad, turns, spread


def transfer_plan(n_fs, span, groups, cuts):
    count = groups * cuts
    paired = span % 2 == 0
    if n_fs == 4 and paired:
        third, half = count // 3, count // 2
        keep = count - third
        lists = {1: [(0, (0, 2)), (0, (2, 4))] + [(v, None) for v in range(1, keep)] + [(keep, (0, 2))],
                 2: [(v, None) for v in range(count - 1, third - 1, -1)]}
        by_y = [(1, v, None) for v in range(half)] + [(1, half, (0, 1))]
        by_x = [(2, v, None) for v in range(count - 1, half, -1)] + [(2, half, (1, 4))]
        crosses = [by_y[k : k + 1] + (by_x[k - 1 : k] if k > 0 else []) for k in range(len(by_y))]
        pairs = [(1, 0, (0, 2)), (1, 0, (2, 4)), (2, count - 1, None)]
        pairs += [(1, v, None) for v in range(1, third - 1)] + [(1, third - 1, (2, 4))]
        pairs += [(2, v, None) for v in range(count - 2, keep - 1, -1)]
        when = {(j, v): k + 1 for j in lists for k, (v, _) in enumerate(lists[j])}
        for k, step in enumerate(crosses):
            for _, v, _ in step:
                when[3, v] = keep + k
        for k, (j, v, _) in enumerate(pairs):
            when[j, count - 1 - v] = half - 1 + k
    else:
        lists = {j: [(v, None) for v in range(count)] for j in range(1, n_fs)}
        crosses, pairs = [], []
        when = {(j, v): v * n_fs + j for j in lists for v, _ in lists[j]}
    last = {(j, g): max(when[j, g * cuts + b] for b in range(cuts)) for j in range(1, n_fs) for g in range(groups)}
    order = [(0, g) for g in range(groups)] + sorted(last, key=lambda one: (last[one], one))
    bounds = [len(order) * part // 8 for part in (0, 4, 6, 7, 8)]
    batches = []
    for lo, hi in zip(bounds, bounds[1:]):
        batch = []
        for j, g in sorted(order[lo:hi]):
            if batch and batch[-1][0] == j and batch[-1][1] + batch[-1][2] == g and batch[-1][2] == 1:
                batch[-1] = (j, batch[-1][1], 2)
            else:
                batch.append((j, g, 1))
        batches.append(batch)
    return lists, crosses, pairs, batches


def arrival_slots(n_fs, groups, cuts, crosses, pairs):
    relayed = {(j, v) for step in crosses + [pairs] for j, v, _ in step}
    slots = {}
    for j in range(1, n_fs):
        for g in range(groups):
            chunks = range(g * cuts, (g + 1) * cuts)
            for v in chunks if any((j, v) in relayed for v in chunks) else chunks[:1]:
                slots[j, v] = len(slots) + (len(slots) > 0)
    return slots


def kernel(
    sizes,
    q_hbm, f_hbm, v_hbm, floor_hbm, extra_hbm, gain_hbm, aq_hbm, lat_hbm, rk_hbm,
    lgain_hbm, wup_hbm, cos_hbm, sin_hbm, turn_hbm, spread_hbm, w1_hbm, w2_hbm,
    out_ref, logw_ref,
    qfv_ref, floor_ref, extra_ref, gain_ref, aq_ref, lat_ref, rk_ref,
    lgain_ref, wup_ref, cs_ref, turn_ref, spread_ref,
    lbuf, ssend, srecv, wbuf, psend, precv, keep,
    kbuf, vbuf, intra, qd_ref, kd_ref, qc_ref, st_ref, act, whole_state, whole_decay,
    in_sem, own_sem, l_send, l_recv, f_send, f_recv, s_send, s_recv, w_send, w_recv,
    x_send, x_recv, ruler,
):
    n_fs, span = sizes
    _, tokens, width = qfv_ref.shape
    heads = width // HG_DK
    att_heads = aq_ref.shape[1] // HEAD
    up = att_heads * (NOPE + VDIM)
    blocks = tokens // BLOCK
    latent_width = lat_ref.shape[1]
    columns = w1_hbm.shape[1]
    cut_rows = w2_hbm.shape[0]
    cuts = w1_hbm.shape[0] // cut_rows + 1
    groups = columns // LANES
    rows = tokens // 2
    half_rope = ROPE // 2

    sp, fs, tp = lax.axis_index("sp"), lax.axis_index("fs"), lax.axis_index("tp")
    place = lax.rem(sp, span)
    base = sp - place
    parity = lax.rem(place, 2)
    has_left, has_right = place > 0, place < span - 1
    left = {"sp": base + jnp.maximum(place - 1, 0)}
    right = {"sp": base + jnp.minimum(place + 1, span - 1)}
    pair = {"sp": base + flip_bits(place, 1)}
    partner = {"tp": 1 - tp}
    mesh_id = pl.DeviceIdType.MESH

    def fs_peer(j):
        return {"fs": flip_bits(fs, j)}

    direct, crosses, pairs, batches = transfer_plan(n_fs, span, groups, cuts)

    def at_chunk(v):
        g, b = divmod(v, cuts)
        return g + parity * (groups - 1 - 2 * g), b + parity * (cuts - 1 - 2 * b)

    def chunk(j, v, part=None):
        g, b = at_chunk(v)
        lo, hi = part or (0, 4)
        quarter = cut_rows // 4
        first = pl.multiple_of(b * cut_rows + lo * quarter, quarter)
        return wbuf.at[j, pl.ds(first, (hi - lo) * quarter), pl.ds(pl.multiple_of(g * LANES, LANES), LANES)]

    slots = arrival_slots(n_fs, groups, cuts, crosses, pairs)

    def alone(j, v):
        return (j, v - v % cuts + 1) in slots

    def arrival(j, v, seen, part=None):
        if not alone(j, seen):
            seen -= seen % cuts
        return w_recv.at[slots[j, seen] + ((j, seen) == (1, 0) and part == (2, 4))]

    def remote(src, dst, send, recv, device):
        return pltpu.make_async_remote_copy(
            src_ref=src, dst_ref=dst, send_sem=send, recv_sem=recv,
            device_id=device, device_id_type=mesh_id,
        )

    def fetched(k, *refs):
        size = sum(math.prod(ref.shape) * ref.dtype.itemsize for ref in refs)
        ref = ruler.at[pl.ds(0, size // (4 * LANES)), :]
        pltpu.make_async_copy(ref, ref, in_sem.at[k]).wait()

    def fetch(k, src, dst):
        return pltpu.make_async_copy(src, dst, in_sem.at[k])

    barrier = pltpu.get_barrier_semaphore()
    for j in direct:
        pl.semaphore_signal(barrier, inc=1, device_id=fs_peer(j), device_id_type=mesh_id)
    pl.semaphore_signal(barrier, inc=1, device_id=partner, device_id_type=mesh_id)

    @pl.when(has_left)
    def _():
        pl.semaphore_signal(barrier, inc=1, device_id=left, device_id_type=mesh_id)

    @pl.when(has_right)
    def _():
        pl.semaphore_signal(barrier, inc=1, device_id=right, device_id_type=mesh_id)

    own = [
        pltpu.make_async_copy(src, wbuf.at[0, pl.ds(at, src.shape[0]), :], own_sem.at[0])
        for k, (src, at) in enumerate(((w1_hbm, 0), (w2_hbm, w1_hbm.shape[0])))
    ]
    for c in own:
        c.start()
    my_tokens = pl.ds(pl.multiple_of(place * tokens, tokens), tokens)
    tp_up = pl.ds(pl.multiple_of(tp * up, LANES), up)
    early = [
        fetch(0, lat_hbm, lat_ref), fetch(0, rk_hbm, rk_ref), fetch(0, lgain_hbm, lgain_ref),
        fetch(0, turn_hbm.at[:, my_tokens], turn_ref),
    ]
    gates = [fetch(1, src, qfv_ref.at[k]) for k, src in enumerate((q_hbm, f_hbm, v_hbm))]
    late = [fetch(2, src.at[my_tokens, :], cs_ref.at[k]) for k, src in enumerate((cos_hbm, sin_hbm))]
    gates += [fetch(1, floor_hbm, floor_ref), fetch(1, extra_hbm, extra_ref)]
    late += [
        fetch(2, gain_hbm, gain_ref), fetch(2, aq_hbm, aq_ref), fetch(2, wup_hbm.at[:, tp_up], wup_ref),
        fetch(2, spread_hbm, spread_ref),
    ]
    for c in early + gates + late:
        c.start()

    fetched(0, lat_ref, rk_ref, lgain_ref, turn_ref)
    lat = lat_ref[...].astype(F32)
    normed = lat * lax.rsqrt(jnp.mean(lat * lat, axis=-1, keepdims=True) + norm_eps) * lgain_ref[...]
    normed = normed.astype(BF16)
    rope_a, rope_b = rk_ref[:half_rope, :].astype(F32), rk_ref[half_rope:, :].astype(F32)
    turn_c, turn_s = turn_ref[:half_rope, :], turn_ref[half_rope:, :]
    turned_a = (rope_a * turn_c - rope_b * turn_s).astype(BF16)
    turned_b = (rope_a * turn_s + rope_b * turn_c).astype(BF16)
    for t in range(2):
        part = slice(t * rows, (t + 1) * rows)
        lbuf[place, t, :rows, :] = normed[part]
        lbuf[place, t, rows:, :rows] = turned_a[:, part]
        lbuf[place, t, rows:, rows:] = turned_b[:, part]

    def source(d, r):
        at = place - r if d == 0 else place + r
        there = at >= 0 if d == 0 else at < span
        onward = jnp.logical_and(there, has_right if d == 0 else has_left)
        return jnp.clip(at, 0, span - 1), there, onward

    def along(d, at):
        return remote(lbuf.at[at, tp], lbuf.at[at, tp], l_send.at[d], l_recv.at[at], right if d == 0 else left)

    def across(at):
        return remote(lbuf.at[at, tp], lbuf.at[at, tp], f_send.at[0], f_recv.at[at], partner)

    def latent_round(r):
        for d in range(2):
            at, there, onward = source(d, r)
            if r > 0:
                @pl.when(there)
                def _():
                    along(d, at).wait_recv()
                    across(at).start()

            if r < span - 1:
                @pl.when(onward)
                def _():
                    along(d, at).start()

    pltpu.make_async_copy(wbuf.at[0], wbuf.at[0], own_sem.at[0]).wait()
    pl.semaphore_wait(barrier, len(direct) + 1 + has_left.astype(jnp.int32) + has_right.astype(jnp.int32))
    latent_round(0)
    for k in range(max((len(direct[j]) for j in direct), default=0)):
        for j in direct:
            if k < len(direct[j]):
                v, part = direct[j][k]
                remote(chunk(0, v, part), chunk(j, v, part), w_send.at[0], arrival(j, v, v, part), fs_peer(j)).start()
    arrived = set()

    def await_chunk(j, v, part=None):
        if not alone(j, v):
            v -= v % cuts
        halves = (part,)
        if crosses and (j, v) == (1, 0) and part is None:
            halves = ((0, 2), (2, 4))
        elif (j, v) != (1, 0):
            halves = (None,)
        for one in halves:
            if (j, v, one) in arrived:
                continue
            arrived.add((j, v, one))
            ref = chunk(j, v, one)
            if not alone(j, v):
                ref = wbuf.at[j, :, pl.ds(pl.multiple_of(at_chunk(v)[0] * LANES, LANES), LANES)]
            remote(ref, ref, w_send.at[0], arrival(j, v, v, one), partner).wait_recv()

    def relay_cross(*ks):
        for k in ks:
            for j, v, part in crosses[k] if k < len(crosses) else ():
                await_chunk(j, v)
                remote(chunk(j, v, part), chunk(3, v, part), w_send.at[0], arrival(3, v, v), fs_peer(3 - j)).start()

    def relay_pair(lo, hi):
        for j, v, part in pairs[lo:hi]:
            await_chunk(j, v, part)
            seen = groups * cuts - 1 - v
            remote(chunk(j, v, part), chunk(j, v, part), w_send.at[0], arrival(j, v, seen), pair).start()

    held_from = max(len(crosses) - 2, 0)
    held_pair = max(len(pairs) - 1, 0)

    def relay_held():
        relay_cross(*range(held_from, len(crosses)))
        relay_pair(held_pair, len(pairs))

    def await_held():
        for j, v, _ in sum(crosses[held_from:], pairs[held_pair:]):
            await_chunk(j, v)

    row = lax.broadcasted_iota(jnp.int32, (BLOCK, BLOCK), 0)
    col = lax.broadcasted_iota(jnp.int32, (BLOCK, BLOCK), 1)
    lower = row >= col
    upper = row <= col
    tri = (jnp.where(lower, 1.0, 0.0).astype(BF16), jnp.where(upper, 1.0, 0.0).astype(BF16))
    fetched(1, qfv_ref, floor_ref, extra_ref)
    spikes = lax.dot_general(
        extra_ref[...],
        jnp.where(
            lax.broadcasted_iota(jnp.int32, (heads, width), 0)
            == lax.broadcasted_iota(jnp.int32, (heads, width), 1) // HG_DK, 1.0, 0.0),
        (((0,), (0,)), ((), ())), precision=lax.Precision.HIGHEST, preferred_element_type=F32)
    first = jnp.where(2 * place < span, 0, 1)

    def link(d, h):
        towards = jnp.clip(place + 1 - 2 * d, 0, span - 1)
        return remote(ssend.at[d, h], srecv.at[d, h], s_send.at[d], s_recv.at[d, h],
                      {"sp": base + towards})

    def has_previous(d):
        return jnp.where(d == 0, place, span - 1 - place) > 0

    def has_next(d):
        return jnp.where(d == 0, span - 1 - place, place) > 0

    def pass_head(d, h):
        @pl.when(has_previous(d))
        def _():
            link(d, h).wait_recv()

        @pl.when(jnp.logical_not(has_previous(d)))
        def _():
            srecv[d, h] = jnp.zeros((HG_DK, HG_DK), BF16)

        @pl.when(has_next(d))
        def _():
            reached = srecv[d, h].astype(F32) * whole_decay[d, h, 0:1] + whole_state[d, h]
            ssend[d, h] = reached.astype(BF16)
            link(d, h).start()

    def pass_on(d):
        for h in range(heads):
            pass_head(d, h)

    twice = [jnp.concatenate([t, t], axis=1) for t in tri]
    block_decay = [[[None] * blocks for _ in range(2)] for _ in range(heads)]
    ahead = 2 if heads % 2 == 0 else 1
    for h0 in range(0, heads, ahead):
        wide_lanes = slice(h0 * HG_DK, (h0 + ahead) * HG_DK)
        for b in range(blocks):
            tok = slice(b * BLOCK, (b + 1) * BLOCK)
            q = qfv_ref[0, tok, wide_lanes].astype(F32)
            miss = 1.0 / (1.0 + jnp.exp(qfv_ref[1, tok, wide_lanes].astype(F32)))
            spike = spikes[tok, wide_lanes]
            ending = []
            for d in range(2):
                keyed = (1.0 - floor_ref[d : d + 1, wide_lanes]) * miss
                decay = jnp.log1p(-keyed) + spike
                hi = decay.astype(BF16)
                lo = (decay - hi.astype(F32)).astype(BF16)
                run = mm(twice[d], jnp.concatenate([hi, lo], axis=0))
                mid_at = BLOCK // 2 - 1 if d == 0 else BLOCK // 2
                end_at = BLOCK - 1 if d == 0 else 0
                mid = run[mid_at : mid_at + 1]
                end = run[end_at : end_at + 1]
                qd = q * jnp.exp(run - mid)
                kd = keyed * jnp.exp(mid - run)
                qd_ref[d, tok, wide_lanes] = qd.astype(BF16)
                kd_ref[d, tok, wide_lanes] = kd.astype(BF16)
                reach = (qd * jnp.exp(mid)).astype(BF16)
                ending.append((kd * jnp.exp(end - mid)).astype(BF16))
                last = jnp.exp(end)
                for i in range(ahead):
                    one = slice(i * HG_DK, (i + 1) * HG_DK)
                    qc_ref[tok, (2 * (h0 + i) + d) * HG_DK : (2 * (h0 + i) + d + 1) * HG_DK] = reach[:, one]
                    block_decay[h0 + i][d][b] = last[:, one]
            for i in range(ahead):
                h = h0 + i
                one = slice(i * HG_DK, (i + 1) * HG_DK)
                both = jnp.concatenate([e[:, one] for e in ending], axis=1)
                st_ref[b, h] = mm_tn(qfv_ref[2, tok, h * HG_DK : (h + 1) * HG_DK], both)
        for h in range(h0, h0 + ahead):
            for d in range(2):
                side = slice(d * HG_DK, (d + 1) * HG_DK)
                going = range(blocks) if d == 0 else range(blocks - 1, -1, -1)
                total, decay_all = None, None
                for b in going:
                    one = st_ref[b, h, :, side]
                    dec = block_decay[h][d][b]
                    total = one if total is None else total * dec + one
                    decay_all = dec if decay_all is None else decay_all * dec
                whole_state[d, h] = total
                whole_decay[d, h] = jnp.broadcast_to(decay_all, (8, HG_DK))

    @pl.when(jnp.logical_not(has_previous(first)))
    def _():
        pass_on(first)

    relay_pair(0, 3)
    if span > 1:
        latent_round(1)
    relay_pair(3, 4)

    for h in range(heads):
        lanes = slice(h * HG_DK, (h + 1) * HG_DK)
        for b in range(blocks):
            tok = slice(b * BLOCK, (b + 1) * BLOCK)
            scores = None
            for d in range(2):
                s = mm_nt(qd_ref[d, tok, lanes], kd_ref[d, tok, lanes])
                s = jnp.where(lower if d == 0 else upper, s, 0.0)
                scores = s if scores is None else scores + s
            intra[tok, lanes] = mm(scores.astype(BF16), qfv_ref[2, tok, lanes])

    fetched(2, cs_ref, gain_ref, aq_ref, wup_ref, spread_ref)
    wup = wup_ref[...]
    half_lane = lax.broadcasted_iota(jnp.int32, (rows, LANES), 1)
    put_a = spread_ref[0, NOPE : NOPE + half_rope, :LANES]
    put_b = spread_ref[0, NOPE + half_rope : HEAD, :LANES]

    def expand(j):
        at = flip_bits(place, j)
        for t in range(2):
            keys = slice((2 * j + t) * rows, (2 * j + t + 1) * rows)
            expanded = mm(lbuf[at, t, :rows, :], wup)
            rot = mm_tn(lbuf[at, t, rows:, :rows], put_a) + mm_tn(lbuf[at, t, rows:, rows:], put_b)
            vbuf[keys, :] = expanded.astype(BF16)
            for h in range(att_heads):
                lanes = slice(h * LANES, (h + 1) * LANES)
                kbuf[keys, lanes] = jnp.where(half_lane < NOPE, expanded[:, lanes], rot).astype(BF16)

    for j in range(1, min(2, span)):
        across(flip_bits(place, j)).wait_recv()
    for j in range(min(2, span)):
        expand(j)
    relay_cross(0, 1)
    if span > 2:
        latent_round(2)
    relay_pair(4, 5)
    relay_cross(2)

    @pl.when(has_previous(first))
    def _():
        pass_on(first)

    relay_cross(3)
    for r in range(3, span):
        latent_round(r)
    for j in range(2, span):
        across(flip_bits(place, j)).wait_recv()
    for j in range(2, span):
        expand(j)
    relay_cross(4)

    def act_slot(t):
        return t + tp * (1 - 2 * t)

    cos, sin = cs_ref[0], cs_ref[1]
    scale = HEAD ** (-0.5)
    lane = lax.broadcasted_iota(jnp.int32, (tokens, LANES), 1)
    logw = jnp.zeros((tokens, LANES), F32)
    kept = None
    for h in range(att_heads):
        lanes = slice(h * LANES, (h + 1) * LANES)
        start = window_start(h, att_heads)
        placed = mm(aq_ref[:, start : start + spread_ref.shape[1]], spread_ref[h])
        query = placed[:, :LANES] * cos + placed[:, LANES:] * sin
        scores = mm_nt(query.astype(BF16), kbuf[:, lanes]) * scale
        peak = jnp.max(scores, axis=-1, keepdims=True)
        weights = jnp.exp(scores - peak)
        totals = jnp.sum(weights, axis=-1, keepdims=True)
        result = mm(weights.astype(BF16), vbuf[:, lanes]) / totals
        logw = jnp.where(lane == h, peak + jnp.log(totals), logw)
        if h % 2 == 0:
            kept = pltpu.roll(result, VDIM, 1)
        else:
            at = width + (h // 2) * LANES
            joined = jnp.where(lane < VDIM, kept, result).astype(BF16)
            for t in range(2):
                act[act_slot(t), :, at : at + LANES] = joined[t * rows : (t + 1) * rows]
            if h == 1:
                @pl.when(has_next(1 - first))
                def _():
                    pass_on(1 - first)

                relay_pair(5, max(held_pair, 5))
    relay_cross(*range(5, max(held_from, 5)))
    await_held()

    @pl.when(tp == 0)
    def _():
        relay_held()

    logw_ref[...] = jnp.transpose(logw)[:att_heads]

    @pl.when(jnp.logical_not(has_next(1 - first)))
    def _():
        pass_on(1 - first)

    for h in range(heads):
        lanes = slice(h * HG_DK, (h + 1) * HG_DK)
        carry = [srecv[d, h].astype(F32) for d in range(2)]
        starts = [[None] * blocks for _ in range(2)]
        for d in range(2):
            side = slice(d * HG_DK, (d + 1) * HG_DK)
            for b in range(blocks) if d == 0 else range(blocks - 1, -1, -1):
                starts[d][b] = carry[d].astype(BF16)
                carry[d] = carry[d] * block_decay[h][d][b] + st_ref[b, h, :, side]
        for b in range(blocks):
            tok = slice(b * BLOCK, (b + 1) * BLOCK)
            t, off = divmod(b * BLOCK, rows)
            begin = jnp.concatenate([starts[0][b], starts[1][b]], axis=1)
            o = intra[tok, lanes] + mm_nt(qc_ref[tok, 2 * h * HG_DK : 2 * (h + 1) * HG_DK], begin)
            o = o * lax.rsqrt(jnp.mean(o * o, axis=-1, keepdims=True) + norm_eps) * gain_ref[:, lanes]
            act[act_slot(t), off : off + BLOCK, lanes] = o.astype(BF16)

    def real_at(g, n):
        return pl.multiple_of((g + parity * (groups - n - 2 * g)) * LANES, LANES)

    x_copies, spans = [], []
    top = act.shape[2]

    def finish(n):
        lo, hi = spans[n]
        x_copies[n].wait_recv()
        at = lo
        for j, g, many in batches[n]:
            w = many * LANES
            there = pl.multiple_of(flip_bits(fs, j) * columns + real_at(g, many), LANES)
            both = keep[:, at : at + w].astype(F32) + precv[:, at : at + w].astype(F32)
            out_ref[:, pl.ds(there, w)] = both.astype(BF16)
            at += w

    offset = 0
    for n, batch in enumerate(batches):
        for j, g, many in batch:
            if j > 0:
                for v in range(g * cuts, (g + many) * cuts):
                    await_chunk(j, v)
        if n == 1:
            @pl.when(tp != 0)
            def _():
                relay_held()

        start = offset
        for j, g, many in batch:
            w = many * LANES
            both = mm(act[...].reshape(2 * rows, top), wbuf[j, :, pl.ds(real_at(g, many), w)]).astype(BF16)
            psend[:, offset : offset + w] = both[rows:]
            keep[:, offset : offset + w] = both[:rows]
            offset += w
        part = slice(start, offset)
        spans.append((start, offset))
        c = remote(psend.at[:, part], precv.at[:, part], x_send.at[0], x_recv.at[n], partner)
        c.start()
        x_copies.append(c)
        if n > 0:
            finish(n - 1)
    finish(len(batches) - 1)

    if direct:
        remote(wbuf.at[1:], wbuf.at[1:], w_send.at[0], w_recv.at[0], partner).wait_send()
    remote(psend, precv, x_send.at[0], x_recv.at[0], partner).wait_send()

    if span > 1:
        all_across = lbuf.at[: span - 1, 0]
        remote(all_across, all_across, f_send.at[0], f_recv.at[0], partner).wait_send()
    for k in range(span - 1):
        passed = lbuf.at[: k + 1, 0]

        @pl.when(place == k)
        def _():
            remote(passed, passed, l_send.at[0], l_recv.at[0], partner).wait_send()

        @pl.when(place == span - 1 - k)
        def _():
            remote(passed, passed, l_send.at[1], l_recv.at[0], partner).wait_send()

    for d in range(2):
        @pl.when(has_next(d))
        def _():
            remote(ssend.at[d], srecv.at[d], s_send.at[d], s_recv.at[d, 0], partner).wait_send()


def flush(mixed_ref, logw_ref, mixed_hbm, logw_hbm, sems):
    logw_copy = pltpu.make_async_copy(logw_ref, logw_hbm, sems.at[1])
    logw_copy.start()
    size = mixed_ref.shape[0] // 4
    for k in range(4):
        part = pl.ds(k * size, size)
        pltpu.make_async_copy(mixed_ref.at[part], mixed_hbm.at[part], sems.at[0]).start()
    logw_copy.wait()
    pltpu.make_async_copy(mixed_ref, mixed_hbm, sems.at[0]).wait()


def local(
    n_fs,
    n_sp,
    recurrent_query,
    forget_logits,
    recurrent_value,
    forget_floor,
    extra_log_decay,
    recurrent_norm_gain,
    attention_query,
    latent,
    rotary_key,
    latent_norm_gain,
    latent_up_weight,
    recurrent_output_weight,
    attention_output_weight,
):
    span = min(n_sp, widest_span)
    tokens, width = recurrent_query.shape[1:]
    heads = width // HG_DK
    att_heads = attention_query.shape[2] // HEAD
    latent_width = latent.shape[2]
    columns = recurrent_output_weight.shape[1]
    att_width = attention_output_weight.shape[0]
    up = att_heads * (NOPE + VDIM)
    blocks = tokens // BLOCK
    rows = tokens // 2
    groups = columns // LANES
    cuts = width // att_width + 1
    _, crosses, pairs, _ = transfer_plan(n_fs, span, groups, cuts)
    slots = len(arrival_slots(n_fs, groups, cuts, crosses, pairs)) + 1
    cos_pad, sin_pad, turns, spread = rope_constants(span * tokens, att_heads)
    vmem = pltpu.VMEM
    whole = pl.BlockSpec(memory_space=vmem)
    hbm = pl.BlockSpec(memory_space=pltpu.HBM)
    dma = pltpu.SemaphoreType.DMA
    mixed, log_weight = pl.pallas_call(
        functools.partial(kernel, (n_fs, span)),
        out_shape=(
            vmem((rows, columns * n_fs), BF16),
            vmem((att_heads, tokens), F32),
        ),
        in_specs=[hbm] * 17,
        out_specs=(whole, whole),
        scratch_shapes=[
            vmem((3, tokens, width), BF16),
            vmem((2, width), F32), vmem((heads, tokens), F32), vmem((1, width), F32),
            vmem((tokens, att_heads * HEAD), BF16), vmem((tokens, latent_width), BF16), vmem((ROPE, tokens), BF16),
            vmem((1, latent_width), F32), vmem((latent_width, up), BF16),
            vmem((2, tokens, LANES), F32), vmem((ROPE, tokens), F32),
            vmem(spread.shape, BF16),
            vmem((span, 2, rows + ROPE // 2, latent_width), BF16),
            vmem((2, heads, HG_DK, HG_DK), BF16),
            vmem((2, heads, HG_DK, HG_DK), BF16),
            vmem((n_fs, width + att_width, columns), BF16),
            vmem((rows, n_fs * columns), BF16),
            vmem((rows, n_fs * columns), BF16),
            vmem((rows, n_fs * columns), BF16),
            vmem((span * tokens, att_heads * LANES), BF16),
            vmem((span * tokens, att_heads * LANES), BF16),
            vmem((tokens, width), F32),
            vmem((2, tokens, width), BF16),
            vmem((2, tokens, width), BF16),
            vmem((tokens, 2 * width), BF16),
            vmem((blocks, heads, HG_DK, 2 * HG_DK), F32),
            vmem((2, rows, width + att_width), BF16),
            vmem((2, heads, HG_DK, HG_DK), F32),
            vmem((2, heads, 8, HG_DK), F32),
            dma((3,)), dma((1,)), dma((2,)), dma((span,)), dma((1,)), dma((span,)),
            dma((2,)), dma((2, heads)),
            dma((1,)), dma((max(slots, 1),)),
            dma((1,)), dma((4,)),
            vmem((4096, LANES), F32),
        ],
        compiler_params=pltpu.CompilerParams(
            collective_id=0, has_side_effects=True, vmem_limit_bytes=56 * 2**20
        ),
        name="mixers",
    )(
        recurrent_query[0],
        forget_logits[0],
        recurrent_value[0],
        forget_floor,
        extra_log_decay[0].T,
        recurrent_norm_gain[None],
        attention_query[0],
        latent[0],
        rotary_key[0].T,
        latent_norm_gain[None],
        latent_up_weight,
        jnp.asarray(cos_pad),
        jnp.asarray(sin_pad),
        jnp.asarray(turns),
        jnp.asarray(spread, BF16),
        recurrent_output_weight,
        attention_output_weight,
    )
    mixed = pltpu.with_memory_space_constraint(mixed, vmem)
    log_weight = pltpu.with_memory_space_constraint(log_weight, vmem)
    mixed, log_weight = pl.pallas_call(
        flush,
        out_shape=(
            jax.ShapeDtypeStruct((rows, columns * n_fs), BF16),
            jax.ShapeDtypeStruct((att_heads, tokens), F32),
        ),
        in_specs=[whole, whole],
        out_specs=(hbm, hbm),
        scratch_shapes=[dma((2,))],
        name="flush",
    )(mixed, log_weight)
    return mixed[None], log_weight.T[None]


def solution(mesh):
    placed = (
        P("fs", "sp", "tp"),
        P("fs", "sp", "tp"),
        P("fs", "sp", "tp"),
        P(None, "tp"),
        P("fs", "sp", "tp"),
        P("tp"),
        P("fs", "sp", "tp"),
        P("fs", "sp", None),
        P("fs", "sp", None),
        P(),
        P(),
        P("tp", "fs"),
        P("tp", "fs"),
    )
    return jax.shard_map(
        functools.partial(local, mesh.shape["fs"], mesh.shape["sp"]),
        mesh=mesh,
        in_specs=placed,
        out_specs=(P("fs", ("sp", "tp"), None), P("fs", "sp", "tp")),
        check_vma=False,
    )
```

```python
import functools
import math

import jax
import jax.numpy as jnp
import numpy as np
from jax import lax
from jax.experimental import pallas as pl
from jax.experimental.pallas import tpu as pltpu
from jax.sharding import PartitionSpec as P

HG_DK = 128
NOPE = 64
ROPE = 32
VDIM = 64
HEAD = NOPE + ROPE
LANES = 128
BLOCK = 128

norm_eps = 1e-06
rope_base = 10000.0
widest_span = 8

F32 = jnp.float32
BF16 = jnp.bfloat16


def mm(a, b):
    return jnp.dot(a, b, preferred_element_type=F32)


def mm_nt(a, b):
    return lax.dot_general(a, b, (((1,), (1,)), ((), ())), preferred_element_type=F32)


def mm_tn(a, b):
    return lax.dot_general(a, b, (((0,), (0,)), ((), ())), preferred_element_type=F32)


def flip_bits(value, mask):
    bit = 1
    while bit <= mask:
        if mask & bit:
            value = value + bit - 2 * bit * lax.rem(value // bit, 2)
        bit *= 2
    return value


def window_start(h, heads):
    return min(h * HEAD // LANES * LANES, max(heads * HEAD - 2 * LANES, 0))


def rope_constants(seq_len, heads):
    half = ROPE // 2
    inverse = (np.float32(rope_base) ** (-np.arange(half, dtype=np.float32) / np.float32(half))).astype(np.float32)
    angles = np.arange(seq_len, dtype=np.float32)[:, None] * inverse[None, :]
    cos_pad = np.zeros((seq_len, LANES), np.float32)
    sin_pad = np.zeros((seq_len, LANES), np.float32)
    cos_pad[:, :NOPE] = 1.0
    cos_pad[:, NOPE:HEAD] = np.tile(np.cos(angles), (1, 2))
    sin_pad[:, NOPE:HEAD] = np.tile(np.sin(angles), (1, 2))
    turns = np.concatenate([np.cos(angles).T, np.sin(angles).T], axis=0)
    window = min(2 * LANES, heads * HEAD)
    spread = np.zeros((heads, window, 2 * LANES), np.float32)
    for h in range(heads):
        off = h * HEAD - window_start(h, heads)
        for i in range(HEAD):
            spread[h, off + i, i] = 1.0
        for i in range(half):
            a, b = NOPE + i, NOPE + half + i
            spread[h, off + b, LANES + a] = -1.0
            spread[h, off + a, LANES + b] = 1.0
    return cos_pad, sin_pad, turns, spread


def transfer_plan(n_fs, span, groups, cuts):
    count = groups * cuts
    paired = span % 2 == 0
    if n_fs == 4 and paired:
        third, half = count // 3, count // 2
        keep = count - third
        lists = {1: [(0, (0, 4)), (0, (4, 8))] + [(v, None) for v in range(1, keep)] + [(keep, (0, 4))],
                 2: [(v, None) for v in range(count - 1, third, -1)] + [(third, (0, 6))]}
        by_y = [(1, v, None) for v in range(half)] + [(1, half, (0, 3))]
        by_x = [(2, v, None) for v in range(count - 1, half, -1)] + [(2, half, (3, 8))]
        crosses = [by_y[k : k + 1] + (by_x[k - 1 : k] if k > 0 else []) for k in range(len(by_y))]
        pairs = [(1, 0, (0, 4)), (1, 0, (4, 8)), (2, count - 1, None)]
        pairs += [(1, v, None) for v in range(1, third - 1)] + [(1, third - 1, (4, 8))]
        pairs += [(2, v, None) for v in range(count - 2, keep - 1, -1)] + [(2, keep - 1, (6, 8))]
        when = {(j, v): k + 1 for j in lists for k, (v, _) in enumerate(lists[j])}
        for k, step in enumerate(crosses):
            for _, v, _ in step:
                when[3, v] = keep + k
        for k, (j, v, _) in enumerate(pairs):
            when[j, count - 1 - v] = half - 1 + k
    else:
        lists = {j: [(v, None) for v in range(count)] for j in range(1, n_fs)}
        crosses, pairs = [], []
        when = {(j, v): v * n_fs + j for j in lists for v, _ in lists[j]}
    last = {(j, g): max(when[j, g * cuts + b] for b in range(cuts)) for j in range(1, n_fs) for g in range(groups)}
    order = [(0, g) for g in range(groups)] + sorted(last, key=lambda one: (last[one], one))
    bounds = [len(order) * part // 8 for part in (0, 4, 6, 7, 8)]
    batches = []
    for lo, hi in zip(bounds, bounds[1:]):
        batch = []
        for j, g in sorted(order[lo:hi]):
            if batch and batch[-1][0] == j and batch[-1][1] + batch[-1][2] == g and batch[-1][2] == 1:
                batch[-1] = (j, batch[-1][1], 2)
            else:
                batch.append((j, g, 1))
        batches.append(batch)
    return lists, crosses, pairs, batches


def arrival_slots(n_fs, groups, cuts, crosses, pairs):
    relayed = {(j, v) for step in crosses + [pairs] for j, v, _ in step}
    slots = {}
    for j in range(1, n_fs):
        for g in range(groups):
            chunks = range(g * cuts, (g + 1) * cuts)
            for v in chunks if any((j, v) in relayed for v in chunks) else chunks[:1]:
                slots[j, v] = len(slots) + (len(slots) > 0)
    return slots


def kernel(
    sizes,
    q_hbm, f_hbm, v_hbm, floor_hbm, extra_hbm, gain_hbm, aq_hbm, lat_hbm, rk_hbm,
    lgain_hbm, wup_hbm, cos_hbm, sin_hbm, turn_hbm, spread_hbm, w1_hbm, w2_hbm,
    out_ref, logw_ref,
    qfv_ref, floor_ref, extra_ref, gain_ref, aq_ref, lat_ref, rk_ref,
    lgain_ref, wup_ref, cs_ref, turn_ref, spread_ref,
    lbuf, ssend, srecv, wbuf, psend, precv, keep,
    kbuf, vbuf, intra, qd_ref, kd_ref, qc_ref, st_ref, act, whole_state, whole_decay,
    in_sem, own_sem, l_send, l_recv, f_send, f_recv, s_send, s_recv, w_send, w_recv,
    x_send, x_recv, ruler,
):
    n_fs, span = sizes
    _, tokens, width = qfv_ref.shape
    heads = width // HG_DK
    att_heads = aq_ref.shape[1] // HEAD
    up = att_heads * (NOPE + VDIM)
    blocks = tokens // BLOCK
    latent_width = lat_ref.shape[1]
    columns = w1_hbm.shape[1]
    cut_rows = w2_hbm.shape[0]
    cuts = w1_hbm.shape[0] // cut_rows + 1
    groups = columns // LANES
    rows = tokens // 2
    half_rope = ROPE // 2

    sp, fs, tp = lax.axis_index("sp"), lax.axis_index("fs"), lax.axis_index("tp")
    place = lax.rem(sp, span)
    base = sp - place
    parity = lax.rem(place, 2)
    has_left, has_right = place > 0, place < span - 1
    left = {"sp": base + jnp.maximum(place - 1, 0)}
    right = {"sp": base + jnp.minimum(place + 1, span - 1)}
    pair = {"sp": base + flip_bits(place, 1)}
    partner = {"tp": 1 - tp}
    mesh_id = pl.DeviceIdType.MESH

    def fs_peer(j):
        return {"fs": flip_bits(fs, j)}

    direct, crosses, pairs, batches = transfer_plan(n_fs, span, groups, cuts)

    def at_chunk(v):
        g, b = divmod(v, cuts)
        return g + parity * (groups - 1 - 2 * g), b + parity * (cuts - 1 - 2 * b)

    def chunk(j, v, part=None):
        g, b = at_chunk(v)
        lo, hi = part or (0, 8)
        eighth = cut_rows // 8
        first = pl.multiple_of(b * cut_rows + lo * eighth, eighth)
        return wbuf.at[j, pl.ds(first, (hi - lo) * eighth), pl.ds(pl.multiple_of(g * LANES, LANES), LANES)]

    slots = arrival_slots(n_fs, groups, cuts, crosses, pairs)

    def alone(j, v):
        return (j, v - v % cuts + 1) in slots

    def arrival(j, v, seen, part=None):
        if not alone(j, seen):
            seen -= seen % cuts
        return w_recv.at[slots[j, seen] + ((j, seen) == (1, 0) and part == (4, 8))]

    def remote(src, dst, send, recv, device):
        return pltpu.make_async_remote_copy(
            src_ref=src, dst_ref=dst, send_sem=send, recv_sem=recv,
            device_id=device, device_id_type=mesh_id,
        )

    def fetched(k, *refs):
        size = sum(math.prod(ref.shape) * ref.dtype.itemsize for ref in refs)
        ref = ruler.at[pl.ds(0, size // (4 * LANES)), :]
        pltpu.make_async_copy(ref, ref, in_sem.at[k]).wait()

    def fetch(k, src, dst):
        return pltpu.make_async_copy(src, dst, in_sem.at[k])

    barrier = pltpu.get_barrier_semaphore()
    for j in direct:
        pl.semaphore_signal(barrier, inc=1, device_id=fs_peer(j), device_id_type=mesh_id)
    pl.semaphore_signal(barrier, inc=1, device_id=partner, device_id_type=mesh_id)

    @pl.when(has_left)
    def _():
        pl.semaphore_signal(barrier, inc=1, device_id=left, device_id_type=mesh_id)

    @pl.when(has_right)
    def _():
        pl.semaphore_signal(barrier, inc=1, device_id=right, device_id_type=mesh_id)

    own = [
        pltpu.make_async_copy(src, wbuf.at[0, pl.ds(at, src.shape[0]), :], own_sem.at[0])
        for k, (src, at) in enumerate(((w1_hbm, 0), (w2_hbm, w1_hbm.shape[0])))
    ]
    for c in own:
        c.start()
    my_tokens = pl.ds(pl.multiple_of(place * tokens, tokens), tokens)
    tp_up = pl.ds(pl.multiple_of(tp * up, LANES), up)
    early = [
        fetch(0, lat_hbm, lat_ref), fetch(0, rk_hbm, rk_ref), fetch(0, lgain_hbm, lgain_ref),
        fetch(0, turn_hbm.at[:, my_tokens], turn_ref),
    ]
    gates = [fetch(1, src, qfv_ref.at[k]) for k, src in enumerate((q_hbm, f_hbm, v_hbm))]
    late = [fetch(2, src.at[my_tokens, :], cs_ref.at[k]) for k, src in enumerate((cos_hbm, sin_hbm))]
    gates += [fetch(1, floor_hbm, floor_ref), fetch(1, extra_hbm, extra_ref)]
    late += [
        fetch(2, gain_hbm, gain_ref), fetch(2, aq_hbm, aq_ref), fetch(2, wup_hbm.at[:, tp_up], wup_ref),
        fetch(2, spread_hbm, spread_ref),
    ]
    for c in early + gates + late:
        c.start()

    fetched(0, lat_ref, rk_ref, lgain_ref, turn_ref)
    lat = lat_ref[...].astype(F32)
    normed = lat * lax.rsqrt(jnp.mean(lat * lat, axis=-1, keepdims=True) + norm_eps) * lgain_ref[...]
    normed = normed.astype(BF16)
    rope_a, rope_b = rk_ref[:half_rope, :].astype(F32), rk_ref[half_rope:, :].astype(F32)
    turn_c, turn_s = turn_ref[:half_rope, :], turn_ref[half_rope:, :]
    turned_a = (rope_a * turn_c - rope_b * turn_s).astype(BF16)
    turned_b = (rope_a * turn_s + rope_b * turn_c).astype(BF16)
    for t in range(2):
        part = slice(t * rows, (t + 1) * rows)
        lbuf[place, t, :rows, :] = normed[part]
        lbuf[place, t, rows:, :rows] = turned_a[:, part]
        lbuf[place, t, rows:, rows:] = turned_b[:, part]

    def source(d, r):
        at = place - r if d == 0 else place + r
        there = at >= 0 if d == 0 else at < span
        onward = jnp.logical_and(there, has_right if d == 0 else has_left)
        return jnp.clip(at, 0, span - 1), there, onward

    def along(d, at):
        return remote(lbuf.at[at, tp], lbuf.at[at, tp], l_send.at[d], l_recv.at[at], right if d == 0 else left)

    def across(at):
        return remote(lbuf.at[at, tp], lbuf.at[at, tp], f_send.at[0], f_recv.at[at], partner)

    def latent_round(r):
        for d in range(2):
            at, there, onward = source(d, r)
            if r > 0:
                @pl.when(there)
                def _():
                    along(d, at).wait_recv()
                    across(at).start()

            if r < span - 1:
                @pl.when(onward)
                def _():
                    along(d, at).start()

    pltpu.make_async_copy(wbuf.at[0], wbuf.at[0], own_sem.at[0]).wait()
    pl.semaphore_wait(barrier, len(direct) + 1 + has_left.astype(jnp.int32) + has_right.astype(jnp.int32))
    latent_round(0)
    for k in range(max((len(direct[j]) for j in direct), default=0)):
        for j in direct:
            if k < len(direct[j]):
                v, part = direct[j][k]
                remote(chunk(0, v, part), chunk(j, v, part), w_send.at[0], arrival(j, v, v, part), fs_peer(j)).start()
    arrived = set()

    def await_chunk(j, v, part=None):
        if not alone(j, v):
            v -= v % cuts
        halves = (part,)
        if crosses and (j, v) == (1, 0) and part is None:
            halves = ((0, 4), (4, 8))
        elif (j, v) != (1, 0):
            halves = (None,)
        for one in halves:
            if (j, v, one) in arrived:
                continue
            arrived.add((j, v, one))
            ref = chunk(j, v, one)
            if not alone(j, v):
                ref = wbuf.at[j, :, pl.ds(pl.multiple_of(at_chunk(v)[0] * LANES, LANES), LANES)]
            remote(ref, ref, w_send.at[0], arrival(j, v, v, one), partner).wait_recv()

    def relay_cross(*ks):
        for k in ks:
            for j, v, part in crosses[k] if k < len(crosses) else ():
                await_chunk(j, v)
                remote(chunk(j, v, part), chunk(3, v, part), w_send.at[0], arrival(3, v, v), fs_peer(3 - j)).start()

    def relay_pair(lo, hi):
        for j, v, part in pairs[lo:hi]:
            await_chunk(j, v, part)
            seen = groups * cuts - 1 - v
            remote(chunk(j, v, part), chunk(j, v, part), w_send.at[0], arrival(j, v, seen), pair).start()

    held_from = max(len(crosses) - 2, 0)
    held_pair = max(len(pairs) - 2, 0)

    def relay_held():
        relay_cross(*range(held_from, len(crosses)))
        relay_pair(held_pair, len(pairs))

    def await_held():
        for j, v, _ in sum(crosses[held_from:], pairs[held_pair:]):
            await_chunk(j, v)

    row = lax.broadcasted_iota(jnp.int32, (BLOCK, BLOCK), 0)
    col = lax.broadcasted_iota(jnp.int32, (BLOCK, BLOCK), 1)
    lower = row >= col
    upper = row <= col
    tri = (jnp.where(lower, 1.0, 0.0).astype(BF16), jnp.where(upper, 1.0, 0.0).astype(BF16))
    fetched(1, qfv_ref, floor_ref, extra_ref)
    spikes = lax.dot_general(
        extra_ref[...],
        jnp.where(
            lax.broadcasted_iota(jnp.int32, (heads, width), 0)
            == lax.broadcasted_iota(jnp.int32, (heads, width), 1) // HG_DK, 1.0, 0.0),
        (((0,), (0,)), ((), ())), precision=lax.Precision.HIGHEST, preferred_element_type=F32)
    first = jnp.where(2 * place < span, 0, 1)

    def link(d, h):
        towards = jnp.clip(place + 1 - 2 * d, 0, span - 1)
        return remote(ssend.at[d, h], srecv.at[d, h], s_send.at[d], s_recv.at[d, h],
                      {"sp": base + towards})

    def has_previous(d):
        return jnp.where(d == 0, place, span - 1 - place) > 0

    def has_next(d):
        return jnp.where(d == 0, span - 1 - place, place) > 0

    def pass_head(d, h):
        @pl.when(has_previous(d))
        def _():
            link(d, h).wait_recv()

        @pl.when(jnp.logical_not(has_previous(d)))
        def _():
            srecv[d, h] = jnp.zeros((HG_DK, HG_DK), BF16)

        @pl.when(has_next(d))
        def _():
            reached = srecv[d, h].astype(F32) * whole_decay[d, h, 0:1] + whole_state[d, h]
            ssend[d, h] = reached.astype(BF16)
            link(d, h).start()

    def pass_on(d):
        for h in range(heads):
            pass_head(d, h)

    twice = [jnp.concatenate([t, t], axis=1) for t in tri]
    block_decay = [[[None] * blocks for _ in range(2)] for _ in range(heads)]
    ahead = 2 if heads % 2 == 0 else 1
    for h0 in range(0, heads, ahead):
        wide_lanes = slice(h0 * HG_DK, (h0 + ahead) * HG_DK)
        for b in range(blocks):
            tok = slice(b * BLOCK, (b + 1) * BLOCK)
            q = qfv_ref[0, tok, wide_lanes].astype(F32)
            miss = 1.0 / (1.0 + jnp.exp(qfv_ref[1, tok, wide_lanes].astype(F32)))
            spike = spikes[tok, wide_lanes]
            ending = []
            for d in range(2):
                keyed = (1.0 - floor_ref[d : d + 1, wide_lanes]) * miss
                decay = jnp.log1p(-keyed) + spike
                hi = decay.astype(BF16)
                lo = (decay - hi.astype(F32)).astype(BF16)
                run = mm(twice[d], jnp.concatenate([hi, lo], axis=0))
                mid_at = BLOCK // 2 - 1 if d == 0 else BLOCK // 2
                end_at = BLOCK - 1 if d == 0 else 0
                mid = run[mid_at : mid_at + 1]
                end = run[end_at : end_at + 1]
                qd = q * jnp.exp(run - mid)
                kd = keyed * jnp.exp(mid - run)
                qd_ref[d, tok, wide_lanes] = qd.astype(BF16)
                kd_ref[d, tok, wide_lanes] = kd.astype(BF16)
                reach = (qd * jnp.exp(mid)).astype(BF16)
                ending.append((kd * jnp.exp(end - mid)).astype(BF16))
                last = jnp.exp(end)
                for i in range(ahead):
                    one = slice(i * HG_DK, (i + 1) * HG_DK)
                    qc_ref[tok, (2 * (h0 + i) + d) * HG_DK : (2 * (h0 + i) + d + 1) * HG_DK] = reach[:, one]
                    block_decay[h0 + i][d][b] = last[:, one]
            for i in range(ahead):
                h = h0 + i
                one = slice(i * HG_DK, (i + 1) * HG_DK)
                both = jnp.concatenate([e[:, one] for e in ending], axis=1)
                st_ref[b, h] = mm_tn(qfv_ref[2, tok, h * HG_DK : (h + 1) * HG_DK], both)
        for h in range(h0, h0 + ahead):
            for d in range(2):
                side = slice(d * HG_DK, (d + 1) * HG_DK)
                going = range(blocks) if d == 0 else range(blocks - 1, -1, -1)
                total, decay_all = None, None
                for b in going:
                    one = st_ref[b, h, :, side]
                    dec = block_decay[h][d][b]
                    total = one if total is None else total * dec + one
                    decay_all = dec if decay_all is None else decay_all * dec
                whole_state[d, h] = total
                whole_decay[d, h] = jnp.broadcast_to(decay_all, (8, HG_DK))

    @pl.when(jnp.logical_not(has_previous(first)))
    def _():
        pass_on(first)

    relay_pair(0, 3)
    if span > 1:
        latent_round(1)
    relay_pair(3, 4)

    for h in range(heads):
        lanes = slice(h * HG_DK, (h + 1) * HG_DK)
        for b in range(blocks):
            tok = slice(b * BLOCK, (b + 1) * BLOCK)
            scores = None
            for d in range(2):
                s = mm_nt(qd_ref[d, tok, lanes], kd_ref[d, tok, lanes])
                s = jnp.where(lower if d == 0 else upper, s, 0.0)
                scores = s if scores is None else scores + s
            intra[tok, lanes] = mm(scores.astype(BF16), qfv_ref[2, tok, lanes])

    fetched(2, cs_ref, gain_ref, aq_ref, wup_ref, spread_ref)
    wup = wup_ref[...]
    half_lane = lax.broadcasted_iota(jnp.int32, (rows, LANES), 1)
    put_a = spread_ref[0, NOPE : NOPE + half_rope, :LANES]
    put_b = spread_ref[0, NOPE + half_rope : HEAD, :LANES]

    def expand(j):
        at = flip_bits(place, j)
        for t in range(2):
            keys = slice((2 * j + t) * rows, (2 * j + t + 1) * rows)
            expanded = mm(lbuf[at, t, :rows, :], wup)
            rot = mm_tn(lbuf[at, t, rows:, :rows], put_a) + mm_tn(lbuf[at, t, rows:, rows:], put_b)
            vbuf[keys, :] = expanded.astype(BF16)
            for h in range(att_heads):
                lanes = slice(h * LANES, (h + 1) * LANES)
                kbuf[keys, lanes] = jnp.where(half_lane < NOPE, expanded[:, lanes], rot).astype(BF16)

    for j in range(1, min(2, span)):
        across(flip_bits(place, j)).wait_recv()
    for j in range(min(2, span)):
        expand(j)
    relay_cross(0, 1)
    if span > 2:
        latent_round(2)
    relay_pair(4, 5)
    relay_cross(2)

    @pl.when(has_previous(first))
    def _():
        pass_on(first)

    relay_cross(3)
    for r in range(3, span):
        latent_round(r)
    for j in range(2, span):
        across(flip_bits(place, j)).wait_recv()
    for j in range(2, span):
        expand(j)
    relay_cross(4)

    def act_slot(t):
        return t + tp * (1 - 2 * t)

    cos, sin = cs_ref[0], cs_ref[1]
    scale = HEAD ** (-0.5)
    lane = lax.broadcasted_iota(jnp.int32, (tokens, LANES), 1)
    logw = jnp.zeros((tokens, LANES), F32)
    kept = None
    for h in range(att_heads):
        lanes = slice(h * LANES, (h + 1) * LANES)
        start = window_start(h, att_heads)
        placed = mm(aq_ref[:, start : start + spread_ref.shape[1]], spread_ref[h])
        query = placed[:, :LANES] * cos + placed[:, LANES:] * sin
        scores = mm_nt(query.astype(BF16), kbuf[:, lanes]) * scale
        peak = jnp.max(scores, axis=-1, keepdims=True)
        weights = jnp.exp(scores - peak)
        totals = jnp.sum(weights, axis=-1, keepdims=True)
        result = mm(weights.astype(BF16), vbuf[:, lanes]) / totals
        logw = jnp.where(lane == h, peak + jnp.log(totals), logw)
        if h % 2 == 0:
            kept = pltpu.roll(result, VDIM, 1)
        else:
            at = width + (h // 2) * LANES
            joined = jnp.where(lane < VDIM, kept, result).astype(BF16)
            for t in range(2):
                act[act_slot(t), :, at : at + LANES] = joined[t * rows : (t + 1) * rows]
            if h == 1:
                @pl.when(has_next(1 - first))
                def _():
                    pass_on(1 - first)

                relay_pair(5, max(held_pair, 5))
    relay_cross(*range(5, max(held_from, 5)))
    await_held()

    @pl.when(tp == 0)
    def _():
        relay_held()

    logw_ref[...] = jnp.transpose(logw)[:att_heads]

    @pl.when(jnp.logical_not(has_next(1 - first)))
    def _():
        pass_on(1 - first)

    for h in range(heads):
        lanes = slice(h * HG_DK, (h + 1) * HG_DK)
        carry = [srecv[d, h].astype(F32) for d in range(2)]
        starts = [[None] * blocks for _ in range(2)]
        for d in range(2):
            side = slice(d * HG_DK, (d + 1) * HG_DK)
            for b in range(blocks) if d == 0 else range(blocks - 1, -1, -1):
                starts[d][b] = carry[d].astype(BF16)
                carry[d] = carry[d] * block_decay[h][d][b] + st_ref[b, h, :, side]
        for b in range(blocks):
            tok = slice(b * BLOCK, (b + 1) * BLOCK)
            t, off = divmod(b * BLOCK, rows)
            begin = jnp.concatenate([starts[0][b], starts[1][b]], axis=1)
            o = intra[tok, lanes] + mm_nt(qc_ref[tok, 2 * h * HG_DK : 2 * (h + 1) * HG_DK], begin)
            o = o * lax.rsqrt(jnp.mean(o * o, axis=-1, keepdims=True) + norm_eps) * gain_ref[:, lanes]
            act[act_slot(t), off : off + BLOCK, lanes] = o.astype(BF16)

    def real_at(g, n):
        return pl.multiple_of((g + parity * (groups - n - 2 * g)) * LANES, LANES)

    x_copies, spans = [], []
    top = act.shape[2]

    def finish(n):
        lo, hi = spans[n]
        x_copies[n].wait_recv()
        at = lo
        for j, g, many in batches[n]:
            w = many * LANES
            there = pl.multiple_of(flip_bits(fs, j) * columns + real_at(g, many), LANES)
            both = keep[:, at : at + w].astype(F32) + precv[:, at : at + w].astype(F32)
            out_ref[:, pl.ds(there, w)] = both.astype(BF16)
            at += w

    offset = 0
    for n, batch in enumerate(batches):
        for j, g, many in batch:
            if j > 0:
                for v in range(g * cuts, (g + many) * cuts):
                    await_chunk(j, v)
        if n == 1:
            @pl.when(tp != 0)
            def _():
                relay_held()

        start = offset
        for j, g, many in batch:
            w = many * LANES
            both = mm(act[...].reshape(2 * rows, top), wbuf[j, :, pl.ds(real_at(g, many), w)]).astype(BF16)
            psend[:, offset : offset + w] = both[rows:]
            keep[:, offset : offset + w] = both[:rows]
            offset += w
        part = slice(start, offset)
        spans.append((start, offset))
        c = remote(psend.at[:, part], precv.at[:, part], x_send.at[0], x_recv.at[n], partner)
        c.start()
        x_copies.append(c)
        if n > 0:
            finish(n - 1)
    finish(len(batches) - 1)

    if direct:
        remote(wbuf.at[1:], wbuf.at[1:], w_send.at[0], w_recv.at[0], partner).wait_send()
    remote(psend, precv, x_send.at[0], x_recv.at[0], partner).wait_send()

    if span > 1:
        all_across = lbuf.at[: span - 1, 0]
        remote(all_across, all_across, f_send.at[0], f_recv.at[0], partner).wait_send()
    for k in range(span - 1):
        passed = lbuf.at[: k + 1, 0]

        @pl.when(place == k)
        def _():
            remote(passed, passed, l_send.at[0], l_recv.at[0], partner).wait_send()

        @pl.when(place == span - 1 - k)
        def _():
            remote(passed, passed, l_send.at[1], l_recv.at[0], partner).wait_send()

    for d in range(2):
        @pl.when(has_next(d))
        def _():
            remote(ssend.at[d], srecv.at[d], s_send.at[d], s_recv.at[d, 0], partner).wait_send()


def flush(mixed_ref, logw_ref, mixed_hbm, logw_hbm, sems):
    logw_copy = pltpu.make_async_copy(logw_ref, logw_hbm, sems.at[1])
    logw_copy.start()
    size = mixed_ref.shape[0] // 4
    for k in range(4):
        part = pl.ds(k * size, size)
        pltpu.make_async_copy(mixed_ref.at[part], mixed_hbm.at[part], sems.at[0]).start()
    logw_copy.wait()
    pltpu.make_async_copy(mixed_ref, mixed_hbm, sems.at[0]).wait()


def local(
    n_fs,
    n_sp,
    recurrent_query,
    forget_logits,
    recurrent_value,
    forget_floor,
    extra_log_decay,
    recurrent_norm_gain,
    attention_query,
    latent,
    rotary_key,
    latent_norm_gain,
    latent_up_weight,
    recurrent_output_weight,
    attention_output_weight,
):
    span = min(n_sp, widest_span)
    tokens, width = recurrent_query.shape[1:]
    heads = width // HG_DK
    att_heads = attention_query.shape[2] // HEAD
    latent_width = latent.shape[2]
    columns = recurrent_output_weight.shape[1]
    att_width = attention_output_weight.shape[0]
    up = att_heads * (NOPE + VDIM)
    blocks = tokens // BLOCK
    rows = tokens // 2
    groups = columns // LANES
    cuts = width // att_width + 1
    _, crosses, pairs, _ = transfer_plan(n_fs, span, groups, cuts)
    slots = len(arrival_slots(n_fs, groups, cuts, crosses, pairs)) + 1
    cos_pad, sin_pad, turns, spread = rope_constants(span * tokens, att_heads)
    vmem = pltpu.VMEM
    whole = pl.BlockSpec(memory_space=vmem)
    hbm = pl.BlockSpec(memory_space=pltpu.HBM)
    dma = pltpu.SemaphoreType.DMA
    mixed, log_weight = pl.pallas_call(
        functools.partial(kernel, (n_fs, span)),
        out_shape=(
            vmem((rows, columns * n_fs), BF16),
            vmem((att_heads, tokens), F32),
        ),
        in_specs=[hbm] * 17,
        out_specs=(whole, whole),
        scratch_shapes=[
            vmem((3, tokens, width), BF16),
            vmem((2, width), F32), vmem((heads, tokens), F32), vmem((1, width), F32),
            vmem((tokens, att_heads * HEAD), BF16), vmem((tokens, latent_width), BF16), vmem((ROPE, tokens), BF16),
            vmem((1, latent_width), F32), vmem((latent_width, up), BF16),
            vmem((2, tokens, LANES), F32), vmem((ROPE, tokens), F32),
            vmem(spread.shape, BF16),
            vmem((span, 2, rows + ROPE // 2, latent_width), BF16),
            vmem((2, heads, HG_DK, HG_DK), BF16),
            vmem((2, heads, HG_DK, HG_DK), BF16),
            vmem((n_fs, width + att_width, columns), BF16),
            vmem((rows, n_fs * columns), BF16),
            vmem((rows, n_fs * columns), BF16),
            vmem((rows, n_fs * columns), BF16),
            vmem((span * tokens, att_heads * LANES), BF16),
            vmem((span * tokens, att_heads * LANES), BF16),
            vmem((tokens, width), F32),
            vmem((2, tokens, width), BF16),
            vmem((2, tokens, width), BF16),
            vmem((tokens, 2 * width), BF16),
            vmem((blocks, heads, HG_DK, 2 * HG_DK), F32),
            vmem((2, rows, width + att_width), BF16),
            vmem((2, heads, HG_DK, HG_DK), F32),
            vmem((2, heads, 8, HG_DK), F32),
            dma((3,)), dma((1,)), dma((2,)), dma((span,)), dma((1,)), dma((span,)),
            dma((2,)), dma((2, heads)),
            dma((1,)), dma((max(slots, 1),)),
            dma((1,)), dma((4,)),
            vmem((4096, LANES), F32),
        ],
        compiler_params=pltpu.CompilerParams(
            collective_id=0, has_side_effects=True, vmem_limit_bytes=56 * 2**20
        ),
        name="mixers",
    )(
        recurrent_query[0],
        forget_logits[0],
        recurrent_value[0],
        forget_floor,
        extra_log_decay[0].T,
        recurrent_norm_gain[None],
        attention_query[0],
        latent[0],
        rotary_key[0].T,
        latent_norm_gain[None],
        latent_up_weight,
        jnp.asarray(cos_pad),
        jnp.asarray(sin_pad),
        jnp.asarray(turns),
        jnp.asarray(spread, BF16),
        recurrent_output_weight,
        attention_output_weight,
    )
    mixed = pltpu.with_memory_space_constraint(mixed, vmem)
    log_weight = pltpu.with_memory_space_constraint(log_weight, vmem)
    mixed, log_weight = pl.pallas_call(
        flush,
        out_shape=(
            jax.ShapeDtypeStruct((rows, columns * n_fs), BF16),
            jax.ShapeDtypeStruct((att_heads, tokens), F32),
        ),
        in_specs=[whole, whole],
        out_specs=(hbm, hbm),
        scratch_shapes=[dma((2,))],
        name="flush",
    )(mixed, log_weight)
    return mixed[None], log_weight.T[None]


def solution(mesh):
    placed = (
        P("fs", "sp", "tp"),
        P("fs", "sp", "tp"),
        P("fs", "sp", "tp"),
        P(None, "tp"),
        P("fs", "sp", "tp"),
        P("tp"),
        P("fs", "sp", "tp"),
        P("fs", "sp", None),
        P("fs", "sp", None),
        P(),
        P(),
        P("tp", "fs"),
        P("tp", "fs"),
    )
    return jax.shard_map(
        functools.partial(local, mesh.shape["fs"], mesh.shape["sp"]),
        mesh=mesh,
        in_specs=placed,
        out_specs=(P("fs", ("sp", "tp"), None), P("fs", "sp", "tp")),
        check_vma=False,
    )
```
